32 devices in a mesh: sp: 4 (over z), fs: 4 (over y, x), tp: 2 (over core).
Axes of the slice: x: 2, y: 2, z: 4, core: 2. Of those that a mesh axis runs over, the one named last changes fastest.
Arguments:
- tokens: bfloat16 [4, 768, 2048], P('fs', 'sp', 'tp'), may hold values from -24 to 24
- norm_gain: bfloat16 [2048], P('tp'), may hold values from 0.099609375 to 1.8984375
- w_q_down: bfloat16 [2048, 512], P('fs'), may hold values from -0.151 to 0.151
- q_gain: float32 [512], replicated, may hold values from 0.1 to 1.9
- w_q_nope: bfloat16 [512, 2048], P(None, 'tp'), may hold values from -1.21 to 1.21
- w_q_rope: bfloat16 [512, 1024], P(None, 'tp'), may hold values from -0.75 to 0.75
- w_kv_down: bfloat16 [2048, 256], P('fs'), may hold values from -0.151 to 0.151
- kv_gain: float32 [256], replicated, may hold values from 0.1 to 1.9
- w_k_up: bfloat16 [256, 2048], P(None, 'tp'), may hold values from -0.81 to 0.81
- w_v_up: bfloat16 [256, 2048], P(None, 'tp'), may hold values from -0.375 to 0.375
- w_k_rope: bfloat16 [2048, 64], replicated, may hold values from -0.125 to 0.125
- w_pool_in: bfloat16 [2048, 1024], P(None, 'tp'), may hold values from -0.125 to 0.125
- w_pool_mix: bfloat16 [4, 256, 256], replicated, may hold values from -0.375 to 0.375
- w_out_attn: bfloat16 [2048, 2048], P('tp'), may hold values from -0.125 to 0.125
- w_out_pool: bfloat16 [1024, 2048], P('tp'), may hold values from -0.1875 to 0.1875
Outputs:
- mixed: bfloat16 [4, 768, 2048], P('fs', ('sp', 'tp'))
The draws below stay inside these ranges and needn't reach their ends.
All inputs are finite; a program needn't handle non-finite values.
Results may differ from the reference program's by a relative error of at most 0.02.
Values may be sent and summed in bfloat16 or wider, within the bound.
A program may use at most 128 MiB of HBM per device.

```python
import jax
import jax.numpy as jnp
from jax import lax

D_MODEL = 2048
HEADS = 16
NOPE_DIM = 128
ROPE_DIM = 64
VALUE_DIM = 128
Q_RANK = 512
KV_RANK = 256
POOL_CH = 1024
GRID_W = 64
TOK_DEV = 192
POOL_GROUP = 256
SEQS = 4
SEQ_LEN = 768


def draw_tokens(key, part):
    base = jax.random.normal(jax.random.fold_in(key, 11), (SEQS, SEQ_LEN, D_MODEL), jnp.float32)
    return jnp.clip(base, -6.0, 6.0).astype(jnp.bfloat16)


def draw_w_q_down(key, part):
    base = jax.random.normal(jax.random.fold_in(key, 21), (D_MODEL, Q_RANK), jnp.float32)
    base = jnp.clip(base, -6.0, 6.0) * D_MODEL ** (-0.5)
    return jnp.clip(base, -0.15, 0.15).astype(jnp.bfloat16)


def draw_w_kv_down(key, part):
    base = jax.random.normal(jax.random.fold_in(key, 31), (D_MODEL, KV_RANK), jnp.float32)
    base = jnp.clip(base, -6.0, 6.0) * D_MODEL ** (-0.5)
    return jnp.clip(base, -0.15, 0.15).astype(jnp.bfloat16)


def draw_w_q_nope(key, part):
    base = jax.random.normal(jax.random.fold_in(key, 41), (Q_RANK, HEADS * NOPE_DIM), jnp.float32)
    base = jnp.clip(base, -6.0, 6.0) * (Q_RANK // 9) ** (-0.5)
    return jnp.clip(base, -1.2, 1.2).astype(jnp.bfloat16)


def draw_w_k_up(key, part):
    base = jax.random.normal(jax.random.fold_in(key, 51), (KV_RANK, HEADS * NOPE_DIM), jnp.float32)
    base = jnp.clip(base, -6.0, 6.0) * KV_RANK ** (-0.5)
    return jnp.clip(base, -0.8, 0.8).astype(jnp.bfloat16)


def block_levels(rng, dims, cuts, least, high):
    def one(axis_at, parts):
        heights = jax.random.uniform(jax.random.fold_in(jax.random.fold_in(rng, 6), axis_at), (parts,), jnp.float32, least / len(cuts), high / len(cuts))
        return jnp.repeat(jnp.exp(heights), dims[axis_at] // parts).reshape((-1,) + (1,) * (len(dims) - axis_at - 1))

    level = one(*cuts[0])
    for cut in cuts[1:]:
        level = level * one(*cut)
    return level


def scatter_about(own_key, shape, scale, reach, cuts=(), kind=jnp.bfloat16):
    values = scale * jax.random.normal(own_key, shape, jnp.float32)
    if cuts:
        values = values * block_levels(own_key, shape, cuts, -0.22, 0.18)
    return jnp.clip(values, -reach, reach).astype(kind)


def setup_inputs(seed: int = 0) -> dict:
    arg_keys = jax.random.split(jax.random.key(seed), 16)
    return {
        "tokens": draw_tokens(jax.random.fold_in(arg_keys[15], 71), 0),
        "norm_gain": jnp.clip(1.0 + 0.18 * jax.random.normal(arg_keys[1], (D_MODEL,), jnp.float32), 0.099609375, 1.8984375).astype(jnp.bfloat16),
        "w_q_down": draw_w_q_down(jax.random.fold_in(arg_keys[15], 71), 0),
        "q_gain": jnp.clip(1.0 + 0.18 * jax.random.normal(arg_keys[3], (Q_RANK,), jnp.float32), 0.1, 1.9),
        "w_q_nope": draw_w_q_nope(jax.random.fold_in(arg_keys[15], 71), 0),
        "w_q_rope": scatter_about(arg_keys[5], (Q_RANK, HEADS * ROPE_DIM), (Q_RANK // 9) ** -0.5, 0.75, ((1, 2),)),
        "w_kv_down": draw_w_kv_down(jax.random.fold_in(arg_keys[15], 71), 0),
        "kv_gain": jnp.clip(1.0 + 0.18 * jax.random.normal(arg_keys[7], (KV_RANK,), jnp.float32), 0.1, 1.9),
        "w_k_up": draw_w_k_up(jax.random.fold_in(arg_keys[15], 71), 0),
        "w_v_up": scatter_about(arg_keys[9], (KV_RANK, HEADS * VALUE_DIM), KV_RANK ** -0.5, 0.375, ((1, 2),)),
        "w_k_rope": scatter_about(arg_keys[10], (D_MODEL, ROPE_DIM), D_MODEL ** -0.5, 0.125),
        "w_pool_in": scatter_about(arg_keys[11], (D_MODEL, POOL_CH), D_MODEL ** -0.5, 0.125, ((1, 2),)),
        "w_pool_mix": scatter_about(arg_keys[12], (4, POOL_GROUP, POOL_GROUP), POOL_GROUP ** -0.5, 0.375),
        "w_out_attn": scatter_about(arg_keys[13], (HEADS * VALUE_DIM, D_MODEL), (HEADS * VALUE_DIM) ** -0.5, 0.125, ((0, 2),)),
        "w_out_pool": scatter_about(arg_keys[14], (POOL_CH, D_MODEL), POOL_CH ** -0.5, 0.1875, ((0, 2),)),
    }


EPS = 1e-06
THETA = 10000.0
window_sizes = (2, 4, 8, 16)

def normed(values, gain_vec):
    widened = values.astype(jnp.float32)
    scaled = widened * lax.rsqrt(lax.optimization_barrier(jnp.mean(widened * widened, axis=-1, keepdims=True)) + EPS)
    return (scaled * gain_vec.astype(jnp.float32)).astype(jnp.bfloat16)

def angles(position):
    row_index = (position // GRID_W).astype(jnp.float32)
    column = (position % GRID_W).astype(jnp.float32)
    inverse = THETA ** (-jnp.arange(0, ROPE_DIM // 2, 2).astype(jnp.float32) / (ROPE_DIM // 2))
    return jnp.stack([row_index, column], axis=-1)[:, :, None] * inverse

def rotate(values, angle_table):
    full_shape = values.shape
    split_parts = values.astype(jnp.float32).reshape(full_shape[:-1] + (2, 2, ROPE_DIM // 4))
    front_half = split_parts[..., 0, :]
    back_half = split_parts[..., 1, :]
    cosine = jnp.cos(angle_table)
    sine_part = jnp.sin(angle_table)
    turned = jnp.stack([front_half * cosine - back_half * sine_part, front_half * sine_part + back_half * cosine], axis=-2)
    return turned.reshape(full_shape).astype(jnp.bfloat16)

def attend(query_nope, query_rope, key_nope, key_rope, values_all):
    length = query_nope.shape[0]
    key_wide = key_nope.astype(jnp.float32)
    rope_wide = key_rope.astype(jnp.float32)
    value_wide = values_all.astype(jnp.float32)
    score_scale = (NOPE_DIM + ROPE_DIM) ** (-0.5)

    def one_block(block):
        query_part, rope_part = block
        scores = jnp.einsum('qhd,khd->hqk', query_part.astype(jnp.float32), key_wide)
        scores = scores + jnp.einsum('qhr,kr->hqk', rope_part.astype(jnp.float32), rope_wide)
        scores = scores * score_scale
        row_max = lax.optimization_barrier(jnp.max(scores, axis=-1, keepdims=True))
        weights = jnp.exp(scores - row_max)
        row_total = lax.optimization_barrier(jnp.sum(weights, axis=-1))
        rounded = lax.optimization_barrier(weights.astype(jnp.bfloat16))
        summed = jnp.einsum('hqk,khd->qhd', rounded.astype(jnp.float32), value_wide)
        return (summed / jnp.transpose(row_total)[:, :, None]).astype(jnp.bfloat16)
    blocks = length // TOK_DEV
    query_blocks = query_nope.reshape(blocks, TOK_DEV, HEADS, NOPE_DIM)
    rope_blocks = query_rope.reshape(blocks, TOK_DEV, HEADS, ROPE_DIM)
    result = lax.map(one_block, (query_blocks, rope_blocks))
    return result.reshape(length, HEADS * VALUE_DIM)

def pooled_mix(pool_in, w_pool_mix):
    length = pool_in.shape[0]
    sums = jnp.pad(jnp.cumsum(pool_in.astype(jnp.float32), axis=0), ((1, 0), (0, 0)))
    position = jnp.arange(length, dtype=jnp.int32)
    outputs = []
    for group, window in enumerate(window_sizes):
        low_edge = jnp.clip(position - window // 2, 0, length)
        high_edge = jnp.clip(position + window - window // 2, 0, length)
        group_sums = sums[:, group * POOL_GROUP:(group + 1) * POOL_GROUP]
        window_mean = (group_sums[high_edge] - group_sums[low_edge]) / (high_edge - low_edge).astype(jnp.float32)[:, None]
        spread = window_mean.astype(jnp.bfloat16) - pool_in[:, group * POOL_GROUP:(group + 1) * POOL_GROUP]
        outputs.append(jnp.dot(spread, w_pool_mix[group], preferred_element_type=jnp.float32).astype(jnp.bfloat16))
    return jnp.concatenate(outputs, axis=1)

def reference(tokens, norm_gain, w_q_down, q_gain, w_q_nope, w_q_rope, w_kv_down, kv_gain, w_k_up, w_v_up, w_k_rope, w_pool_in, w_pool_mix, w_out_attn, w_out_pool):

    def one_sequence(token_rows):
        length = token_rows.shape[0]
        position = jnp.arange(length, dtype=jnp.int32)
        angle_table = angles(position)
        hidden = normed(token_rows, norm_gain)
        q_latent = normed(jnp.dot(hidden, w_q_down, preferred_element_type=jnp.float32).astype(jnp.bfloat16), q_gain)
        kv_latent = normed(jnp.dot(hidden, w_kv_down, preferred_element_type=jnp.float32).astype(jnp.bfloat16), kv_gain)
        query_nope = jnp.dot(q_latent, w_q_nope, preferred_element_type=jnp.float32).astype(jnp.bfloat16)
        query_nope = query_nope.reshape(length, HEADS, NOPE_DIM)
        query_pre = jnp.dot(q_latent, w_q_rope, preferred_element_type=jnp.float32).astype(jnp.bfloat16)
        query_rope = rotate(query_pre.reshape(length, HEADS, ROPE_DIM), angle_table[:, None])
        key_nope = jnp.dot(kv_latent, w_k_up, preferred_element_type=jnp.float32).astype(jnp.bfloat16)
        key_nope = key_nope.reshape(length, HEADS, NOPE_DIM)
        values_all = jnp.dot(kv_latent, w_v_up, preferred_element_type=jnp.float32).astype(jnp.bfloat16)
        values_all = values_all.reshape(length, HEADS, VALUE_DIM)
        key_pre = jnp.dot(hidden, w_k_rope, preferred_element_type=jnp.float32).astype(jnp.bfloat16)
        key_rope = rotate(key_pre, angle_table)
        attended = attend(query_nope, query_rope, key_nope, key_rope, values_all)
        pool_in = jnp.dot(hidden, w_pool_in, preferred_element_type=jnp.float32).astype(jnp.bfloat16)
        pooled = pooled_mix(pool_in, w_pool_mix)
        combined = jnp.dot(attended, w_out_attn, preferred_element_type=jnp.float32)
        combined = combined + jnp.dot(pooled, w_out_pool, preferred_element_type=jnp.float32)
        return combined.astype(jnp.bfloat16)
    return lax.map(one_sequence, tokens)
```

```python
import functools
import math

import jax
import jax.numpy as jnp
from jax import lax
from jax.experimental import pallas as pl
from jax.experimental.pallas import tpu as pltpu
from jax.sharding import PartitionSpec as P

NOPE_DIM = 128
ROPE_DIM = 64
VALUE_DIM = 128
GRID_W = 64
POOL_GROUP = 256
EPS = 1e-06
THETA = 10000.0
WINDOWS = (2, 4, 8, 16)
RIM = 8
SPAN_LIMIT = 1024
F32 = jnp.float32
BF16 = jnp.bfloat16
MESH = pl.DeviceIdType.MESH


def mm(a, b):
    return jnp.dot(a, b, preferred_element_type=F32)


def mm_t(a, b):
    return lax.dot_general(a, b, (((1,), (1,)), ((), ())), preferred_element_type=F32)


def normed(wide, gain):
    scale = lax.rsqrt(jnp.mean(wide * wide, axis=-1, keepdims=True) + EPS)
    return (wide * scale * gain).astype(BF16)


def layer(
    n_sp,
    n_fs,
    tokens,
    norm_gain,
    w_q_down,
    q_gain,
    w_q_nope,
    w_q_rope,
    w_kv_down,
    kv_gain,
    w_k_up,
    w_v_up,
    w_k_rope,
    w_pool_in,
    w_pool_mix,
    w_out_attn,
    w_out_pool,
    out,
    tok,
    gain,
    hid,
    wq_all,
    wkv_all,
    qg,
    kvg,
    wqn,
    wqr,
    wku,
    wvu,
    wkr,
    wpi,
    mix,
    woa,
    wop,
    halo_out,
    halo_in,
    kvp,
    qp,
    ropes,
    kcat,
    qcat,
    ctx,
    att,
    acc,
    share,
    arrived,
    local_sem,
    send_sem,
    recv_sem,
    gather_send,
    gather_recv,
    pass_send,
    pass_recv,
    rope_send,
    rope_recv,
):
    s = lax.axis_index("sp")
    f = lax.axis_index("fs")
    t = lax.axis_index("tp")
    rows = tok.shape[1]
    half = rows // 2
    depth = w_q_down.shape[0]
    q_half = wq_all.shape[1]
    kv_half = wkv_all.shape[1]
    kv_rank = 2 * kv_half
    heads = wqn.shape[1] // NOPE_DIM
    groups = wpi.shape[1] // POOL_GROUP
    length = rows * n_sp

    def col(ref, width):
        return ref.at[:, pl.ds(pl.multiple_of(t * width, width), width)]

    def down(ref, owner, first=0, size=depth):
        start = pl.multiple_of(owner * depth + first, 16)
        return ref.at[pl.ds(start, size), :]

    pairs = (
        (tokens.at[0], tok.at[t]),
        (norm_gain, gain.at[t]),
        (col(w_kv_down, kv_half), down(wkv_all, f)),
        (col(w_q_down, q_half), down(wq_all, f)),
        (w_k_rope, wkr),
        (w_pool_in, wpi),
        (kv_gain, kvg),
        (q_gain, qg),
        (w_pool_mix.at[pl.ds(t * groups, groups)], mix),
        (w_out_pool, wop),
        (w_q_nope, wqn),
        (w_q_rope, wqr),
        (w_k_up, wku),
        (w_v_up, wvu),
        (w_out_attn, woa),
    )
    loads = [
        pltpu.make_async_copy(src, dst, local_sem.at[i]) for i, (src, dst) in enumerate(pairs)
    ]
    for load in loads:
        load.start()
    (
        l_tok,
        l_gain,
        l_kv,
        l_q,
        l_kr,
        l_pi,
        l_kvg,
        l_qg,
        l_mix,
        l_op,
        l_qn,
        l_qr,
        l_ku,
        l_vu,
        l_oa,
    ) = loads

    def signal_all():
        barrier = pltpu.get_barrier_semaphore()
        pl.semaphore_signal(barrier, inc=1, device_id={"tp": 1 - t}, device_id_type=MESH)
        for j in range(1, n_fs):
            pl.semaphore_signal(
                barrier, inc=1, device_id={"fs": (f + j) % n_fs}, device_id_type=MESH
            )
        for j in range(1, n_sp):
            pl.semaphore_signal(
                barrier, inc=1, device_id={"sp": (s + j) % n_sp}, device_id_type=MESH
            )
        return barrier

    barrier = signal_all()

    lane = lax.broadcasted_iota(jnp.int32, (rows, 128), 1)
    place = s * rows + lax.broadcasted_iota(jnp.int32, (rows, 128), 0)
    quarter = ROPE_DIM // 4
    power = (lane % quarter).astype(F32) * (2.0 / (ROPE_DIM // 2))
    inverse = jnp.exp(power * (-math.log(THETA)))
    grid_row = place // GRID_W
    grid_col = place - grid_row * GRID_W
    in_a = (lane % ROPE_DIM) < (ROPE_DIM // 2)
    angle = jnp.where(in_a, grid_row, grid_col).astype(F32) * inverse
    is_u = (lane % (2 * quarter)) < quarter
    cosine = jnp.cos(angle)
    sine = jnp.where(is_u, -jnp.sin(angle), jnp.sin(angle))

    def rotated(pre):
        wide = pre.astype(BF16).astype(F32)
        swapped = jnp.where(is_u, pltpu.roll(wide, 128 - quarter, 1), pltpu.roll(wide, quarter, 1))
        return wide * cosine + swapped * sine

    pl.semaphore_wait(barrier, n_sp + n_fs - 1)

    def remote(src, dst, sem, device):
        return pltpu.make_async_remote_copy(
            src_ref=src,
            dst_ref=dst,
            send_sem=send_sem.at[sem],
            recv_sem=recv_sem.at[sem],
            device_id=device,
            device_id_type=MESH,
        )

    mate = {"tp": 1 - t}
    l_tok.wait()
    c_tok = remote(tok.at[t], tok.at[t], 0, mate)
    c_tok.start()
    l_gain.wait()
    c_gain = remote(gain.at[t], gain.at[t], 1, mate)
    c_gain.start()

    chunks = 4
    chunk_rows = depth // chunks
    sends = [c_tok, c_gain]
    hops = n_fs == 4
    if hops:
        near = f + 1 - 2 * (f % 2)
        far = (f + 2) % 4
        through = near * (1 - t) + far * t
        onward = far * (1 - t) + near * t
        across = 3 - f
        partners = (near, far)
    else:
        partners = tuple((f + j) % n_fs for j in range(1, n_fs))
    senders = partners if hops else tuple((f + n_fs - j) % n_fs for j in range(1, n_fs))

    def spread_out(ref, base, first, size):
        for j, peer in enumerate(partners):
            copy = remote(
                down(ref, f, first, size), down(ref, f, first, size), base + j, {"fs": peer}
            )
            copy.start()
            sends.append(copy)

    def take(ref, owner, sem, first=0, size=depth):
        remote(
            down(ref, owner, first, size), down(ref, owner, first, size), sem, mate
        ).wait_recv()

    width = n_fs - 1
    b_kv = 8

    def b_q(chunk):
        return 8 + (1 + chunk) * width

    def spread_q(chunk):
        spread_out(wq_all, b_q(chunk), chunk * chunk_rows, chunk_rows)

    l_kv.wait()
    spread_out(wkv_all, b_kv, 0, depth)
    l_q.wait()
    spread_q(0)

    remote(gain.at[1 - t], gain.at[1 - t], 1, mate).wait_recv()
    remote(tok.at[1 - t], tok.at[1 - t], 0, mate).wait_recv()
    whole = jnp.concatenate([tok[0], tok[1]], axis=1).astype(F32)
    lines = gain.shape[1]
    wide_gain = [gain[0].astype(F32), gain[1].astype(F32)]
    flat_gain = jnp.concatenate(
        [side[i : i + 1, :] for side in wide_gain for i in range(lines)], axis=1
    )
    hid[...] = normed(whole, flat_gain)

    own_rows = pl.ds(pl.multiple_of(s * rows, rows), rows)

    def rows_of(owner):
        return pl.ds(pl.multiple_of(owner * rows, rows), rows)

    def over_sp(ref, pool_send, pool_recv, j, device):
        return pltpu.make_async_remote_copy(
            src_ref=ref,
            dst_ref=ref,
            send_sem=pool_send.at[j],
            recv_sem=pool_recv.at[j],
            device_id=device,
            device_id_type=MESH,
        )

    def rope_copy(j, owner, device):
        return over_sp(ropes.at[owner], rope_send, rope_recv, j - 1, device)

    def gathered(j, owner, device):
        return over_sp(kvp.at[t, rows_of(owner)], gather_send, gather_recv, j - 1, device)

    def passed(j, owner, which):
        return over_sp(kvp.at[which, rows_of(owner)], pass_send, pass_recv, j - 1, mate)

    def relay(ref, sem, first=0, size=depth):
        part = down(ref, through, first, size)
        copy = remote(part, part, sem, {"fs": onward})
        copy.start()
        sends.append(copy)

    def relay_q(chunk):
        if hops:
            for j in range(2):
                take(wq_all, senders[j], b_q(chunk) + j, chunk * chunk_rows, chunk_rows)
            relay(wq_all, b_q(chunk) + 2, chunk * chunk_rows, chunk_rows)

    if hops:
        for j in range(2):
            take(wkv_all, senders[j], b_kv + j)
        relay(wkv_all, b_kv + 2)

    l_pi.wait()
    pool_in = mm(hid[...], wpi[...]).astype(BF16)
    halo_out[0] = pool_in[rows - 2 * RIM :, :].astype(F32)[RIM:, :]
    halo_out[1] = pool_in[: 2 * RIM, :].astype(F32)[:RIM, :]
    c_up = remote(halo_out.at[0], halo_in.at[0], 2, {"sp": (s + 1) % n_sp})
    c_dn = remote(halo_out.at[1], halo_in.at[1], 3, {"sp": (s + n_sp - 1) % n_sp})
    has_prev, has_next = s > 0, s < n_sp - 1
    pl.when(has_next)(c_up.start)
    pl.when(has_prev)(c_dn.start)

    for chunk in range(1, chunks):
        spread_q(chunk)

    l_kr.wait()
    key_pre = mm_t(hid[...], wkr[...])
    key_rope = rotated(jnp.concatenate([key_pre, key_pre], axis=1))
    lower_half = lax.broadcasted_iota(jnp.int32, (half, 128), 1) < ROPE_DIM
    ropes[s] = jnp.where(lower_half, key_rope[:half], key_rope[half:]).astype(BF16)
    for j in range(1, n_sp):
        copy = rope_copy(j, s, {"sp": (s + j) % n_sp})
        copy.start()
        sends.append(copy)

    relay_q(0)
    def no_rim(side):
        def clear():
            halo_in[side] = jnp.zeros(halo_in.shape[1:], F32)

        return clear

    pl.when(has_prev)(c_up.wait_recv)
    pl.when(has_next)(c_dn.wait_recv)
    pl.when(s == 0)(no_rim(0))
    pl.when(s == n_sp - 1)(no_rim(1))
    halo = jnp.concatenate([halo_in[0], halo_in[1]], axis=0).astype(BF16)
    padded = jnp.concatenate([pool_in, halo], axis=0)
    span = rows + 2 * RIM
    k_index = lax.broadcasted_iota(jnp.int32, (rows, span), 1)
    q_index = lax.broadcasted_iota(jnp.int32, (rows, span), 0)
    k_place = jnp.where(
        k_index < rows,
        k_index,
        jnp.where(k_index < rows + RIM, k_index - rows - RIM, k_index - RIM),
    )
    offset = k_place - q_index
    inside = (k_place + s * rows >= 0) & (k_place + s * rows < length)
    l_mix.wait()
    pooled = []
    for g in range(groups):
        group = t * groups + g
        window = jnp.int32(0)
        for index, size in enumerate(WINDOWS):
            window = jnp.where(group == index, size, window)
        before = window // 2
        band = jnp.where(
            inside & (offset >= -before) & (offset < window - before), 1.0, 0.0
        )
        count = jnp.sum(band, axis=1, keepdims=True)
        cols = slice(g * POOL_GROUP, (g + 1) * POOL_GROUP)
        mean = (mm(band.astype(BF16), padded[:, cols]) / count).astype(BF16)
        spread = (mean.astype(F32) - pool_in[:, cols].astype(F32)).astype(BF16)
        pooled.append(mm(spread, mix[g]).astype(BF16))
    l_op.wait()
    acc[...] = mm(jnp.concatenate(pooled, axis=1), wop[...])

    if hops:
        take(wkv_all, across, b_kv + 2)
    else:
        for j, owner in enumerate(senders):
            take(wkv_all, owner, b_kv + j)
    kvp[t, own_rows] = mm(hid[...], wkv_all[...]).astype(BF16)
    for j in range(1, n_sp):
        copy = gathered(j, s, {"sp": (s + j) % n_sp})
        copy.start()
        sends.append(copy)
    c_kvp = remote(kvp.at[t, rows_of(s)], kvp.at[t, rows_of(s)], 4, mate)
    c_kvp.start()
    sends.append(c_kvp)

    relay_q(1)
    relay_q(2)
    relay_q(3)
    shards = (f,) + senders
    last = shards[:1]
    if hops:
        last = (across,)
    else:
        for chunk in range(chunks):
            for j, owner in enumerate(senders):
                take(wq_all, owner, b_q(chunk) + j, chunk * chunk_rows, chunk_rows)
        shards = senders

    def from_shard(owner):
        start = pl.multiple_of(owner * depth, depth)
        return mm(hid[:, pl.ds(start, depth)], wq_all[pl.ds(start, depth), :])

    q_sum = functools.reduce(jnp.add, [from_shard(owner) for owner in shards])
    for j in range(1, n_sp):
        owner = (s + n_sp - j) % n_sp
        gathered(j, owner, mate).wait_recv()
        copy = passed(j, owner, t)
        copy.start()
        sends.append(copy)

    l_kvg.wait()

    def finish_keys(owner):
        here = rows_of(owner)
        kv_pre = jnp.concatenate([kvp[0, here], kvp[1, here]], axis=1).astype(F32)
        kcat[here, :kv_rank] = normed(kv_pre, kvg[...])
        packed = ropes[owner].astype(F32)
        swapped = pltpu.roll(packed, ROPE_DIM, 1)
        low = jnp.where(lower_half, packed, swapped)
        high = jnp.where(lower_half, swapped, packed)
        kcat[here, kv_rank:] = jnp.concatenate([low, high], axis=0).astype(BF16)

    remote(kvp.at[1 - t, rows_of(s)], kvp.at[1 - t, rows_of(s)], 4, mate).wait_recv()
    finish_keys(s)
    for j in range(1, n_sp):
        owner = (s + n_sp - j) % n_sp
        rope_copy(j, owner, mate).wait_recv()
        passed(j, owner, 1 - t).wait_recv()
        finish_keys(owner)

    if hops:
        for chunk in range(chunks):
            take(wq_all, across, b_q(chunk) + 2, chunk * chunk_rows, chunk_rows)
    q_sum = functools.reduce(jnp.add, [from_shard(owner) for owner in last], q_sum)
    qp[t] = q_sum.astype(BF16)
    c_qp = remote(qp.at[t], qp.at[t], 5, mate)
    c_qp.start()
    sends.append(c_qp)

    l_qg.wait()
    remote(qp.at[1 - t], qp.at[1 - t], 5, mate).wait_recv()
    q_latent = normed(jnp.concatenate([qp[0], qp[1]], axis=1).astype(F32), qg[...])
    l_qn.wait()
    q_nope = mm(q_latent, wqn[...]).astype(BF16)
    l_qr.wait()
    q_pre = mm(q_latent, wqr[...])
    l_ku.wait()
    low_lanes = lane < ROPE_DIM
    for h in range(heads):
        cols = slice(h * NOPE_DIM, (h + 1) * NOPE_DIM)
        absorbed = mm_t(q_nope[:, cols], wku[:, cols]).astype(BF16)
        if h % 2 == 0:
            turned = rotated(q_pre[:, h * ROPE_DIM : (h + 2) * ROPE_DIM])
        rope = jnp.where(low_lanes if h % 2 == 0 else ~low_lanes, turned, 0.0).astype(BF16)
        for part in range(2):
            piece = slice(part * half, (part + 1) * half)
            qcat[part, h * half : (h + 1) * half, :kv_rank] = absorbed[piece]
            qcat[part, h * half : (h + 1) * half, kv_rank:] = rope[piece]

    factor = (NOPE_DIM + ROPE_DIM) ** (-0.5) * math.log2(math.e)
    span_keys = rows * max(
        c for c in range(1, n_sp + 1) if n_sp % c == 0 and (c == 1 or rows * c <= SPAN_LIMIT)
    )
    spans = length // span_keys
    block = 4 * half

    def attend(part):
        def one_block(b, carry):
            block_rows = pl.ds(pl.multiple_of(b * block, block), block)
            queries = qcat[part, block_rows, :]

            def absorb(keys, state):
                scores = mm_t(queries, keys)
                top = jnp.max(scores, axis=1, keepdims=True)
                if state is not None:
                    top = jnp.maximum(top, state[0])
                weights = jnp.exp2((scores - top) * factor)
                total = jnp.sum(weights, axis=1, keepdims=True)
                summed = mm(weights.astype(BF16), keys[:, :kv_rank])
                if state is not None:
                    shrink = jnp.exp2((state[0] - top) * factor)
                    total = total + state[1] * shrink
                    summed = summed + state[2] * shrink
                return top, total, summed

            if spans == 1:
                state = absorb(kcat[...], None)
            else:
                state = absorb(kcat[:span_keys, :], None)

                def step(i, now):
                    start = pl.multiple_of(i * span_keys, span_keys)
                    return absorb(kcat[pl.ds(start, span_keys), :], now)

                state = lax.fori_loop(1, spans, step, state)
            ctx[block_rows, :] = (state[2] / state[1]).astype(BF16)
            return carry

        lax.fori_loop(0, heads * half // block, one_block, 0, unroll=True)
        for h in range(heads):
            cols = slice(h * VALUE_DIM, (h + 1) * VALUE_DIM)
            att[:, cols] = mm(ctx[h * half : (h + 1) * half, :], wvu[:, cols]).astype(BF16)
        own = acc[pl.ds(pl.multiple_of(part * half, half), half), :]
        return own + mm(att[...], woa[...])

    l_vu.wait()
    l_oa.wait()
    share[...] = attend(1 - t).astype(BF16)
    c_share = remote(share, arrived, 6, mate)
    c_share.start()
    sends.append(c_share)
    mine = attend(t)
    c_share.wait_recv()
    out[0] = (mine + arrived[...].astype(F32)).astype(BF16)
    pl.when(has_next)(c_up.wait_send)
    pl.when(has_prev)(c_dn.wait_send)
    for copy in sends:
        copy.wait_send()


def solution(mesh):
    n_sp, n_fs = mesh.shape["sp"], mesh.shape["fs"]

    def on_device(*args):
        args = list(args)
        args[1] = args[1].reshape(-1, 128)
        for i in (3, 7):
            args[i] = args[i].reshape(1, -1)
        args[10] = args[10].T
        (tokens, gain, wqd, qg, wqn, wqr, wkvd, kvg, wku, wvu, wkr, wpi, mix, woa, wop) = args
        rows, cols = tokens.shape[1:]
        half = rows // 2
        heads = wqn.shape[1] // NOPE_DIM
        kv_rank = wkvd.shape[1]
        q_rank = wqd.shape[1]
        d_model = woa.shape[1]
        groups = wpi.shape[1] // POOL_GROUP
        n_sems = 8 + 5 * (n_fs - 1)

        def vmem(*shape, kind=BF16):
            return pltpu.VMEM(shape, kind)

        def same(array):
            return pltpu.VMEM(array.shape, array.dtype)

        dma = pltpu.SemaphoreType.DMA
        return pl.pallas_call(
            functools.partial(layer, n_sp, n_fs),
            out_shape=pltpu.VMEM((1, half, d_model), BF16),
            in_specs=[pl.BlockSpec(memory_space=pltpu.HBM)] * len(args),
            out_specs=pl.BlockSpec(memory_space=pltpu.VMEM),
            scratch_shapes=[
                vmem(2, rows, cols),
                vmem(2, cols // 128, 128),
                vmem(rows, 2 * cols),
                vmem(n_fs * wqd.shape[0], q_rank // 2),
                vmem(n_fs * wkvd.shape[0], kv_rank // 2),
                same(qg),
                same(kvg),
                same(wqn),
                same(wqr),
                same(wku),
                same(wvu),
                same(wkr),
                same(wpi),
                vmem(groups, POOL_GROUP, POOL_GROUP),
                same(woa),
                same(wop),
                vmem(2, RIM, wpi.shape[1], kind=F32),
                vmem(2, RIM, wpi.shape[1], kind=F32),
                vmem(2, n_sp * rows, kv_rank // 2),
                vmem(2, rows, q_rank // 2),
                vmem(n_sp, half, 2 * ROPE_DIM),
                vmem(n_sp * rows, kv_rank + 2 * ROPE_DIM),
                vmem(2, heads * half, kv_rank + 2 * ROPE_DIM),
                vmem(heads * half, kv_rank),
                vmem(half, heads * VALUE_DIM),
                vmem(rows, d_model, kind=F32),
                vmem(half, d_model),
                vmem(half, d_model),
                dma((16,)),
                dma((n_sems,)),
                dma((n_sems,)),
                dma((n_sp - 1,)),
                dma((n_sp - 1,)),
                dma((n_sp - 1,)),
                dma((n_sp - 1,)),
                dma((n_sp - 1,)),
                dma((n_sp - 1,)),
            ],
            compiler_params=pltpu.CompilerParams(collective_id=0, has_side_effects=True, vmem_limit_bytes=40 * 1024 * 1024),
        )(*[pltpu.with_memory_space_constraint(a, pltpu.HBM) for a in args])

    placed = (
        P("fs", "sp", "tp"),
        P("tp"),
        P("fs", None),
        P(),
        P(None, "tp"),
        P(None, "tp"),
        P("fs", None),
        P(),
        P(None, "tp"),
        P(None, "tp"),
        P(),
        P(None, "tp"),
        P(),
        P("tp", None),
        P("tp", None),
    )
    return jax.shard_map(
        on_device,
        mesh=mesh,
        in_specs=placed,
        out_specs=P("fs", ("sp", "tp"), None),
        check_vma=False,
    )
```

```python
import functools
import math

import jax
import jax.numpy as jnp
from jax import lax
from jax.experimental import pallas as pl
from jax.experimental.pallas import tpu as pltpu
from jax.sharding import PartitionSpec as P

NOPE_DIM = 128
ROPE_DIM = 64
VALUE_DIM = 128
GRID_W = 64
POOL_GROUP = 256
EPS = 1e-06
THETA = 10000.0
WINDOWS = (2, 4, 8, 16)
RIM = 8
SPAN_LIMIT = 1024
F32 = jnp.float32
BF16 = jnp.bfloat16
MESH = pl.DeviceIdType.MESH
USE_Z = False


def mm(a, b):
    return jnp.dot(a, b, preferred_element_type=F32)


def mm_t(a, b):
    return lax.dot_general(a, b, (((1,), (1,)), ((), ())), preferred_element_type=F32)


def normed(wide, gain):
    scale = lax.rsqrt(jnp.mean(wide * wide, axis=-1, keepdims=True) + EPS)
    return (wide * scale * gain).astype(BF16)


def layer(
    n_sp,
    n_fs,
    tokens,
    norm_gain,
    w_q_down,
    q_gain,
    w_q_nope,
    w_q_rope,
    w_kv_down,
    kv_gain,
    w_k_up,
    w_v_up,
    w_k_rope,
    w_pool_in,
    w_pool_mix,
    w_out_attn,
    w_out_pool,
    out,
    tok,
    gain,
    hid,
    wq_all,
    wkv_all,
    qg,
    kvg,
    wqn,
    wqr,
    wku,
    wvu,
    wkr,
    wpi,
    mix,
    woa,
    wop,
    halo_out,
    halo_in,
    q_part,
    q_lat,
    kv_lat,
    ropes,
    kcat,
    qcat,
    ctx,
    att,
    acc,
    share,
    arrived,
    local_sem,
    send_sem,
    recv_sem,
    gather_send,
    gather_recv,
    pass_send,
    pass_recv,
    rope_send,
    rope_recv,
    word,
):
    s = lax.axis_index("sp")
    f = lax.axis_index("fs")
    t = lax.axis_index("tp")
    rows = tok.shape[1]
    half = rows // 2
    depth = w_q_down.shape[0]
    kv_rank = wkv_all.shape[1]
    kv_core, q_core = t == 1, t == 0
    heads = wqn.shape[1] // NOPE_DIM
    groups = wpi.shape[1] // POOL_GROUP
    length = rows * n_sp

    def down(ref, owner, first=0, size=depth):
        start = pl.multiple_of(owner * depth + first, 16)
        return ref.at[pl.ds(start, size), :]

    pairs = (
        (w_kv_down, down(wkv_all, f)),
        (tokens.at[0], tok.at[t]),
        (norm_gain, gain.at[t]),
        (w_q_down, down(wq_all, f)),
        (w_k_rope, wkr),
        (w_pool_in, wpi),
        (kv_gain, kvg),
        (q_gain, qg),
        (w_pool_mix.at[pl.ds(t * groups, groups)], mix),
        (w_out_pool, wop),
        (w_q_nope, wqn),
        (w_q_rope, wqr),
        (w_k_up, wku),
        (w_v_up, wvu),
        (w_out_attn, woa),
    )
    loads = [
        pltpu.make_async_copy(src, dst, local_sem.at[i]) for i, (src, dst) in enumerate(pairs)
    ]
    (
        l_kv,
        l_tok,
        l_gain,
        l_q,
        l_kr,
        l_pi,
        l_kvg,
        l_qg,
        l_mix,
        l_op,
        l_qn,
        l_qr,
        l_ku,
        l_vu,
        l_oa,
    ) = loads
    for load in loads:
        if load is l_kv:
            pl.when(kv_core)(load.start)
        elif load is l_q:
            pl.when(q_core)(load.start)
        else:
            load.start()

    barrier = pltpu.get_barrier_semaphore()

    def greet(device):
        pl.semaphore_signal(barrier, inc=1, device_id=device, device_id_type=MESH)

    hops = n_fs == 4
    line = hops and n_sp == 4
    has_prev, has_next = s > 0, s < n_sp - 1
    mate = {"tp": 1 - t}
    above, below = {"sp": (s + 1) % n_sp}, {"sp": (s + n_sp - 1) % n_sp}
    parity = s % 2
    if hops:
        near = f + 1 - 2 * (f % 2)
        far = (f + 2) % 4
        across = 3 - f
    greet(mate)
    if line:
        greet({"fs": near})
        greet({"fs": far})
        pl.when(has_next)(lambda: greet(above))
        pl.when(has_prev)(lambda: greet(below))
        guests = 5 - (s == 0).astype(jnp.int32) - (s == n_sp - 1).astype(jnp.int32)
    else:
        for j in range(1, n_fs):
            greet({"fs": (f + j) % n_fs})
        for j in range(1, n_sp):
            greet({"sp": (s + j) % n_sp})
        guests = n_sp + n_fs - 1
    pl.semaphore_wait(barrier, guests)

    def tell(side, device):
        pl.semaphore_signal(word.at[side], inc=1, device_id=device, device_id_type=MESH)

    def hear(side, count):
        return lambda: pl.semaphore_wait(word.at[side], count)

    if line:

        def both_ways():
            tell(0, above)
            tell(1, below)

        pl.when(has_prev & has_next)(both_ways)

    def spread_word():
        def up():
            hear(0, 1)()
            tell(0, above)

        def down_():
            hear(1, 1)()
            tell(1, below)

        pl.when(s == n_sp - 2)(up)
        pl.when(s == 1)(down_)

    def hear_word():
        pl.when(s == n_sp - 1)(hear(0, 2))
        pl.when(s == 0)(hear(1, 2))

    def remote(src, dst, sem, device):
        return pltpu.make_async_remote_copy(
            src_ref=src,
            dst_ref=dst,
            send_sem=send_sem.at[sem],
            recv_sem=recv_sem.at[sem],
            device_id=device,
            device_id_type=MESH,
        )

    chunks = 4
    chunk_rows = depth // chunks
    sends, kv_sends, q_sends = [], [], []
    over_z = hops and n_sp % 2 == 0 and USE_Z
    if hops:
        partners = senders = (near, far)
    else:
        partners = tuple((f + j) % n_fs for j in range(1, n_fs))
        senders = tuple((f + n_fs - j) % n_fs for j in range(1, n_fs))
    width = max(n_fs - 1, 4)
    b_kv = 8
    b_z = 8 + (1 + chunks) * width

    def b_q(turn):
        return 8 + (1 + turn) * width

    def piece_at(turn):
        if over_z:
            return ((3 - parity), 0, 1, (2 + parity))[turn] * chunk_rows
        return turn * chunk_rows

    turns = range(chunks - 1) if over_z else range(chunks)

    def outgoing(ref, base, first, size):
        part = down(ref, f, first, size)
        return [remote(part, part, base + j, {"fs": peer}) for j, peer in enumerate(partners)]

    def incoming(ref, base, first, size):
        return [
            remote(part, part, base + j, mate)
            for j, part in enumerate(down(ref, owner, first, size) for owner in senders)
        ]

    def onward(ref, base, first, size):
        piece = size // 2
        low, high = down(ref, near, first, piece), down(ref, far, first + piece, piece)
        return [remote(low, low, base + 2, {"fs": far}), remote(high, high, base + 3, {"fs": near})]

    def across_in(ref, base, first, size):
        piece = size // 2
        parts = (down(ref, across, first, piece), down(ref, across, first + piece, piece))
        return [remote(part, part, base + 2 + j, mate) for j, part in enumerate(parts)]

    def start(copies, pool):
        for copy in copies:
            copy.start()
        pool += copies

    def arrive(copies):
        for copy in copies:
            copy.wait_recv()

    kv_out = outgoing(wkv_all, b_kv, 0, depth)
    kv_in = incoming(wkv_all, b_kv, 0, depth)
    q_out = [outgoing(wq_all, b_q(turn), piece_at(turn), chunk_rows) for turn in turns]
    q_in = [incoming(wq_all, b_q(turn), piece_at(turn), chunk_rows) for turn in turns]
    if hops:
        kv_on = onward(wkv_all, b_kv, 0, depth)
        kv_across = across_in(wkv_all, b_kv, 0, depth)
        q_on = [onward(wq_all, b_q(turn), piece_at(turn), chunk_rows) for turn in turns]
        q_across = [across_in(wq_all, b_q(turn), piece_at(turn), chunk_rows) for turn in turns]
    else:
        kv_on, kv_across = [], []
        q_on = q_across = [[] for turn in turns]
    if over_z:
        over = {"sp": s + 1 - 2 * parity}
        z_owners = (near, far, across)

        def z_pieces(turn):
            parts = [down(wq_all, owner, piece_at(turn), chunk_rows) for owner in z_owners]
            return [remote(part, part, b_z + j, over) for j, part in enumerate(parts)]

        z_out, z_in = z_pieces(0), z_pieces(chunks - 1)

    @pl.when(kv_core)
    def _():
        l_kv.wait()
        start(kv_out, kv_sends)

    l_tok.wait()
    c_tok = remote(tok.at[t], tok.at[t], 0, mate)
    c_tok.start()
    l_gain.wait()
    c_gain = remote(gain.at[t], gain.at[t], 1, mate)
    c_gain.start()
    sends += [c_tok, c_gain]
    lane = lax.broadcasted_iota(jnp.int32, (rows, 128), 1)
    place = s * rows + lax.broadcasted_iota(jnp.int32, (rows, 128), 0)
    quarter = ROPE_DIM // 4
    power = (lane % quarter).astype(F32) * (2.0 / (ROPE_DIM // 2))
    inverse = jnp.exp(power * (-math.log(THETA)))
    grid_row = place // GRID_W
    grid_col = place - grid_row * GRID_W
    in_a = (lane % ROPE_DIM) < (ROPE_DIM // 2)
    angle = jnp.where(in_a, grid_row, grid_col).astype(F32) * inverse
    is_u = (lane % (2 * quarter)) < quarter
    cosine = jnp.cos(angle)
    sine = jnp.where(is_u, -jnp.sin(angle), jnp.sin(angle))

    def rotated(pre):
        wide = pre.astype(BF16).astype(F32)
        swapped = jnp.where(is_u, pltpu.roll(wide, 128 - quarter, 1), pltpu.roll(wide, quarter, 1))
        return wide * cosine + swapped * sine

    if line:
        spread_word()
    remote(gain.at[1 - t], gain.at[1 - t], 1, mate).wait_recv()
    remote(tok.at[1 - t], tok.at[1 - t], 0, mate).wait_recv()
    whole = jnp.concatenate([tok[0], tok[1]], axis=1).astype(F32)
    lines = gain.shape[1]
    wide_gain = [gain[0].astype(F32), gain[1].astype(F32)]
    flat_gain = jnp.concatenate(
        [side[i : i + 1, :] for side in wide_gain for i in range(lines)], axis=1
    )
    hid[...] = normed(whole, flat_gain)

    own_rows = pl.ds(pl.multiple_of(s * rows, rows), rows)

    def rows_of(owner):
        return pl.ds(pl.multiple_of(owner * rows, rows), rows)

    if n_sp == 4:
        peers_to = (s + 1 - 2 * parity, (s + 2) % 4, 3 - s)
        peers_from = peers_to
    else:
        peers_to = tuple((s + j) % n_sp for j in range(1, n_sp))
        peers_from = tuple((s + n_sp - j) % n_sp for j in range(1, n_sp))

    def over_sp(ref, pool_send, pool_recv, j, device):
        return pltpu.make_async_remote_copy(
            src_ref=ref,
            dst_ref=ref,
            send_sem=pool_send.at[j],
            recv_sem=pool_recv.at[j],
            device_id=device,
            device_id_type=MESH,
        )

    def rope_copy(j, owner, device):
        return over_sp(ropes.at[owner], rope_send, rope_recv, j, device)

    def latent(owner):
        return kv_lat.at[rows_of(owner)]

    c_own = remote(latent(s), latent(s), 4, mate)
    gather_out = [
        over_sp(latent(s), gather_send, gather_recv, j, {"sp": peer})
        for j, peer in enumerate(peers_to)
    ]
    gather_in = [
        over_sp(latent(owner), gather_send, gather_recv, j, mate)
        for j, owner in enumerate(peers_from)
    ]
    passed = [
        over_sp(latent(owner), pass_send, pass_recv, j, mate)
        for j, owner in enumerate(peers_from)
    ]

    l_pi.wait()
    pool_in = mm(hid[...], wpi[...]).astype(BF16)
    halo_out[0] = pool_in[rows - 2 * RIM :, :].astype(F32)[RIM:, :]
    halo_out[1] = pool_in[: 2 * RIM, :].astype(F32)[:RIM, :]
    c_up = remote(halo_out.at[0], halo_in.at[0], 2, above)
    c_dn = remote(halo_out.at[1], halo_in.at[1], 3, below)
    pl.when(has_next)(c_up.start)
    pl.when(has_prev)(c_dn.start)

    @pl.when(q_core)
    def _():
        l_q.wait()
        for copies in q_out:
            start(copies, q_sends)


    l_kr.wait()
    key_pre = mm_t(hid[...], wkr[...])
    key_rope = rotated(jnp.concatenate([key_pre, key_pre], axis=1))
    lower_half = lax.broadcasted_iota(jnp.int32, (half, 128), 1) < ROPE_DIM
    ropes[s] = jnp.where(lower_half, key_rope[:half], key_rope[half:]).astype(BF16)
    if line:
        hear_word()
    for j, peer in enumerate(peers_to):
        copy = rope_copy(j, s, {"sp": peer})
        copy.start()
        sends.append(copy)

    @pl.when(kv_core)
    def _():
        arrive(kv_in)
        start(kv_on, kv_sends)

    def no_rim(side):
        def clear():
            halo_in[side] = jnp.zeros(halo_in.shape[1:], F32)

        return clear

    pl.when(has_prev)(c_up.wait_recv)
    pl.when(has_next)(c_dn.wait_recv)
    pl.when(s == 0)(no_rim(0))
    pl.when(s == n_sp - 1)(no_rim(1))
    halo = jnp.concatenate([halo_in[0], halo_in[1]], axis=0).astype(BF16)
    padded = jnp.concatenate([pool_in, halo], axis=0)
    span = rows + 2 * RIM
    k_index = lax.broadcasted_iota(jnp.int32, (rows, span), 1)
    q_index = lax.broadcasted_iota(jnp.int32, (rows, span), 0)
    k_place = jnp.where(
        k_index < rows,
        k_index,
        jnp.where(k_index < rows + RIM, k_index - rows - RIM, k_index - RIM),
    )
    offset = k_place - q_index
    inside = (k_place + s * rows >= 0) & (k_place + s * rows < length)
    l_mix.wait()
    pooled = []
    for g in range(groups):
        group = t * groups + g
        window = jnp.int32(0)
        for index, size in enumerate(WINDOWS):
            window = jnp.where(group == index, size, window)
        before = window // 2
        band = jnp.where(
            inside & (offset >= -before) & (offset < window - before), 1.0, 0.0
        )
        count = jnp.sum(band, axis=1, keepdims=True)
        cols = slice(g * POOL_GROUP, (g + 1) * POOL_GROUP)
        mean = (mm(band.astype(BF16), padded[:, cols]) / count).astype(BF16)
        spread = (mean.astype(F32) - pool_in[:, cols].astype(F32)).astype(BF16)
        pooled.append(mm(spread, mix[g]).astype(BF16))
    l_op.wait()
    acc[...] = mm(jnp.concatenate(pooled, axis=1), wop[...])

    l_kvg.wait()
    l_qg.wait()

    @pl.when(kv_core)
    def _():
        arrive(kv_across)
        pre = mm(hid[...], wkv_all[...]).astype(BF16).astype(F32)
        kv_lat[own_rows] = normed(pre, kvg[...])
        start(gather_out + [c_own], kv_sends)

    @pl.when(q_core)
    def _():
        for turn in turns:
            arrive(q_in[turn])
            start(q_on[turn], q_sends)
            if over_z and turn == 0:
                start(z_out[:2], q_sends)
            if over_z and turn == 1:
                arrive(q_across[0])
                start(z_out[2:], q_sends)

    def finish_rope(owner):
        here = rows_of(owner)
        packed = ropes[owner].astype(F32)
        swapped = pltpu.roll(packed, ROPE_DIM, 1)
        low = jnp.where(lower_half, packed, swapped)
        high = jnp.where(lower_half, swapped, packed)
        kcat[here, kv_rank:] = jnp.concatenate([low, high], axis=0).astype(BF16)

    finish_rope(s)
    for j, owner in enumerate(peers_from):
        rope_copy(j, owner, mate).wait_recv()
        finish_rope(owner)

    c_lat = remote(q_lat, q_lat, 5, mate)

    def from_shard(owner):
        first = pl.multiple_of(owner * depth, depth)
        return mm(hid[:, pl.ds(first, depth)], wq_all[pl.ds(first, depth), :])

    @pl.when(kv_core)
    def _():
        for j in range(n_sp - 1):
            gather_in[j].wait_recv()
            start([passed[j]], kv_sends)
        c_lat.wait_recv()

    @pl.when(q_core)
    def _():
        if over_z:
            arrive(z_in[:2])
        q_part[...] = functools.reduce(jnp.add, [from_shard(owner) for owner in (f,) + senders])
        for turn in turns:
            if not (over_z and turn == 0):
                arrive(q_across[turn])
        if over_z:
            arrive(z_in[2:])
        q_sum = q_part[...]
        if hops:
            q_sum = q_sum + from_shard(across)
        q_lat[...] = normed(q_sum.astype(BF16).astype(F32), qg[...])
        start([c_lat], q_sends)

    q_latent = q_lat[...]
    l_qn.wait()
    q_nope = mm(q_latent, wqn[...]).astype(BF16)
    l_qr.wait()
    q_pre = mm(q_latent, wqr[...])
    l_ku.wait()
    low_lanes = lane < ROPE_DIM
    for h in range(heads):
        cols = slice(h * NOPE_DIM, (h + 1) * NOPE_DIM)
        absorbed = mm_t(q_nope[:, cols], wku[:, cols]).astype(BF16)
        if h % 2 == 0:
            turned = rotated(q_pre[:, h * ROPE_DIM : (h + 2) * ROPE_DIM])
        rope = jnp.where(low_lanes if h % 2 == 0 else ~low_lanes, turned, 0.0).astype(BF16)
        for part in range(2):
            piece = slice(part * half, (part + 1) * half)
            qcat[part, h * half : (h + 1) * half, :kv_rank] = absorbed[piece]
            qcat[part, h * half : (h + 1) * half, kv_rank:] = rope[piece]

    factor = (NOPE_DIM + ROPE_DIM) ** (-0.5) * math.log2(math.e)
    span_keys = rows * max(
        c for c in range(1, n_sp + 1) if n_sp % c == 0 and (c == 1 or rows * c <= SPAN_LIMIT)
    )
    spans = length // span_keys
    block = 4 * half

    def attend(part):
        def one_block(b, carry):
            block_rows = pl.ds(pl.multiple_of(b * block, block), block)
            queries = qcat[part, block_rows, :]

            def absorb(keys, state):
                scores = mm_t(queries, keys)
                top = jnp.max(scores, axis=1, keepdims=True)
                if state is not None:
                    top = jnp.maximum(top, state[0])
                weights = jnp.exp2((scores - top) * factor)
                total = jnp.sum(weights, axis=1, keepdims=True)
                summed = mm(weights.astype(BF16), keys[:, :kv_rank])
                if state is not None:
                    shrink = jnp.exp2((state[0] - top) * factor)
                    total = total + state[1] * shrink
                    summed = summed + state[2] * shrink
                return top, total, summed

            if spans == 1:
                state = absorb(kcat[...], None)
            else:
                state = absorb(kcat[:span_keys, :], None)

                def step(i, now):
                    start = pl.multiple_of(i * span_keys, span_keys)
                    return absorb(kcat[pl.ds(start, span_keys), :], now)

                state = lax.fori_loop(1, spans, step, state)
            ctx[block_rows, :] = (state[2] / state[1]).astype(BF16)
            return carry

        lax.fori_loop(0, heads * half // block, one_block, 0, unroll=True)
        for h in range(heads):
            cols = slice(h * VALUE_DIM, (h + 1) * VALUE_DIM)
            att[:, cols] = mm(ctx[h * half : (h + 1) * half, :], wvu[:, cols]).astype(BF16)
        own = acc[pl.ds(pl.multiple_of(part * half, half), half), :]
        return own + mm(att[...], woa[...])

    l_vu.wait()
    l_oa.wait()

    @pl.when(q_core)
    def _():
        c_own.wait_recv()
        arrive(passed)

    kcat[:, :kv_rank] = kv_lat[...]
    share[...] = attend(1 - t).astype(BF16)
    c_share = remote(share, arrived, 6, mate)
    c_share.start()
    sends.append(c_share)
    mine = attend(t)
    c_share.wait_recv()
    out[0] = (mine + arrived[...].astype(F32)).astype(BF16)
    pl.when(has_next)(c_up.wait_send)
    pl.when(has_prev)(c_dn.wait_send)
    for copy in sends:
        copy.wait_send()

    @pl.when(kv_core)
    def _():
        for copy in kv_sends:
            copy.wait_send()

    @pl.when(q_core)
    def _():
        for copy in q_sends:
            copy.wait_send()


def solution(mesh):
    n_sp, n_fs = mesh.shape["sp"], mesh.shape["fs"]

    def on_device(*args):
        args = list(args)
        args[1] = args[1].reshape(-1, 128)
        for i in (3, 7):
            args[i] = args[i].reshape(1, -1)
        args[10] = args[10].T
        (tokens, gain, wqd, qg, wqn, wqr, wkvd, kvg, wku, wvu, wkr, wpi, mix, woa, wop) = args
        rows, cols = tokens.shape[1:]
        half = rows // 2
        heads = wqn.shape[1] // NOPE_DIM
        kv_rank = wkvd.shape[1]
        q_rank = wqd.shape[1]
        d_model = woa.shape[1]
        groups = wpi.shape[1] // POOL_GROUP
        n_sems = 8 + 5 * max(n_fs - 1, 4) + 3

        def vmem(*shape, kind=BF16):
            return pltpu.VMEM(shape, kind)

        def same(array):
            return pltpu.VMEM(array.shape, array.dtype)

        dma = pltpu.SemaphoreType.DMA
        return pl.pallas_call(
            functools.partial(layer, n_sp, n_fs),
            out_shape=pltpu.VMEM((1, half, d_model), BF16),
            in_specs=[pl.BlockSpec(memory_space=pltpu.HBM)] * len(args),
            out_specs=pl.BlockSpec(memory_space=pltpu.VMEM),
            scratch_shapes=[
                vmem(2, rows, cols),
                vmem(2, cols // 128, 128),
                vmem(rows, 2 * cols),
                vmem(n_fs * wqd.shape[0], q_rank),
                vmem(n_fs * wkvd.shape[0], kv_rank),
                same(qg),
                same(kvg),
                same(wqn),
                same(wqr),
                same(wku),
                same(wvu),
                same(wkr),
                same(wpi),
                vmem(groups, POOL_GROUP, POOL_GROUP),
                same(woa),
                same(wop),
                vmem(2, RIM, wpi.shape[1], kind=F32),
                vmem(2, RIM, wpi.shape[1], kind=F32),
                vmem(rows, q_rank, kind=F32),
                vmem(rows, q_rank),
                vmem(n_sp * rows, kv_rank),
                vmem(n_sp, half, 2 * ROPE_DIM),
                vmem(n_sp * rows, kv_rank + 2 * ROPE_DIM),
                vmem(2, heads * half, kv_rank + 2 * ROPE_DIM),
                vmem(heads * half, kv_rank),
                vmem(half, heads * VALUE_DIM),
                vmem(rows, d_model, kind=F32),
                vmem(half, d_model),
                vmem(half, d_model),
                dma((16,)),
                dma((n_sems,)),
                dma((n_sems,)),
                dma((n_sp - 1,)),
                dma((n_sp - 1,)),
                dma((n_sp - 1,)),
                dma((n_sp - 1,)),
                dma((n_sp - 1,)),
                dma((n_sp - 1,)),
                pltpu.SemaphoreType.REGULAR((2,)),
            ],
            compiler_params=pltpu.CompilerParams(collective_id=0, has_side_effects=True, vmem_limit_bytes=40 * 1024 * 1024),
        )(*[pltpu.with_memory_space_constraint(a, pltpu.HBM) for a in args])

    placed = (
        P("fs", "sp", "tp"),
        P("tp"),
        P("fs", None),
        P(),
        P(None, "tp"),
        P(None, "tp"),
        P("fs", None),
        P(),
        P(None, "tp"),
        P(None, "tp"),
        P(),
        P(None, "tp"),
        P(),
        P("tp", None),
        P("tp", None),
    )
    return jax.shard_map(
        on_device,
        mesh=mesh,
        in_specs=placed,
        out_specs=P("fs", ("sp", "tp"), None),
        check_vma=False,
    )
```

```python
import functools
import math

import jax
import jax.numpy as jnp
from jax import lax
from jax.experimental import pallas as pl
from jax.experimental.pallas import tpu as pltpu
from jax.sharding import PartitionSpec as P

NOPE_DIM = 128
ROPE_DIM = 64
VALUE_DIM = 128
GRID_W = 64
POOL_GROUP = 256
EPS = 1e-06
THETA = 10000.0
WINDOWS = (2, 4, 8, 16)
RIM = 8
SPAN_LIMIT = 1024
F32 = jnp.float32
BF16 = jnp.bfloat16
MESH = pl.DeviceIdType.MESH
TOK, GAIN, UP, DOWN, LATENT, SHARE, ROPE, STAGE = range(8)
MAIN, GATHER, PASS, BLOCK, SIDE_A, SIDE_B = range(6)


def mm(a, b):
    return jnp.dot(a, b, preferred_element_type=F32)


def mm_t(a, b):
    return lax.dot_general(a, b, (((1,), (1,)), ((), ())), preferred_element_type=F32)


def normed(wide, gain):
    scale = lax.rsqrt(jnp.mean(wide * wide, axis=-1, keepdims=True) + EPS)
    return (wide * scale * gain).astype(BF16)


def layer(
    n_sp,
    n_fs,
    tokens,
    norm_gain,
    w_q_down,
    q_gain,
    w_q_nope,
    w_q_rope,
    w_kv_down,
    kv_gain,
    w_k_up,
    w_v_up,
    w_k_rope,
    w_pool_in,
    w_pool_mix,
    w_out_attn,
    w_out_pool,
    out,
    tok,
    gain,
    hid,
    wq_all,
    wkv_all,
    qg,
    kvg,
    wqn,
    wqr,
    wku,
    wvu,
    wkr,
    wpi,
    mix,
    woa,
    wop,
    halo_out,
    halo_in,
    q_part,
    q_lat,
    kv_lat,
    ropes,
    kcat,
    qcat,
    ctx,
    att,
    acc,
    share,
    arrived,
    local_sem,
    send_sem,
    recv_sem,
    word,
):
    s = lax.axis_index("sp")
    f = lax.axis_index("fs")
    t = lax.axis_index("tp")
    rows = tok.shape[1]
    half = rows // 2
    depth = w_q_down.shape[0]
    kv_rank = wkv_all.shape[1]
    kv_core, q_core = t == 1, t == 0
    heads = wqn.shape[1] // NOPE_DIM
    groups = wpi.shape[1] // POOL_GROUP
    length = rows * n_sp

    def down(ref, owner, first=0, size=depth):
        start = pl.multiple_of(owner * depth + first, 16)
        return ref.at[pl.ds(start, size), :]

    pairs = (
        (w_kv_down, down(wkv_all, f)),
        (tokens.at[0], tok.at[t]),
        (norm_gain, gain.at[t]),
        (w_q_down, down(wq_all, f)),
        (w_k_rope, wkr),
        (w_pool_in, wpi),
        (kv_gain, kvg),
        (q_gain, qg),
        (w_pool_mix.at[pl.ds(t * groups, groups)], mix),
        (w_out_pool, wop),
        (w_q_nope, wqn),
        (w_q_rope, wqr),
        (w_k_up, wku),
        (w_v_up, wvu),
        (w_out_attn, woa),
    )
    slots = (0, 1, 2, 0, 3, 3, 4, 5, 6, 6, 7, 7, 7, 7, 8)
    loads = [
        pltpu.make_async_copy(src, dst, local_sem.at[slot])
        for slot, (src, dst) in zip(slots, pairs)
    ]
    (
        l_kv,
        l_tok,
        l_gain,
        l_q,
        l_kr,
        l_pi,
        l_kvg,
        l_qg,
        l_mix,
        l_op,
        l_qn,
        l_qr,
        l_ku,
        l_vu,
        l_oa,
    ) = loads
    for load in loads:
        if load is l_kv:
            pl.when(kv_core)(load.start)
        elif load is l_q:
            pl.when(q_core)(load.start)
        else:
            load.start()

    barrier = pltpu.get_barrier_semaphore()

    def greet(device):
        pl.semaphore_signal(barrier, inc=1, device_id=device, device_id_type=MESH)

    hops = n_fs == 4
    line = hops and n_sp == 4
    has_prev, has_next = s > 0, s < n_sp - 1
    mate = {"tp": 1 - t}
    above, below = {"sp": (s + 1) % n_sp}, {"sp": (s + n_sp - 1) % n_sp}
    parity = s % 2
    if hops:
        near = f + 1 - 2 * (f % 2)
        far = (f + 2) % 4
        across = 3 - f
    greet(mate)
    if line:
        greet({"fs": near})
        greet({"fs": far})
        pl.when(has_next)(lambda: greet(above))
        pl.when(has_prev)(lambda: greet(below))
        guests = 5 - (s == 0).astype(jnp.int32) - (s == n_sp - 1).astype(jnp.int32)
    else:
        for j in range(1, n_fs):
            greet({"fs": (f + j) % n_fs})
        for j in range(1, n_sp):
            greet({"sp": (s + j) % n_sp})
        guests = n_sp + n_fs - 1
    pl.semaphore_wait(barrier, guests)

    def tell(side, device):
        pl.semaphore_signal(word.at[side], inc=1, device_id=device, device_id_type=MESH)

    def hear(side, count):
        return lambda: pl.semaphore_wait(word.at[side], count)

    if line:

        def both_ways():
            tell(0, above)
            tell(1, below)

        pl.when(has_prev & has_next)(both_ways)

    def spread_word():
        def up():
            hear(0, 1)()
            tell(0, above)

        def down_():
            hear(1, 1)()
            tell(1, below)

        pl.when(s == n_sp - 2)(up)
        pl.when(s == 1)(down_)

    def hear_word():
        pl.when(s == n_sp - 1)(hear(0, 2))
        pl.when(s == 0)(hear(1, 2))

    def remote(src, dst, sent, slot, device):
        return pltpu.make_async_remote_copy(
            src_ref=src,
            dst_ref=dst,
            send_sem=send_sem.at[sent],
            recv_sem=recv_sem.at[slot],
            device_id=device,
            device_id_type=MESH,
        )

    def part_of(ref, count):
        return ref.at[pl.ds(0, count)]

    def all_sent(ref, count, sent):
        part = part_of(ref, count)
        remote(part, part, sent, TOK, mate).wait_send()

    def all_taken(ref, count, slot):
        part = part_of(ref, count)
        remote(part, part, MAIN, slot, mate).wait_recv()

    def all_loaded(*refs):
        slot = {id(ref): i for ref, i in zip((dst for _, dst in pairs), slots)}[id(refs[0])]
        line_bytes = 2 * woa.shape[1]
        total = sum(math.prod(ref.shape) * ref.dtype.itemsize for ref in refs)
        part = part_of(woa, total // line_bytes)
        pltpu.make_async_copy(part, part, local_sem.at[slot]).wait()

    chunks = 4
    chunk_rows = depth // chunks
    if hops:
        partners = senders = (near, far)
    else:
        partners = tuple((f + j) % n_fs for j in range(1, n_fs))
        senders = tuple((f + n_fs - j) % n_fs for j in range(1, n_fs))
    def piece_at(turn):
        return turn * chunk_rows

    turns = range(chunks)

    def outgoing(ref, slot, first, size):
        part = down(ref, f, first, size)
        return [remote(part, part, MAIN, slot, {"fs": peer}) for peer in partners]

    def onward(ref, slot, first, size):
        piece = size // 2
        low, high = down(ref, near, first, piece), down(ref, far, first + piece, piece)
        return [
            remote(low, low, MAIN, slot, {"fs": far}),
            remote(high, high, MAIN, slot, {"fs": near}),
        ]

    def start(copies):
        for copy in copies:
            copy.start()

    kv_out = outgoing(wkv_all, STAGE, 0, depth)
    q_out = [outgoing(wq_all, STAGE + turn, piece_at(turn), chunk_rows) for turn in turns]
    if hops:
        kv_on = onward(wkv_all, STAGE + 1, 0, depth)
        last = STAGE + chunks
        q_on = [onward(wq_all, last, piece_at(turn), chunk_rows) for turn in turns]
    else:
        kv_on = []
        q_on = [[] for turn in turns]
    @pl.when(kv_core)
    def _():
        l_kv.wait()
        start(kv_out)

    l_tok.wait()
    l_gain.wait()
    c_tok = remote(tok.at[t], tok.at[t], SIDE_A, TOK, mate)
    c_tok.start()
    c_gain = remote(gain.at[t], gain.at[t], SIDE_B, GAIN, mate)
    c_gain.start()
    lane = lax.broadcasted_iota(jnp.int32, (rows, 128), 1)
    place = s * rows + lax.broadcasted_iota(jnp.int32, (rows, 128), 0)
    quarter = ROPE_DIM // 4
    power = (lane % quarter).astype(F32) * (2.0 / (ROPE_DIM // 2))
    inverse = jnp.exp(power * (-math.log(THETA)))
    grid_row = place // GRID_W
    grid_col = place - grid_row * GRID_W
    in_a = (lane % ROPE_DIM) < (ROPE_DIM // 2)
    angle = jnp.where(in_a, grid_row, grid_col).astype(F32) * inverse
    is_u = (lane % (2 * quarter)) < quarter
    cosine = jnp.cos(angle)
    sine = jnp.where(is_u, -jnp.sin(angle), jnp.sin(angle))

    def rotated(pre):
        wide = pre.astype(BF16).astype(F32)
        swapped = jnp.where(is_u, pltpu.roll(wide, 128 - quarter, 1), pltpu.roll(wide, quarter, 1))
        return wide * cosine + swapped * sine

    if line:
        spread_word()
    c_gain.wait()
    c_tok.wait()
    whole = jnp.concatenate([tok[0], tok[1]], axis=1).astype(F32)
    lines = gain.shape[1]
    wide_gain = [gain[0].astype(F32), gain[1].astype(F32)]
    flat_gain = jnp.concatenate(
        [side[i : i + 1, :] for side in wide_gain for i in range(lines)], axis=1
    )
    hid[...] = normed(whole, flat_gain)

    own_rows = pl.ds(pl.multiple_of(s * rows, rows), rows)

    def rows_of(owner):
        return pl.ds(pl.multiple_of(owner * rows, rows), rows)

    if n_sp == 4:
        peers_to = (s + 1 - 2 * parity, (s + 2) % 4, 3 - s)
        peers_from = peers_to
    else:
        peers_to = tuple((s + j) % n_sp for j in range(1, n_sp))
        peers_from = tuple((s + n_sp - j) % n_sp for j in range(1, n_sp))

    def rope_copy(owner, device):
        return remote(ropes.at[owner], ropes.at[owner], BLOCK, ROPE, device)

    def latent(owner, sent, slot, device):
        here = kv_lat.at[rows_of(owner)]
        return remote(here, here, sent, slot, device)

    base = STAGE + 2
    taken = LATENT
    c_own = latent(s, GATHER, taken, mate)
    gather_out = [latent(s, GATHER, base + j, {"sp": peer}) for j, peer in enumerate(peers_to)]
    gather_in = [latent(owner, GATHER, base + j, mate) for j, owner in enumerate(peers_from)]
    passed = [latent(owner, PASS, taken, mate) for owner in peers_from]

    all_loaded(wkr, wpi)
    pool_in = mm(hid[...], wpi[...]).astype(BF16)
    halo_out[0] = pool_in[rows - 2 * RIM :, :].astype(F32)[RIM:, :]
    halo_out[1] = pool_in[: 2 * RIM, :].astype(F32)[:RIM, :]
    c_up = remote(halo_out.at[0], halo_in.at[0], SIDE_A, UP, above)
    c_dn = remote(halo_out.at[1], halo_in.at[1], SIDE_B, DOWN, below)
    pl.when(has_next)(c_up.start)
    pl.when(has_prev)(c_dn.start)

    @pl.when(q_core)
    def _():
        l_q.wait()
        for copies in q_out:
            start(copies)


    key_pre = mm_t(hid[...], wkr[...])
    key_rope = rotated(jnp.concatenate([key_pre, key_pre], axis=1))
    lower_half = lax.broadcasted_iota(jnp.int32, (half, 128), 1) < ROPE_DIM
    ropes[s] = jnp.where(lower_half, key_rope[:half], key_rope[half:]).astype(BF16)
    if line:
        hear_word()
    for peer in peers_to:
        copy = rope_copy(s, {"sp": peer})
        copy.start()

    @pl.when(kv_core)
    def _():
        all_taken(wkv_all, len(senders) * depth, STAGE)
        start(kv_on)

    def no_rim(side):
        def clear():
            halo_in[side] = jnp.zeros(halo_in.shape[1:], F32)

        return clear

    pl.when(has_prev)(c_up.wait_recv)
    pl.when(has_next)(c_dn.wait_recv)
    pl.when(s == 0)(no_rim(0))
    pl.when(s == n_sp - 1)(no_rim(1))
    halo = jnp.concatenate([halo_in[0], halo_in[1]], axis=0).astype(BF16)
    padded = jnp.concatenate([pool_in, halo], axis=0)
    span = rows + 2 * RIM
    k_index = lax.broadcasted_iota(jnp.int32, (rows, span), 1)
    q_index = lax.broadcasted_iota(jnp.int32, (rows, span), 0)
    k_place = jnp.where(
        k_index < rows,
        k_index,
        jnp.where(k_index < rows + RIM, k_index - rows - RIM, k_index - RIM),
    )
    offset = k_place - q_index
    l_kvg.wait()
    l_qg.wait()
    all_loaded(mix, wop)
    inside = (k_place + s * rows >= 0) & (k_place + s * rows < length)
    pooled = []
    for g in range(groups):
        group = t * groups + g
        window = jnp.int32(0)
        for index, size in enumerate(WINDOWS):
            window = jnp.where(group == index, size, window)
        before = window // 2
        band = jnp.where(
            inside & (offset >= -before) & (offset < window - before), 1.0, 0.0
        )
        count = jnp.sum(band, axis=1, keepdims=True)
        cols = slice(g * POOL_GROUP, (g + 1) * POOL_GROUP)
        mean = (mm(band.astype(BF16), padded[:, cols]) / count).astype(BF16)
        spread = (mean.astype(F32) - pool_in[:, cols].astype(F32)).astype(BF16)
        pooled.append(mm(spread, mix[g]).astype(BF16))
    acc[...] = mm(jnp.concatenate(pooled, axis=1), wop[...])


    @pl.when(kv_core)
    def _():
        if hops:
            all_taken(wkv_all, depth, STAGE + 1)
        pre = mm(hid[...], wkv_all[...]).astype(BF16).astype(F32)
        kv_lat[own_rows] = normed(pre, kvg[...])
        start(gather_out + [c_own])

    @pl.when(q_core)
    def _():
        for turn in turns:
            all_taken(wq_all, len(senders) * chunk_rows, STAGE + turn)
            start(q_on[turn])

    def finish_rope(owner):
        here = rows_of(owner)
        packed = ropes[owner].astype(F32)
        swapped = pltpu.roll(packed, ROPE_DIM, 1)
        low = jnp.where(lower_half, packed, swapped)
        high = jnp.where(lower_half, swapped, packed)
        kcat[here, kv_rank:] = jnp.concatenate([low, high], axis=0).astype(BF16)

    all_taken(ropes, n_sp - 1, ROPE)
    all_sent(ropes, n_sp - 1, BLOCK)
    for owner in (s,) + peers_from:
        finish_rope(owner)

    c_lat = remote(q_lat, q_lat, GATHER, LATENT, mate)

    def from_shard(owner):
        first = pl.multiple_of(owner * depth, depth)
        return mm(hid[:, pl.ds(first, depth)], wq_all[pl.ds(first, depth), :])

    @pl.when(kv_core)
    def _():
        for j in range(n_sp - 1):
            gather_in[j].wait_recv()
            passed[j].start()
        c_lat.wait_recv()

    @pl.when(q_core)
    def _():
        q_part[...] = functools.reduce(jnp.add, [from_shard(owner) for owner in (f,) + senders])
        if hops:
            all_taken(wq_all, depth, STAGE + chunks)
        q_sum = q_part[...]
        if hops:
            q_sum = q_sum + from_shard(across)
        q_lat[...] = normed(q_sum.astype(BF16).astype(F32), qg[...])
        c_lat.start()

    q_latent = q_lat[...]
    all_loaded(wqn, wqr, wku, wvu)
    l_oa.wait()
    q_nope = mm(q_latent, wqn[...]).astype(BF16)
    q_pre = mm(q_latent, wqr[...])
    low_lanes = lane < ROPE_DIM
    for h in range(heads):
        cols = slice(h * NOPE_DIM, (h + 1) * NOPE_DIM)
        absorbed = mm_t(q_nope[:, cols], wku[:, cols]).astype(BF16)
        if h % 2 == 0:
            turned = rotated(q_pre[:, h * ROPE_DIM : (h + 2) * ROPE_DIM])
        rope = jnp.where(low_lanes if h % 2 == 0 else ~low_lanes, turned, 0.0).astype(BF16)
        for part in range(2):
            piece = slice(part * half, (part + 1) * half)
            qcat[part, h * half : (h + 1) * half, :kv_rank] = absorbed[piece]
            qcat[part, h * half : (h + 1) * half, kv_rank:] = rope[piece]

    factor = (NOPE_DIM + ROPE_DIM) ** (-0.5) * math.log2(math.e)
    span_keys = rows * max(
        c for c in range(1, n_sp + 1) if n_sp % c == 0 and (c == 1 or rows * c <= SPAN_LIMIT)
    )
    spans = length // span_keys
    block = 4 * half

    def attend(part):
        def one_block(b, carry):
            block_rows = pl.ds(pl.multiple_of(b * block, block), block)
            queries = qcat[part, block_rows, :]

            def absorb(keys, state):
                scores = mm_t(queries, keys)
                top = jnp.max(scores, axis=1, keepdims=True)
                if state is not None:
                    top = jnp.maximum(top, state[0])
                weights = jnp.exp2((scores - top) * factor)
                total = jnp.sum(weights, axis=1, keepdims=True)
                summed = mm(weights.astype(BF16), keys[:, :kv_rank])
                if state is not None:
                    shrink = jnp.exp2((state[0] - top) * factor)
                    total = total + state[1] * shrink
                    summed = summed + state[2] * shrink
                return top, total, summed

            if spans == 1:
                state = absorb(kcat[...], None)
            else:
                state = absorb(kcat[:span_keys, :], None)

                def step(i, now):
                    start = pl.multiple_of(i * span_keys, span_keys)
                    return absorb(kcat[pl.ds(start, span_keys), :], now)

                state = lax.fori_loop(1, spans, step, state)
            ctx[block_rows, :] = (state[2] / state[1]).astype(BF16)
            return carry

        lax.fori_loop(0, heads * half // block, one_block, 0, unroll=True)
        for h in range(heads):
            cols = slice(h * VALUE_DIM, (h + 1) * VALUE_DIM)
            att[:, cols] = mm(ctx[h * half : (h + 1) * half, :], wvu[:, cols]).astype(BF16)
        own = acc[pl.ds(pl.multiple_of(part * half, half), half), :]
        return own + mm(att[...], woa[...])


    @pl.when(q_core)
    def _():
        all_taken(kv_lat, n_sp * rows, LATENT)

    kcat[:, :kv_rank] = kv_lat[...]
    share[...] = attend(1 - t).astype(BF16)
    c_share = remote(share, arrived, BLOCK, SHARE, mate)
    c_share.start()
    mine = attend(t)
    c_share.wait()
    out[0] = (mine + arrived[...].astype(F32)).astype(BF16)
    pl.when(has_next)(c_up.wait_send)
    pl.when(has_prev)(c_dn.wait_send)

    @pl.when(kv_core)
    def _():
        all_sent(wkv_all, (n_fs - 1) * depth, MAIN)
        all_sent(kv_lat, n_sp * rows, GATHER)
        all_sent(kv_lat, (n_sp - 1) * rows, PASS)

    @pl.when(q_core)
    def _():
        all_sent(wq_all, (n_fs - 1) * depth, MAIN)
        c_lat.wait_send()


def solution(mesh):
    n_sp, n_fs = mesh.shape["sp"], mesh.shape["fs"]

    def on_device(*args):
        args = list(args)
        args[1] = args[1].reshape(-1, 128)
        for i in (3, 7):
            args[i] = args[i].reshape(1, -1)
        args[10] = args[10].T
        (tokens, gain, wqd, qg, wqn, wqr, wkvd, kvg, wku, wvu, wkr, wpi, mix, woa, wop) = args
        rows, cols = tokens.shape[1:]
        half = rows // 2
        heads = wqn.shape[1] // NOPE_DIM
        kv_rank = wkvd.shape[1]
        q_rank = wqd.shape[1]
        d_model = woa.shape[1]
        groups = wpi.shape[1] // POOL_GROUP

        def vmem(*shape, kind=BF16):
            return pltpu.VMEM(shape, kind)

        def same(array):
            return pltpu.VMEM(array.shape, array.dtype)

        dma = pltpu.SemaphoreType.DMA
        return pl.pallas_call(
            functools.partial(layer, n_sp, n_fs),
            out_shape=pltpu.VMEM((1, half, d_model), BF16),
            in_specs=[pl.BlockSpec(memory_space=pltpu.HBM)] * len(args),
            out_specs=pl.BlockSpec(memory_space=pltpu.VMEM),
            scratch_shapes=[
                vmem(2, rows, cols),
                vmem(2, cols // 128, 128),
                vmem(rows, 2 * cols),
                vmem(n_fs * wqd.shape[0], q_rank),
                vmem(n_fs * wkvd.shape[0], kv_rank),
                same(qg),
                same(kvg),
                same(wqn),
                same(wqr),
                same(wku),
                same(wvu),
                same(wkr),
                same(wpi),
                vmem(groups, POOL_GROUP, POOL_GROUP),
                same(woa),
                same(wop),
                vmem(2, RIM, wpi.shape[1], kind=F32),
                vmem(2, RIM, wpi.shape[1], kind=F32),
                vmem(rows, q_rank, kind=F32),
                vmem(rows, q_rank),
                vmem(n_sp * rows, kv_rank),
                vmem(n_sp, half, 2 * ROPE_DIM),
                vmem(n_sp * rows, kv_rank + 2 * ROPE_DIM),
                vmem(2, heads * half, kv_rank + 2 * ROPE_DIM),
                vmem(heads * half, kv_rank),
                vmem(half, heads * VALUE_DIM),
                vmem(rows, d_model, kind=F32),
                vmem(half, d_model),
                vmem(half, d_model),
                dma((9,)),
                dma((6,)),
                dma((STAGE + max(5, n_sp + 1),)),
                pltpu.SemaphoreType.REGULAR((2,)),
            ],
            compiler_params=pltpu.CompilerParams(collective_id=0, has_side_effects=True, vmem_limit_bytes=40 * 1024 * 1024),
        )(*[pltpu.with_memory_space_constraint(a, pltpu.HBM) for a in args])

    placed = (
        P("fs", "sp", "tp"),
        P("tp"),
        P("fs", None),
        P(),
        P(None, "tp"),
        P(None, "tp"),
        P("fs", None),
        P(),
        P(None, "tp"),
        P(None, "tp"),
        P(),
        P(None, "tp"),
        P(),
        P("tp", None),
        P("tp", None),
    )
    return jax.shard_map(
        on_device,
        mesh=mesh,
        in_specs=placed,
        out_specs=P("fs", ("sp", "tp"), None),
        check_vma=False,
    )
```

```python
import functools
import math

import jax
import jax.numpy as jnp
from jax import lax
from jax.experimental import pallas as pl
from jax.experimental.pallas import tpu as pltpu
from jax.sharding import PartitionSpec as P

NOPE_DIM = 128
ROPE_DIM = 64
VALUE_DIM = 128
GRID_W = 64
POOL_GROUP = 256
EPS = 1e-06
THETA = 10000.0
WINDOWS = (2, 4, 8, 16)
RIM = 8
SPAN_LIMIT = 1024
F32 = jnp.float32
BF16 = jnp.bfloat16
MESH = pl.DeviceIdType.MESH
TOK, GAIN, UP, DOWN, LATENT, SHARE, ROPE, STAGE = range(8)
MAIN, GATHER, PASS, BLOCK, SIDE_A, SIDE_B = range(6)


def mm(a, b):
    return jnp.dot(a, b, preferred_element_type=F32)


def mm_t(a, b):
    return lax.dot_general(a, b, (((1,), (1,)), ((), ())), preferred_element_type=F32)


def normed(wide, gain):
    scale = lax.rsqrt(jnp.mean(wide * wide, axis=-1, keepdims=True) + EPS)
    return (wide * scale * gain).astype(BF16)


def layer(
    n_sp,
    n_fs,
    tokens,
    norm_gain,
    w_q_down,
    q_gain,
    w_q_nope,
    w_q_rope,
    w_kv_down,
    kv_gain,
    w_k_up,
    w_v_up,
    w_k_rope,
    w_pool_in,
    w_pool_mix,
    w_out_attn,
    w_out_pool,
    out,
    tok,
    gain,
    hid,
    wq_all,
    wkv_all,
    qg,
    kvg,
    wqn,
    wqr,
    wku,
    wvu,
    wkr,
    wpi,
    mix,
    woa,
    wop,
    halo_out,
    halo_in,
    q_part,
    q_lat,
    kv_lat,
    ropes,
    kcat,
    qcat,
    ctx,
    acc,
    share,
    arrived,
    local_sem,
    send_sem,
    recv_sem,
    word,
):
    s = lax.axis_index("sp")
    f = lax.axis_index("fs")
    t = lax.axis_index("tp")
    rows = tok.shape[1]
    half = rows // 2
    depth = w_q_down.shape[0]
    kv_rank = wkv_all.shape[1]
    kv_core, q_core = t == 1, t == 0
    heads = wqn.shape[1] // NOPE_DIM
    groups = wpi.shape[1] // POOL_GROUP
    length = rows * n_sp

    def down(ref, owner, first=0, size=depth):
        start = pl.multiple_of(owner * depth + first, 16)
        return ref.at[pl.ds(start, size), :]

    pairs = (
        (w_kv_down, down(wkv_all, f)),
        (tokens.at[0], tok.at[t]),
        (norm_gain, gain.at[t]),
        (w_q_down, down(wq_all, f)),
        (w_k_rope, wkr),
        (w_pool_in, wpi),
        (kv_gain, kvg),
        (q_gain, qg),
        (w_pool_mix.at[pl.ds(t * groups, groups)], mix),
        (w_out_pool, wop),
        (w_q_nope, wqn),
        (w_q_rope, wqr),
        (w_k_up, wku),
        (w_v_up, wvu),
        (w_out_attn, woa),
    )
    slots = (0, 1, 2, 0, 3, 3, 4, 5, 6, 6, 7, 7, 7, 7, 8)
    loads = [
        pltpu.make_async_copy(src, dst, local_sem.at[slot])
        for slot, (src, dst) in zip(slots, pairs)
    ]
    (
        l_kv,
        l_tok,
        l_gain,
        l_q,
        l_kr,
        l_pi,
        l_kvg,
        l_qg,
        l_mix,
        l_op,
        l_qn,
        l_qr,
        l_ku,
        l_vu,
        l_oa,
    ) = loads
    for load in loads:
        if load is l_kv:
            pl.when(kv_core)(load.start)
        elif load is l_q:
            pl.when(q_core)(load.start)
        else:
            load.start()

    barrier = pltpu.get_barrier_semaphore()

    def greet(device):
        pl.semaphore_signal(barrier, inc=1, device_id=device, device_id_type=MESH)

    hops = n_fs == 4
    line = hops and n_sp == 4
    has_prev, has_next = s > 0, s < n_sp - 1
    mate = {"tp": 1 - t}
    above, below = {"sp": (s + 1) % n_sp}, {"sp": (s + n_sp - 1) % n_sp}
    parity = s % 2
    if hops:
        near = f + 1 - 2 * (f % 2)
        far = (f + 2) % 4
        across = 3 - f
    greet(mate)
    if line:
        greet({"fs": near})
        greet({"fs": far})
        pl.when(has_next)(lambda: greet(above))
        pl.when(has_prev)(lambda: greet(below))
        guests = 5 - (s == 0).astype(jnp.int32) - (s == n_sp - 1).astype(jnp.int32)
    else:
        for j in range(1, n_fs):
            greet({"fs": (f + j) % n_fs})
        for j in range(1, n_sp):
            greet({"sp": (s + j) % n_sp})
        guests = n_sp + n_fs - 1
    pl.semaphore_wait(barrier, guests)

    def tell(side, device):
        pl.semaphore_signal(word.at[side], inc=1, device_id=device, device_id_type=MESH)

    def hear(side, count):
        return lambda: pl.semaphore_wait(word.at[side], count)

    if line:

        def both_ways():
            tell(0, above)
            tell(1, below)

        pl.when(has_prev & has_next)(both_ways)

    def spread_word():
        def up():
            hear(0, 1)()
            tell(0, above)

        def down_():
            hear(1, 1)()
            tell(1, below)

        pl.when(s == n_sp - 2)(up)
        pl.when(s == 1)(down_)

    def hear_word():
        pl.when(s == n_sp - 1)(hear(0, 2))
        pl.when(s == 0)(hear(1, 2))

    def remote(src, dst, sent, slot, device):
        return pltpu.make_async_remote_copy(
            src_ref=src,
            dst_ref=dst,
            send_sem=send_sem.at[sent],
            recv_sem=recv_sem.at[slot],
            device_id=device,
            device_id_type=MESH,
        )

    def part_of(ref, count):
        return ref.at[pl.ds(0, count)]

    def all_sent(ref, count, sent):
        part = part_of(ref, count)
        remote(part, part, sent, TOK, mate).wait_send()

    def all_taken(ref, count, slot):
        part = part_of(ref, count)
        remote(part, part, MAIN, slot, mate).wait_recv()

    def all_loaded(*refs):
        slot = {id(ref): i for ref, i in zip((dst for _, dst in pairs), slots)}[id(refs[0])]
        line_bytes = 2 * woa.shape[1]
        total = sum(math.prod(ref.shape) * ref.dtype.itemsize for ref in refs)
        part = part_of(woa, total // line_bytes)
        pltpu.make_async_copy(part, part, local_sem.at[slot]).wait()

    chunks = 4
    chunk_rows = depth // chunks
    if hops:
        partners = senders = (near, far)
    else:
        partners = tuple((f + j) % n_fs for j in range(1, n_fs))
        senders = tuple((f + n_fs - j) % n_fs for j in range(1, n_fs))
    def piece_at(turn):
        return turn * chunk_rows

    turns = range(chunks)

    def outgoing(ref, slot, first, size):
        part = down(ref, f, first, size)
        return [remote(part, part, MAIN, slot, {"fs": peer}) for peer in partners]

    def onward(ref, slot, first, size):
        piece = size // 2
        low, high = down(ref, near, first, piece), down(ref, far, first + piece, piece)
        return [
            remote(low, low, MAIN, slot, {"fs": far}),
            remote(high, high, MAIN, slot, {"fs": near}),
        ]

    def start(copies):
        for copy in copies:
            copy.start()

    kv_out = outgoing(wkv_all, STAGE, 0, depth)
    q_out = [outgoing(wq_all, STAGE + turn, piece_at(turn), chunk_rows) for turn in turns]
    if hops:
        kv_on = onward(wkv_all, STAGE + 1, 0, depth)
        last = STAGE + chunks
        q_on = [onward(wq_all, last, piece_at(turn), chunk_rows) for turn in turns]
    else:
        kv_on = []
        q_on = [[] for turn in turns]
    @pl.when(kv_core)
    def _():
        l_kv.wait()
        start(kv_out)

    l_tok.wait()
    l_gain.wait()
    c_tok = remote(tok.at[t], tok.at[t], SIDE_A, TOK, mate)
    c_tok.start()
    c_gain = remote(gain.at[t], gain.at[t], SIDE_B, GAIN, mate)
    c_gain.start()
    lane = lax.broadcasted_iota(jnp.int32, (rows, 128), 1)
    place = s * rows + lax.broadcasted_iota(jnp.int32, (rows, 128), 0)
    quarter = ROPE_DIM // 4
    power = (lane % quarter).astype(F32) * (2.0 / (ROPE_DIM // 2))
    inverse = jnp.exp(power * (-math.log(THETA)))
    grid_row = place // GRID_W
    grid_col = place - grid_row * GRID_W
    in_a = (lane % ROPE_DIM) < (ROPE_DIM // 2)
    angle = jnp.where(in_a, grid_row, grid_col).astype(F32) * inverse
    is_u = (lane % (2 * quarter)) < quarter
    cosine = jnp.cos(angle)
    sine = jnp.where(is_u, -jnp.sin(angle), jnp.sin(angle))

    def rotated(pre):
        wide = pre.astype(BF16).astype(F32)
        swapped = jnp.where(is_u, pltpu.roll(wide, 128 - quarter, 1), pltpu.roll(wide, quarter, 1))
        return wide * cosine + swapped * sine

    if line:
        spread_word()
    c_gain.wait_recv()
    c_tok.wait_recv()
    whole = jnp.concatenate([tok[0], tok[1]], axis=1).astype(F32)
    lines = gain.shape[1]
    wide_gain = [gain[0].astype(F32), gain[1].astype(F32)]
    flat_gain = jnp.concatenate(
        [side[i : i + 1, :] for side in wide_gain for i in range(lines)], axis=1
    )
    hid[...] = normed(whole, flat_gain)

    own_rows = pl.ds(pl.multiple_of(s * rows, rows), rows)

    def rows_of(owner):
        return pl.ds(pl.multiple_of(owner * rows, rows), rows)

    if n_sp == 4:
        peers_to = (s + 1 - 2 * parity, (s + 2) % 4, 3 - s)
        peers_from = peers_to
    else:
        peers_to = tuple((s + j) % n_sp for j in range(1, n_sp))
        peers_from = tuple((s + n_sp - j) % n_sp for j in range(1, n_sp))

    def rope_copy(owner, device):
        return remote(ropes.at[owner], ropes.at[owner], BLOCK, ROPE, device)

    def latent(owner, sent, slot, device):
        here = kv_lat.at[rows_of(owner)]
        return remote(here, here, sent, slot, device)

    base = STAGE + 2
    taken = LATENT
    c_own = latent(s, GATHER, taken, mate)
    gather_out = [latent(s, GATHER, base + j, {"sp": peer}) for j, peer in enumerate(peers_to)]
    gather_in = [latent(owner, GATHER, base + j, mate) for j, owner in enumerate(peers_from)]
    passed = [latent(owner, PASS, taken, mate) for owner in peers_from]

    all_loaded(wkr, wpi)
    pool_in = mm(hid[...], wpi[...]).astype(BF16)
    halo_out[0] = pool_in[rows - 2 * RIM :, :].astype(F32)[RIM:, :]
    halo_out[1] = pool_in[: 2 * RIM, :].astype(F32)[:RIM, :]
    c_up = remote(halo_out.at[0], halo_in.at[0], SIDE_A, UP, above)
    c_dn = remote(halo_out.at[1], halo_in.at[1], SIDE_B, DOWN, below)
    c_gain.wait_send()
    c_tok.wait_send()
    pl.when(has_next)(c_up.start)
    pl.when(has_prev)(c_dn.start)

    @pl.when(q_core)
    def _():
        l_q.wait()
        for copies in q_out:
            start(copies)


    key_pre = mm_t(hid[...], wkr[...])
    key_rope = rotated(jnp.concatenate([key_pre, key_pre], axis=1))
    lower_half = lax.broadcasted_iota(jnp.int32, (half, 128), 1) < ROPE_DIM
    ropes[s] = jnp.where(lower_half, key_rope[:half], key_rope[half:]).astype(BF16)
    if line:
        hear_word()
    for peer in peers_to:
        copy = rope_copy(s, {"sp": peer})
        copy.start()

    @pl.when(kv_core)
    def _():
        all_taken(wkv_all, len(senders) * depth, STAGE)
        start(kv_on)

    def no_rim(side):
        def clear():
            halo_in[side] = jnp.zeros(halo_in.shape[1:], F32)

        return clear

    pl.when(has_prev)(c_up.wait_recv)
    pl.when(has_next)(c_dn.wait_recv)
    pl.when(s == 0)(no_rim(0))
    pl.when(s == n_sp - 1)(no_rim(1))
    halo = jnp.concatenate([halo_in[0], halo_in[1]], axis=0).astype(BF16)
    padded = jnp.concatenate([pool_in, halo], axis=0)
    span = rows + 2 * RIM
    k_index = lax.broadcasted_iota(jnp.int32, (rows, span), 1)
    q_index = lax.broadcasted_iota(jnp.int32, (rows, span), 0)
    k_place = jnp.where(
        k_index < rows,
        k_index,
        jnp.where(k_index < rows + RIM, k_index - rows - RIM, k_index - RIM),
    )
    offset = k_place - q_index
    l_kvg.wait()
    l_qg.wait()
    all_loaded(mix, wop)
    inside = (k_place + s * rows >= 0) & (k_place + s * rows < length)
    pooled = []
    for g in range(groups):
        group = t * groups + g
        window = jnp.int32(0)
        for index, size in enumerate(WINDOWS):
            window = jnp.where(group == index, size, window)
        before = window // 2
        band = jnp.where(
            inside & (offset >= -before) & (offset < window - before), 1.0, 0.0
        )
        count = jnp.sum(band, axis=1, keepdims=True)
        cols = slice(g * POOL_GROUP, (g + 1) * POOL_GROUP)
        mean = (mm(band.astype(BF16), padded[:, cols]) / count).astype(BF16)
        spread = (mean.astype(F32) - pool_in[:, cols].astype(F32)).astype(BF16)
        pooled.append(mm(spread, mix[g]).astype(BF16))
    acc[...] = mm(jnp.concatenate(pooled, axis=1), wop[...])


    @pl.when(kv_core)
    def _():
        if hops:
            all_taken(wkv_all, depth, STAGE + 1)
        pre = mm(hid[...], wkv_all[...]).astype(BF16).astype(F32)
        kv_lat[own_rows] = normed(pre, kvg[...])
        start(gather_out + [c_own])

    @pl.when(q_core)
    def _():
        for turn in turns:
            all_taken(wq_all, len(senders) * chunk_rows, STAGE + turn)
            start(q_on[turn])

    def finish_rope(owner):
        here = rows_of(owner)
        packed = ropes[owner].astype(F32)
        swapped = pltpu.roll(packed, ROPE_DIM, 1)
        low = jnp.where(lower_half, packed, swapped)
        high = jnp.where(lower_half, swapped, packed)
        kcat[here, kv_rank:] = jnp.concatenate([low, high], axis=0).astype(BF16)

    all_taken(ropes, n_sp - 1, ROPE)
    all_sent(ropes, n_sp - 1, BLOCK)
    for owner in (s,) + peers_from:
        finish_rope(owner)

    c_lat = remote(q_lat, q_lat, GATHER, LATENT, mate)

    def from_shard(owner):
        first = pl.multiple_of(owner * depth, depth)
        return mm(hid[:, pl.ds(first, depth)], wq_all[pl.ds(first, depth), :])

    @pl.when(kv_core)
    def _():
        for j in range(n_sp - 1):
            gather_in[j].wait_recv()
            passed[j].start()
        c_lat.wait_recv()

    @pl.when(q_core)
    def _():
        q_part[...] = functools.reduce(jnp.add, [from_shard(owner) for owner in (f,) + senders])
        if hops:
            all_taken(wq_all, depth, STAGE + chunks)
        q_sum = q_part[...]
        if hops:
            q_sum = q_sum + from_shard(across)
        q_lat[...] = normed(q_sum.astype(BF16).astype(F32), qg[...])
        c_lat.start()

    q_latent = q_lat[...]
    all_loaded(wqn, wqr, wku, wvu)
    l_oa.wait()
    q_nope = mm(q_latent, wqn[...]).astype(BF16)
    q_pre = mm(q_latent, wqr[...])
    low_lanes = lane < ROPE_DIM
    for h in range(heads):
        cols = slice(h * NOPE_DIM, (h + 1) * NOPE_DIM)
        absorbed = mm_t(q_nope[:, cols], wku[:, cols]).astype(BF16)
        if h % 2 == 0:
            turned = rotated(q_pre[:, h * ROPE_DIM : (h + 2) * ROPE_DIM])
        rope = jnp.where(low_lanes if h % 2 == 0 else ~low_lanes, turned, 0.0).astype(BF16)
        for part in range(2):
            piece = slice(part * half, (part + 1) * half)
            qcat[part, h * half : (h + 1) * half, :kv_rank] = absorbed[piece]
            qcat[part, h * half : (h + 1) * half, kv_rank:] = rope[piece]

    factor = (NOPE_DIM + ROPE_DIM) ** (-0.5) * math.log2(math.e)
    span_keys = rows * max(
        c for c in range(1, n_sp + 1) if n_sp % c == 0 and (c == 1 or rows * c <= SPAN_LIMIT)
    )
    spans = length // span_keys
    block = 4 * half

    @pl.when(q_core)
    def _():
        all_taken(kv_lat, n_sp * rows, LATENT)

    kcat[:, :kv_rank] = kv_lat[...]

    def scored(part, first, keys):
        return mm_t(qcat[part, pl.ds(first, block), :], keys)

    def weighed(scores, keys, state):
        top = jnp.max(scores, axis=1, keepdims=True)
        if state is not None:
            top = jnp.maximum(top, state[0])
        weights = jnp.exp2((scores - top) * factor)
        total = jnp.sum(weights, axis=1, keepdims=True)
        summed = mm(weights.astype(BF16), keys[:, :kv_rank])
        if state is not None:
            shrink = jnp.exp2((state[0] - top) * factor)
            total = total + state[1] * shrink
            summed = summed + state[2] * shrink
        return top, total, summed

    part_rows = heads * half
    blocks = part_rows // block

    def keep(order, index, state):
        ctx[pl.ds(order * part_rows + index * block, block), :] = (state[2] / state[1]).astype(BF16)

    def projected(order, part):
        pieces = []
        for h in range(heads):
            mixed_latent = ctx[pl.ds(order * part_rows + h * half, half), :]
            cols = slice(h * VALUE_DIM, (h + 1) * VALUE_DIM)
            pieces.append(mm(mixed_latent, wvu[:, cols]).astype(BF16))
        own = acc[pl.ds(pl.multiple_of(part * half, half), half), :]
        return own + mm(jnp.concatenate(pieces, axis=1), woa[...])

    parts = (1 - t, t)
    c_share = remote(share, arrived, BLOCK, SHARE, mate)

    def give():
        share[...] = projected(0, parts[0]).astype(BF16)
        c_share.start()

    if spans == 1:
        jobs = [(order, index) for order in range(2) for index in range(blocks)]
        ahead = scored(parts[0], 0, kcat[...])
        for i, (order, index) in enumerate(jobs):
            scores = ahead
            if i + 1 < len(jobs):
                later, place_of = jobs[i + 1]
                ahead = scored(parts[later], place_of * block, kcat[...])
            keep(order, index, weighed(scores, kcat[...], None))
            if i == blocks:
                give()
    else:
        for order in range(2):

            def one_block(index, carry):
                first = pl.multiple_of(index * block, block)

                def step(i, state):
                    start_key = pl.multiple_of(i * span_keys, span_keys)
                    keys = kcat[pl.ds(start_key, span_keys), :]
                    return weighed(scored(parts[order], first, keys), keys, state)

                keys = kcat[:span_keys, :]
                state = weighed(scored(parts[order], first, keys), keys, None)
                state = lax.fori_loop(1, spans, step, state)
                row = pl.multiple_of(order * part_rows + first, block)
                ctx[pl.ds(row, block), :] = (state[2] / state[1]).astype(BF16)
                return carry

            lax.fori_loop(0, blocks, one_block, 0, unroll=True)
            if order == 0:
                give()
    mine = projected(1, parts[1])
    c_share.wait()
    out[0] = (mine + arrived[...].astype(F32)).astype(BF16)
    pl.when(has_next)(c_up.wait_send)
    pl.when(has_prev)(c_dn.wait_send)

    @pl.when(kv_core)
    def _():
        all_sent(wkv_all, (n_fs - 1) * depth, MAIN)
        all_sent(kv_lat, n_sp * rows, GATHER)
        all_sent(kv_lat, (n_sp - 1) * rows, PASS)

    @pl.when(q_core)
    def _():
        all_sent(wq_all, (n_fs - 1) * depth, MAIN)
        c_lat.wait_send()


def solution(mesh):
    n_sp, n_fs = mesh.shape["sp"], mesh.shape["fs"]

    def on_device(*args):
        args = list(args)
        args[1] = args[1].reshape(-1, 128)
        for i in (3, 7):
            args[i] = args[i].reshape(1, -1)
        args[10] = args[10].T
        (tokens, gain, wqd, qg, wqn, wqr, wkvd, kvg, wku, wvu, wkr, wpi, mix, woa, wop) = args
        rows, cols = tokens.shape[1:]
        half = rows // 2
        heads = wqn.shape[1] // NOPE_DIM
        kv_rank = wkvd.shape[1]
        q_rank = wqd.shape[1]
        d_model = woa.shape[1]
        groups = wpi.shape[1] // POOL_GROUP

        def vmem(*shape, kind=BF16):
            return pltpu.VMEM(shape, kind)

        def same(array):
            return pltpu.VMEM(array.shape, array.dtype)

        dma = pltpu.SemaphoreType.DMA
        return pl.pallas_call(
            functools.partial(layer, n_sp, n_fs),
            out_shape=pltpu.VMEM((1, half, d_model), BF16),
            in_specs=[pl.BlockSpec(memory_space=pltpu.HBM)] * len(args),
            out_specs=pl.BlockSpec(memory_space=pltpu.VMEM),
            scratch_shapes=[
                vmem(2, rows, cols),
                vmem(2, cols // 128, 128),
                vmem(rows, 2 * cols),
                vmem(n_fs * wqd.shape[0], q_rank),
                vmem(n_fs * wkvd.shape[0], kv_rank),
                same(qg),
                same(kvg),
                same(wqn),
                same(wqr),
                same(wku),
                same(wvu),
                same(wkr),
                same(wpi),
                vmem(groups, POOL_GROUP, POOL_GROUP),
                same(woa),
                same(wop),
                vmem(2, RIM, wpi.shape[1], kind=F32),
                vmem(2, RIM, wpi.shape[1], kind=F32),
                vmem(rows, q_rank, kind=F32),
                vmem(rows, q_rank),
                vmem(n_sp * rows, kv_rank),
                vmem(n_sp, half, 2 * ROPE_DIM),
                vmem(n_sp * rows, kv_rank + 2 * ROPE_DIM),
                vmem(2, heads * half, kv_rank + 2 * ROPE_DIM),
                vmem(2 * heads * half, kv_rank),
                vmem(rows, d_model, kind=F32),
                vmem(half, d_model),
                vmem(half, d_model),
                dma((9,)),
                dma((6,)),
                dma((STAGE + max(5, n_sp + 1),)),
                pltpu.SemaphoreType.REGULAR((2,)),
            ],
            compiler_params=pltpu.CompilerParams(collective_id=0, has_side_effects=True, vmem_limit_bytes=40 * 1024 * 1024),
        )(*[pltpu.with_memory_space_constraint(a, pltpu.HBM) for a in args])

    placed = (
        P("fs", "sp", "tp"),
        P("tp"),
        P("fs", None),
        P(),
        P(None, "tp"),
        P(None, "tp"),
        P("fs", None),
        P(),
        P(None, "tp"),
        P(None, "tp"),
        P(),
        P(None, "tp"),
        P(),
        P("tp", None),
        P("tp", None),
    )
    return jax.shard_map(
        on_device,
        mesh=mesh,
        in_specs=placed,
        out_specs=P("fs", ("sp", "tp"), None),
        check_vma=False,
    )
```

```python
import functools
import math

import jax
import jax.numpy as jnp
from jax import lax
from jax.experimental import pallas as pl
from jax.experimental.pallas import tpu as pltpu
from jax.sharding import PartitionSpec as P

NOPE_DIM = 128
ROPE_DIM = 64
VALUE_DIM = 128
GRID_W = 64
POOL_GROUP = 256
EPS = 1e-06
THETA = 10000.0
WINDOWS = (2, 4, 8, 16)
RIM = 8
SPAN_LIMIT = 1024
F32 = jnp.float32
BF16 = jnp.bfloat16
MESH = pl.DeviceIdType.MESH
TOK, GAIN, UP, DOWN, LATENT, SHARE, ROPE, STAGE = range(8)
MAIN, GATHER, PASS, BLOCK, SIDE_A, SIDE_B = range(6)


def mm(a, b):
    return jnp.dot(a, b, preferred_element_type=F32)


def mm_t(a, b):
    return lax.dot_general(a, b, (((1,), (1,)), ((), ())), preferred_element_type=F32)


def normed(wide, gain):
    scale = lax.rsqrt(jnp.mean(wide * wide, axis=-1, keepdims=True) + EPS)
    return (wide * scale * gain).astype(BF16)


def layer(
    n_sp,
    n_fs,
    tokens,
    norm_gain,
    w_q_down,
    q_gain,
    w_q_nope,
    w_q_rope,
    w_kv_down,
    kv_gain,
    w_k_up,
    w_v_up,
    w_k_rope,
    w_pool_in,
    w_pool_mix,
    w_out_attn,
    w_out_pool,
    out,
    tok,
    gain,
    hid,
    wq_all,
    wkv_all,
    qg,
    kvg,
    wqn,
    wqr,
    wku,
    wvu,
    wkr,
    wpi,
    mix,
    woa,
    wop,
    halo_out,
    halo_in,
    q_part,
    q_lat,
    kv_lat,
    ropes,
    kcat,
    qcat,
    ctx,
    acc,
    share,
    arrived,
    local_sem,
    send_sem,
    recv_sem,
    word,
):
    s = lax.axis_index("sp")
    f = lax.axis_index("fs")
    t = lax.axis_index("tp")
    rows = tok.shape[1]
    half = rows // 2
    depth = w_q_down.shape[0]
    kv_rank = wkv_all.shape[1]
    kv_core, q_core = t == 1, t == 0
    heads = wqn.shape[1] // NOPE_DIM
    groups = wpi.shape[1] // POOL_GROUP
    length = rows * n_sp

    def down(ref, owner, first=0, size=depth):
        start = pl.multiple_of(owner * depth + first, 16)
        return ref.at[pl.ds(start, size), :]

    pairs = (
        (w_kv_down, down(wkv_all, f)),
        (tokens.at[0], tok.at[t]),
        (norm_gain, gain.at[t]),
        (w_q_down, down(wq_all, f)),
        (w_k_rope, wkr),
        (w_pool_in, wpi),
        (kv_gain, kvg),
        (q_gain, qg),
        (w_pool_mix.at[pl.ds(t * groups, groups)], mix),
        (w_out_pool, wop),
        (w_q_nope, wqn),
        (w_q_rope, wqr),
        (w_k_up, wku),
        (w_v_up, wvu),
        (w_out_attn, woa),
    )
    slots = (0, 1, 2, 0, 3, 3, 4, 5, 6, 6, 7, 7, 7, 7, 8)
    loads = [
        pltpu.make_async_copy(src, dst, local_sem.at[slot])
        for slot, (src, dst) in zip(slots, pairs)
    ]
    (
        l_kv,
        l_tok,
        l_gain,
        l_q,
        l_kr,
        l_pi,
        l_kvg,
        l_qg,
        l_mix,
        l_op,
        l_qn,
        l_qr,
        l_ku,
        l_vu,
        l_oa,
    ) = loads
    for load in loads:
        if load is l_kv:
            pl.when(kv_core)(load.start)
        elif load is l_q:
            pl.when(q_core)(load.start)
        else:
            load.start()

    barrier = pltpu.get_barrier_semaphore()

    def greet(device):
        pl.semaphore_signal(barrier, inc=1, device_id=device, device_id_type=MESH)

    hops = n_fs == 4
    line = hops and n_sp == 4
    has_prev, has_next = s > 0, s < n_sp - 1
    mate = {"tp": 1 - t}
    above, below = {"sp": (s + 1) % n_sp}, {"sp": (s + n_sp - 1) % n_sp}
    parity = s % 2
    if hops:
        near = f + 1 - 2 * (f % 2)
        far = (f + 2) % 4
        across = 3 - f
    greet(mate)
    if line:
        greet({"fs": near})
        greet({"fs": far})
        pl.when(has_next)(lambda: greet(above))
        pl.when(has_prev)(lambda: greet(below))
        guests = 5 - (s == 0).astype(jnp.int32) - (s == n_sp - 1).astype(jnp.int32)
    else:
        for j in range(1, n_fs):
            greet({"fs": (f + j) % n_fs})
        for j in range(1, n_sp):
            greet({"sp": (s + j) % n_sp})
        guests = n_sp + n_fs - 1
    pl.semaphore_wait(barrier, guests)

    def tell(side, device):
        pl.semaphore_signal(word.at[side], inc=1, device_id=device, device_id_type=MESH)

    def hear(side, count):
        return lambda: pl.semaphore_wait(word.at[side], count)

    if line:

        def both_ways():
            tell(0, above)
            tell(1, below)

        pl.when(has_prev & has_next)(both_ways)

    def spread_word():
        def up():
            hear(0, 1)()
            tell(0, above)

        def down_():
            hear(1, 1)()
            tell(1, below)

        pl.when(s == n_sp - 2)(up)
        pl.when(s == 1)(down_)

    def hear_word():
        pl.when(s == n_sp - 1)(hear(0, 2))
        pl.when(s == 0)(hear(1, 2))

    def remote(src, dst, sent, slot, device):
        return pltpu.make_async_remote_copy(
            src_ref=src,
            dst_ref=dst,
            send_sem=send_sem.at[sent],
            recv_sem=recv_sem.at[slot],
            device_id=device,
            device_id_type=MESH,
        )

    def part_of(ref, count):
        return ref.at[pl.ds(0, count)]

    def all_sent(ref, count, sent):
        part = part_of(ref, count)
        remote(part, part, sent, TOK, mate).wait_send()

    def all_taken(ref, count, slot):
        part = part_of(ref, count)
        remote(part, part, MAIN, slot, mate).wait_recv()

    def all_loaded(*refs):
        slot = {id(ref): i for ref, i in zip((dst for _, dst in pairs), slots)}[id(refs[0])]
        line_bytes = 2 * woa.shape[1]
        total = sum(math.prod(ref.shape) * ref.dtype.itemsize for ref in refs)
        part = part_of(woa, total // line_bytes)
        pltpu.make_async_copy(part, part, local_sem.at[slot]).wait()

    sizes = (depth // 4,) * 3 + (depth // 8,) * 2
    places = tuple(sum(sizes[:turn]) for turn in range(len(sizes)))
    kv_turns = 2
    kv_rows = depth // kv_turns
    if hops:
        partners = senders = (near, far)
    else:
        partners = tuple((f + j) % n_fs for j in range(1, n_fs))
        senders = tuple((f + n_fs - j) % n_fs for j in range(1, n_fs))
    turns = range(len(sizes))

    def outgoing(ref, slot, first, size):
        part = down(ref, f, first, size)
        return [remote(part, part, MAIN, slot, {"fs": peer}) for peer in partners]

    def onward(ref, slot, first, size):
        piece = size // 2
        low, high = down(ref, near, first, piece), down(ref, far, first + piece, piece)
        return [
            remote(low, low, MAIN, slot, {"fs": far}),
            remote(high, high, MAIN, slot, {"fs": near}),
        ]

    def start(copies):
        for copy in copies:
            copy.start()

    kv_out = [
        outgoing(wkv_all, STAGE + turn, turn * kv_rows, kv_rows) for turn in range(kv_turns)
    ]
    q_out = [outgoing(wq_all, STAGE + turn, places[turn], sizes[turn]) for turn in turns]
    kv_last, q_last = STAGE + kv_turns, STAGE + len(sizes)
    if hops:
        kv_on = [
            onward(wkv_all, kv_last, turn * kv_rows, kv_rows) for turn in range(kv_turns)
        ]
        q_on = [onward(wq_all, q_last, places[turn], sizes[turn]) for turn in turns]
    else:
        kv_on = [[] for turn in range(kv_turns)]
        q_on = [[] for turn in turns]

    def from_shard(ref, owner):
        first = pl.multiple_of(owner * depth, depth)
        return mm(hid[:, pl.ds(first, depth)], ref[pl.ds(first, depth), :])

    def from_near(ref):
        return functools.reduce(jnp.add, [from_shard(ref, owner) for owner in (f,) + senders])

    @pl.when(kv_core)
    def _():
        l_kv.wait()
        for copies in kv_out:
            start(copies)

    l_tok.wait()
    l_gain.wait()
    c_tok = remote(tok.at[t], tok.at[t], SIDE_A, TOK, mate)
    c_tok.start()
    c_gain = remote(gain.at[t], gain.at[t], SIDE_B, GAIN, mate)
    c_gain.start()
    lane = lax.broadcasted_iota(jnp.int32, (rows, 128), 1)
    place = s * rows + lax.broadcasted_iota(jnp.int32, (rows, 128), 0)
    quarter = ROPE_DIM // 4
    power = (lane % quarter).astype(F32) * (2.0 / (ROPE_DIM // 2))
    inverse = jnp.exp(power * (-math.log(THETA)))
    grid_row = place // GRID_W
    grid_col = place - grid_row * GRID_W
    in_a = (lane % ROPE_DIM) < (ROPE_DIM // 2)
    angle = jnp.where(in_a, grid_row, grid_col).astype(F32) * inverse
    is_u = (lane % (2 * quarter)) < quarter
    cosine = jnp.cos(angle)
    sine = jnp.where(is_u, -jnp.sin(angle), jnp.sin(angle))

    def rotated(pre):
        wide = pre.astype(BF16).astype(F32)
        swapped = jnp.where(is_u, pltpu.roll(wide, 128 - quarter, 1), pltpu.roll(wide, quarter, 1))
        return wide * cosine + swapped * sine

    if line:
        spread_word()
    c_gain.wait_recv()
    c_tok.wait_recv()
    whole = jnp.concatenate([tok[0], tok[1]], axis=1).astype(F32)
    lines = gain.shape[1]
    wide_gain = [gain[0].astype(F32), gain[1].astype(F32)]
    flat_gain = jnp.concatenate(
        [side[i : i + 1, :] for side in wide_gain for i in range(lines)], axis=1
    )
    hid[...] = normed(whole, flat_gain)

    own_rows = pl.ds(pl.multiple_of(s * rows, rows), rows)

    def rows_of(owner):
        return pl.ds(pl.multiple_of(owner * rows, rows), rows)

    if n_sp == 4:
        peers_to = (s + 1 - 2 * parity, (s + 2) % 4, 3 - s)
        peers_from = peers_to
    else:
        peers_to = tuple((s + j) % n_sp for j in range(1, n_sp))
        peers_from = tuple((s + n_sp - j) % n_sp for j in range(1, n_sp))

    def rope_copy(owner, device):
        return remote(ropes.at[owner], ropes.at[owner], BLOCK, ROPE, device)

    def latent(owner, sent, slot, device):
        here = kv_lat.at[rows_of(owner)]
        return remote(here, here, sent, slot, device)

    base = STAGE + kv_turns + 1
    taken = LATENT
    c_own = latent(s, GATHER, taken, mate)
    order_to = list(enumerate(peers_to))
    if n_sp == 4:
        high = s // 2
        edge = 1 - (s + high) % 2
        order_to = [(1 + edge, 3 - 3 * high), (2 - edge, 2 - high), order_to[0]]
    gather_out = [latent(s, GATHER, base + j, {"sp": peer}) for j, peer in order_to]
    gather_in = [latent(owner, GATHER, base + j, mate) for j, owner in enumerate(peers_from)]
    passed = [latent(owner, PASS, taken, mate) for owner in peers_from]

    all_loaded(wkr, wpi)
    pool_in = mm(hid[...], wpi[...]).astype(BF16)
    halo_out[0] = pool_in[rows - 2 * RIM :, :].astype(F32)[RIM:, :]
    halo_out[1] = pool_in[: 2 * RIM, :].astype(F32)[:RIM, :]
    c_up = remote(halo_out.at[0], halo_in.at[0], SIDE_A, UP, above)
    c_dn = remote(halo_out.at[1], halo_in.at[1], SIDE_B, DOWN, below)
    c_gain.wait_send()
    c_tok.wait_send()
    pl.when(has_next)(c_up.start)
    pl.when(has_prev)(c_dn.start)

    @pl.when(q_core)
    def _():
        l_q.wait()
        for copies in q_out:
            start(copies)


    key_pre = mm_t(hid[...], wkr[...])
    key_rope = rotated(jnp.concatenate([key_pre, key_pre], axis=1))
    lower_half = lax.broadcasted_iota(jnp.int32, (half, 128), 1) < ROPE_DIM
    ropes[s] = jnp.where(lower_half, key_rope[:half], key_rope[half:]).astype(BF16)
    if line:
        hear_word()
    for peer in peers_to:
        copy = rope_copy(s, {"sp": peer})
        copy.start()

    @pl.when(kv_core)
    def _():
        for turn in range(kv_turns):
            all_taken(wkv_all, len(senders) * kv_rows, STAGE + turn)
            start(kv_on[turn])

    def no_rim(side):
        def clear():
            halo_in[side] = jnp.zeros(halo_in.shape[1:], F32)

        return clear

    pl.when(has_prev)(c_up.wait_recv)
    pl.when(has_next)(c_dn.wait_recv)
    pl.when(s == 0)(no_rim(0))
    pl.when(s == n_sp - 1)(no_rim(1))
    halo = jnp.concatenate([halo_in[0], halo_in[1]], axis=0).astype(BF16)
    padded = jnp.concatenate([pool_in, halo], axis=0)
    span = rows + 2 * RIM
    k_index = lax.broadcasted_iota(jnp.int32, (rows, span), 1)
    q_index = lax.broadcasted_iota(jnp.int32, (rows, span), 0)
    k_place = jnp.where(
        k_index < rows,
        k_index,
        jnp.where(k_index < rows + RIM, k_index - rows - RIM, k_index - RIM),
    )
    offset = k_place - q_index
    l_kvg.wait()
    l_qg.wait()
    all_loaded(mix, wop)
    inside = (k_place + s * rows >= 0) & (k_place + s * rows < length)
    pooled = []
    for g in range(groups):
        group = t * groups + g
        window = jnp.int32(0)
        for index, size in enumerate(WINDOWS):
            window = jnp.where(group == index, size, window)
        before = window // 2
        band = jnp.where(
            inside & (offset >= -before) & (offset < window - before), 1.0, 0.0
        )
        count = jnp.sum(band, axis=1, keepdims=True)
        cols = slice(g * POOL_GROUP, (g + 1) * POOL_GROUP)
        mean = (mm(band.astype(BF16), padded[:, cols]) / count).astype(BF16)
        spread = (mean.astype(F32) - pool_in[:, cols].astype(F32)).astype(BF16)
        pooled.append(mm(spread, mix[g]).astype(BF16))
    acc[...] = mm(jnp.concatenate(pooled, axis=1), wop[...])


    @pl.when(kv_core)
    def _():
        kv_sum = from_near(wkv_all)
        if hops:
            all_taken(wkv_all, depth, kv_last)
            kv_sum = kv_sum + from_shard(wkv_all, across)
        kv_lat[own_rows] = normed(kv_sum.astype(BF16).astype(F32), kvg[...])
        start(gather_out + [c_own])

    @pl.when(q_core)
    def _():
        for turn in turns:
            all_taken(wq_all, len(senders) * sizes[turn], STAGE + turn)
            start(q_on[turn])

    def finish_rope(owner):
        here = rows_of(owner)
        packed = ropes[owner].astype(F32)
        swapped = pltpu.roll(packed, ROPE_DIM, 1)
        low = jnp.where(lower_half, packed, swapped)
        high = jnp.where(lower_half, swapped, packed)
        kcat[here, kv_rank:] = jnp.concatenate([low, high], axis=0).astype(BF16)

    all_taken(ropes, n_sp - 1, ROPE)
    all_sent(ropes, n_sp - 1, BLOCK)
    for owner in (s,) + peers_from:
        finish_rope(owner)

    c_lat = remote(q_lat, q_lat, GATHER, LATENT, mate)
    lat_parts = [q_lat.at[pl.ds(part * half, half)] for part in range(2)]

    @pl.when(kv_core)
    def _():
        for j in range(n_sp - 1):
            gather_in[j].wait_recv()
            passed[j].start()
        c_lat.wait_recv()

    @pl.when(q_core)
    def _():
        q_part[...] = from_near(wq_all)
        if hops:
            all_taken(wq_all, depth, q_last)
        q_sum = q_part[...]
        if hops:
            q_sum = q_sum + from_shard(wq_all, across)
        for part, piece in enumerate(lat_parts):
            some = q_sum[part * half : (part + 1) * half].astype(BF16).astype(F32)
            piece[...] = normed(some, qg[...])
            remote(piece, piece, GATHER, LATENT, mate).start()

    q_latent = q_lat[...]
    all_loaded(wqn, wqr, wku, wvu)
    l_oa.wait()
    q_nope = mm(q_latent, wqn[...]).astype(BF16)
    q_pre = mm(q_latent, wqr[...])
    low_lanes = lane < ROPE_DIM
    for h in range(heads):
        cols = slice(h * NOPE_DIM, (h + 1) * NOPE_DIM)
        absorbed = mm_t(q_nope[:, cols], wku[:, cols]).astype(BF16)
        if h % 2 == 0:
            turned = rotated(q_pre[:, h * ROPE_DIM : (h + 2) * ROPE_DIM])
        rope = jnp.where(low_lanes if h % 2 == 0 else ~low_lanes, turned, 0.0).astype(BF16)
        for part in range(2):
            piece = slice(part * half, (part + 1) * half)
            qcat[part, h * half : (h + 1) * half, :kv_rank] = absorbed[piece]
            qcat[part, h * half : (h + 1) * half, kv_rank:] = rope[piece]

    factor = (NOPE_DIM + ROPE_DIM) ** (-0.5) * math.log2(math.e)
    span_keys = rows * max(
        c for c in range(1, n_sp + 1) if n_sp % c == 0 and (c == 1 or rows * c <= SPAN_LIMIT)
    )
    spans = length // span_keys
    block = 4 * half

    @pl.when(q_core)
    def _():
        all_taken(kv_lat, n_sp * rows, LATENT)

    kcat[:, :kv_rank] = kv_lat[...]

    def scored(part, first, keys):
        return mm_t(qcat[part, pl.ds(first, block), :], keys)

    def weighed(scores, keys, state):
        top = jnp.max(scores, axis=1, keepdims=True)
        if state is not None:
            top = jnp.maximum(top, state[0])
        weights = jnp.exp2((scores - top) * factor)
        total = jnp.sum(weights, axis=1, keepdims=True)
        summed = mm(weights.astype(BF16), keys[:, :kv_rank])
        if state is not None:
            shrink = jnp.exp2((state[0] - top) * factor)
            total = total + state[1] * shrink
            summed = summed + state[2] * shrink
        return top, total, summed

    part_rows = heads * half
    blocks = part_rows // block

    def keep(order, index, state):
        ctx[pl.ds(order * part_rows + index * block, block), :] = (state[2] / state[1]).astype(BF16)

    def attended(order):
        pieces = []
        for h in range(heads):
            mixed_latent = ctx[pl.ds(order * part_rows + h * half, half), :]
            cols = slice(h * VALUE_DIM, (h + 1) * VALUE_DIM)
            pieces.append(mm(mixed_latent, wvu[:, cols]).astype(BF16))
        return jnp.concatenate(pieces, axis=1)

    def projected(features, part, side):
        cols = slice(side * side_width, (side + 1) * side_width)
        own = acc[pl.ds(pl.multiple_of(part * half, half), half), cols]
        return own + mm(features, woa[:, cols])

    parts = (1 - t, t)
    side_width = share.shape[2]
    shares = [
        remote(share.at[side], arrived.at[side], BLOCK, SHARE, mate) for side in range(2)
    ]
    c_share = remote(share, arrived, BLOCK, SHARE, mate)

    def give():
        features = attended(0)
        for side in range(2):
            share[side] = projected(features, parts[0], side).astype(BF16)
            shares[side].start()

    if spans == 1:
        jobs = [(order, index) for order in range(2) for index in range(blocks)]
        ahead = scored(parts[0], 0, kcat[...])
        for i, (order, index) in enumerate(jobs):
            scores = ahead
            if i + 1 < len(jobs):
                later, place_of = jobs[i + 1]
                ahead = scored(parts[later], place_of * block, kcat[...])
            keep(order, index, weighed(scores, kcat[...], None))
            if i == blocks:
                give()
    else:
        for order in range(2):

            def one_block(index, carry):
                first = pl.multiple_of(index * block, block)

                def step(i, state):
                    start_key = pl.multiple_of(i * span_keys, span_keys)
                    keys = kcat[pl.ds(start_key, span_keys), :]
                    return weighed(scored(parts[order], first, keys), keys, state)

                keys = kcat[:span_keys, :]
                state = weighed(scored(parts[order], first, keys), keys, None)
                state = lax.fori_loop(1, spans, step, state)
                row = pl.multiple_of(order * part_rows + first, block)
                ctx[pl.ds(row, block), :] = (state[2] / state[1]).astype(BF16)
                return carry

            lax.fori_loop(0, blocks, one_block, 0, unroll=True)
            if order == 0:
                give()
    features = attended(1)
    mine = [projected(features, parts[1], side) for side in range(2)]
    c_share.wait()
    for side in range(2):
        cols = slice(side * side_width, (side + 1) * side_width)
        out[0, :, cols] = (mine[side] + arrived[side].astype(F32)).astype(BF16)
    pl.when(has_next)(c_up.wait_send)
    pl.when(has_prev)(c_dn.wait_send)

    @pl.when(kv_core)
    def _():
        all_sent(wkv_all, (n_fs - 1) * depth, MAIN)
        all_sent(kv_lat, n_sp * rows, GATHER)
        all_sent(kv_lat, (n_sp - 1) * rows, PASS)

    @pl.when(q_core)
    def _():
        all_sent(wq_all, (n_fs - 1) * depth, MAIN)
        c_lat.wait_send()


def solution(mesh):
    n_sp, n_fs = mesh.shape["sp"], mesh.shape["fs"]

    def on_device(*args):
        args = list(args)
        args[1] = args[1].reshape(-1, 128)
        for i in (3, 7):
            args[i] = args[i].reshape(1, -1)
        args[10] = args[10].T
        (tokens, gain, wqd, qg, wqn, wqr, wkvd, kvg, wku, wvu, wkr, wpi, mix, woa, wop) = args
        rows, cols = tokens.shape[1:]
        half = rows // 2
        heads = wqn.shape[1] // NOPE_DIM
        kv_rank = wkvd.shape[1]
        q_rank = wqd.shape[1]
        d_model = woa.shape[1]
        groups = wpi.shape[1] // POOL_GROUP

        def vmem(*shape, kind=BF16):
            return pltpu.VMEM(shape, kind)

        def same(array):
            return pltpu.VMEM(array.shape, array.dtype)

        dma = pltpu.SemaphoreType.DMA
        return pl.pallas_call(
            functools.partial(layer, n_sp, n_fs),
            out_shape=pltpu.VMEM((1, half, d_model), BF16),
            in_specs=[pl.BlockSpec(memory_space=pltpu.HBM)] * len(args),
            out_specs=pl.BlockSpec(memory_space=pltpu.VMEM),
            scratch_shapes=[
                vmem(2, rows, cols),
                vmem(2, cols // 128, 128),
                vmem(rows, 2 * cols),
                vmem(n_fs * wqd.shape[0], q_rank),
                vmem(n_fs * wkvd.shape[0], kv_rank),
                same(qg),
                same(kvg),
                same(wqn),
                same(wqr),
                same(wku),
                same(wvu),
                same(wkr),
                same(wpi),
                vmem(groups, POOL_GROUP, POOL_GROUP),
                same(woa),
                same(wop),
                vmem(2, RIM, wpi.shape[1], kind=F32),
                vmem(2, RIM, wpi.shape[1], kind=F32),
                vmem(rows, q_rank, kind=F32),
                vmem(rows, q_rank),
                vmem(n_sp * rows, kv_rank),
                vmem(n_sp, half, 2 * ROPE_DIM),
                vmem(n_sp * rows, kv_rank + 2 * ROPE_DIM),
                vmem(2, heads * half, kv_rank + 2 * ROPE_DIM),
                vmem(2 * heads * half, kv_rank),
                vmem(rows, d_model, kind=F32),
                vmem(2, half, d_model // 2),
                vmem(2, half, d_model // 2),
                dma((9,)),
                dma((6,)),
                dma((STAGE + max(6, n_sp + 2),)),
                pltpu.SemaphoreType.REGULAR((2,)),
            ],
            compiler_params=pltpu.CompilerParams(collective_id=0, has_side_effects=True, vmem_limit_bytes=40 * 1024 * 1024),
        )(*[pltpu.with_memory_space_constraint(a, pltpu.HBM) for a in args])

    placed = (
        P("fs", "sp", "tp"),
        P("tp"),
        P("fs", None),
        P(),
        P(None, "tp"),
        P(None, "tp"),
        P("fs", None),
        P(),
        P(None, "tp"),
        P(None, "tp"),
        P(),
        P(None, "tp"),
        P(),
        P("tp", None),
        P("tp", None),
    )
    return jax.shard_map(
        on_device,
        mesh=mesh,
        in_specs=placed,
        out_specs=P("fs", ("sp", "tp"), None),
        check_vma=False,
    )
```

```python
import functools
import math

import jax
import jax.numpy as jnp
from jax import lax
from jax.experimental import pallas as pl
from jax.experimental.pallas import tpu as pltpu
from jax.sharding import PartitionSpec as P

NOPE_DIM = 128
ROPE_DIM = 64
VALUE_DIM = 128
GRID_W = 64
POOL_GROUP = 256
EPS = 1e-06
THETA = 10000.0
WINDOWS = (2, 4, 8, 16)
RIM = 8
SPAN_LIMIT = 1024
F32 = jnp.float32
BF16 = jnp.bfloat16
MESH = pl.DeviceIdType.MESH
TOK, GAIN, UP, DOWN, LATENT, SHARE, ROPE, STAGE = range(8)
MAIN, GATHER, PASS, BLOCK, SIDE_A, SIDE_B = range(6)


def mm(a, b):
    return jnp.dot(a, b, preferred_element_type=F32)


def mm_t(a, b):
    return lax.dot_general(a, b, (((1,), (1,)), ((), ())), preferred_element_type=F32)


def normed(wide, gain):
    scale = lax.rsqrt(jnp.mean(wide * wide, axis=-1, keepdims=True) + EPS)
    return (wide * scale * gain).astype(BF16)


def layer(
    n_sp,
    n_fs,
    tokens,
    norm_gain,
    w_q_down,
    q_gain,
    w_q_nope,
    w_q_rope,
    w_kv_down,
    kv_gain,
    w_k_up,
    w_v_up,
    w_k_rope,
    w_pool_in,
    w_pool_mix,
    w_out_attn,
    w_out_pool,
    out,
    tok,
    gain,
    hid,
    wq_all,
    wkv_all,
    qg,
    kvg,
    wqn,
    wqr,
    wku,
    wvu,
    wkr,
    wpi,
    mix,
    woa,
    wop,
    halo_out,
    halo_in,
    q_part,
    q_first,
    q_lat,
    kv_lat,
    ropes,
    kcat,
    qcat,
    ctx,
    acc,
    share,
    arrived,
    local_sem,
    send_sem,
    recv_sem,
    word,
):
    s = lax.axis_index("sp")
    f = lax.axis_index("fs")
    t = lax.axis_index("tp")
    rows = tok.shape[1]
    half = rows // 2
    depth = w_q_down.shape[0]
    kv_rank = wkv_all.shape[1]
    kv_core, q_core = t == 1, t == 0
    heads = wqn.shape[1] // NOPE_DIM
    groups = wpi.shape[1] // POOL_GROUP
    length = rows * n_sp

    def down(ref, owner, first=0, size=depth):
        start = pl.multiple_of(owner * depth + first, 16)
        return ref.at[pl.ds(start, size), :]

    pairs = (
        (w_kv_down, down(wkv_all, f)),
        (tokens.at[0], tok.at[t]),
        (norm_gain, gain.at[t]),
        (w_q_down, down(wq_all, f)),
        (w_k_rope, wkr),
        (w_pool_in, wpi),
        (kv_gain, kvg),
        (q_gain, qg),
        (w_pool_mix.at[pl.ds(t * groups, groups)], mix),
        (w_out_pool, wop),
        (w_q_nope, wqn),
        (w_q_rope, wqr),
        (w_k_up, wku),
        (w_v_up, wvu),
        (w_out_attn, woa),
    )
    slots = (0, 1, 2, 0, 3, 3, 4, 5, 6, 6, 7, 7, 7, 7, 8)
    loads = [
        pltpu.make_async_copy(src, dst, local_sem.at[slot])
        for slot, (src, dst) in zip(slots, pairs)
    ]
    (
        l_kv,
        l_tok,
        l_gain,
        l_q,
        l_kr,
        l_pi,
        l_kvg,
        l_qg,
        l_mix,
        l_op,
        l_qn,
        l_qr,
        l_ku,
        l_vu,
        l_oa,
    ) = loads
    for load in loads:
        if load is l_kv:
            pl.when(kv_core)(load.start)
        elif load is l_q:
            pl.when(q_core)(load.start)
        else:
            load.start()

    barrier = pltpu.get_barrier_semaphore()

    def greet(device):
        pl.semaphore_signal(barrier, inc=1, device_id=device, device_id_type=MESH)

    hops = n_fs == 4
    line = hops and n_sp == 4
    has_prev, has_next = s > 0, s < n_sp - 1
    mate = {"tp": 1 - t}
    above, below = {"sp": (s + 1) % n_sp}, {"sp": (s + n_sp - 1) % n_sp}
    parity = s % 2
    if hops:
        near = f + 1 - 2 * (f % 2)
        far = (f + 2) % 4
        across = 3 - f
    greet(mate)
    if line:
        greet({"fs": near})
        greet({"fs": far})
        pl.when(has_next)(lambda: greet(above))
        pl.when(has_prev)(lambda: greet(below))
        guests = 5 - (s == 0).astype(jnp.int32) - (s == n_sp - 1).astype(jnp.int32)
    else:
        for j in range(1, n_fs):
            greet({"fs": (f + j) % n_fs})
        for j in range(1, n_sp):
            greet({"sp": (s + j) % n_sp})
        guests = n_sp + n_fs - 1
    pl.semaphore_wait(barrier, guests)

    def tell(side, device):
        pl.semaphore_signal(word.at[side], inc=1, device_id=device, device_id_type=MESH)

    def hear(side, count):
        return lambda: pl.semaphore_wait(word.at[side], count)

    if line:

        def both_ways():
            tell(0, above)
            tell(1, below)

        pl.when(has_prev & has_next)(both_ways)

    def spread_word():
        def up():
            hear(0, 1)()
            tell(0, above)

        def down_():
            hear(1, 1)()
            tell(1, below)

        pl.when(s == n_sp - 2)(up)
        pl.when(s == 1)(down_)

    def hear_word():
        pl.when(s == n_sp - 1)(hear(0, 2))
        pl.when(s == 0)(hear(1, 2))

    def remote(src, dst, sent, slot, device):
        return pltpu.make_async_remote_copy(
            src_ref=src,
            dst_ref=dst,
            send_sem=send_sem.at[sent],
            recv_sem=recv_sem.at[slot],
            device_id=device,
            device_id_type=MESH,
        )

    def part_of(ref, count):
        return ref.at[pl.ds(0, count)]

    def all_sent(ref, count, sent):
        part = part_of(ref, count)
        remote(part, part, sent, TOK, mate).wait_send()

    def all_taken(ref, count, slot):
        part = part_of(ref, count)
        remote(part, part, MAIN, slot, mate).wait_recv()

    def all_loaded(*refs):
        slot = {id(ref): i for ref, i in zip((dst for _, dst in pairs), slots)}[id(refs[0])]
        line_bytes = 2 * woa.shape[1]
        total = sum(math.prod(ref.shape) * ref.dtype.itemsize for ref in refs)
        part = part_of(woa, total // line_bytes)
        pltpu.make_async_copy(part, part, local_sem.at[slot]).wait()

    sizes = (depth // 4,) * 3 + (depth // 8,) * 2
    places = tuple(sum(sizes[:turn]) for turn in range(len(sizes)))
    kv_turns = 2
    kv_rows = depth // kv_turns
    if hops:
        partners = senders = (near, far)
    else:
        partners = tuple((f + j) % n_fs for j in range(1, n_fs))
        senders = tuple((f + n_fs - j) % n_fs for j in range(1, n_fs))
    turns = range(len(sizes))

    def outgoing(ref, slot, first, size):
        part = down(ref, f, first, size)
        return [remote(part, part, MAIN, slot, {"fs": peer}) for peer in partners]

    def onward(ref, slot, first, size, core):
        piece = size // 2
        low, high = down(ref, near, first, piece), down(ref, far, first + piece, piece)
        return [
            remote(low, low, MAIN, slot, {"fs": far, "tp": core}),
            remote(high, high, MAIN, slot, {"fs": near, "tp": core}),
        ]

    def start(copies):
        for copy in copies:
            copy.start()

    kv_out = [
        outgoing(wkv_all, STAGE + turn, turn * kv_rows, kv_rows) for turn in range(kv_turns)
    ]
    q_out = [outgoing(wq_all, STAGE + turn, places[turn], sizes[turn]) for turn in turns]
    kv_last, lat_slot = STAGE + kv_turns, STAGE + len(sizes)
    q_last = STAGE + max(len(sizes) + 1, kv_turns + n_sp)
    if hops:
        kv_on = [
            onward(wkv_all, kv_last, turn * kv_rows, kv_rows, t) for turn in range(kv_turns)
        ]
        q_on = [onward(wq_all, q_last, places[turn], sizes[turn], 1 - t) for turn in turns]
    else:
        kv_on = [[] for turn in range(kv_turns)]
        q_on = [[] for turn in turns]

    def from_shard(ref, owner):
        first = pl.multiple_of(owner * depth, depth)
        return mm(hid[:, pl.ds(first, depth)], ref[pl.ds(first, depth), :])

    def from_near(ref):
        return functools.reduce(jnp.add, [from_shard(ref, owner) for owner in (f,) + senders])

    @pl.when(kv_core)
    def _():
        l_kv.wait()
        for copies in kv_out:
            start(copies)

    l_tok.wait()
    l_gain.wait()
    c_tok = remote(tok.at[t], tok.at[t], SIDE_A, TOK, mate)
    c_tok.start()
    c_gain = remote(gain.at[t], gain.at[t], SIDE_B, GAIN, mate)
    c_gain.start()
    lane = lax.broadcasted_iota(jnp.int32, (rows, 128), 1)
    place = s * rows + lax.broadcasted_iota(jnp.int32, (rows, 128), 0)
    quarter = ROPE_DIM // 4
    power = (lane % quarter).astype(F32) * (2.0 / (ROPE_DIM // 2))
    inverse = jnp.exp(power * (-math.log(THETA)))
    grid_row = place // GRID_W
    grid_col = place - grid_row * GRID_W
    in_a = (lane % ROPE_DIM) < (ROPE_DIM // 2)
    angle = jnp.where(in_a, grid_row, grid_col).astype(F32) * inverse
    is_u = (lane % (2 * quarter)) < quarter
    cosine = jnp.cos(angle)
    sine = jnp.where(is_u, -jnp.sin(angle), jnp.sin(angle))

    def rotated(pre):
        wide = pre.astype(BF16).astype(F32)
        swapped = jnp.where(is_u, pltpu.roll(wide, 128 - quarter, 1), pltpu.roll(wide, quarter, 1))
        return wide * cosine + swapped * sine

    if line:
        spread_word()
    c_gain.wait_recv()
    c_tok.wait_recv()
    whole = jnp.concatenate([tok[0], tok[1]], axis=1).astype(F32)
    lines = gain.shape[1]
    wide_gain = [gain[0].astype(F32), gain[1].astype(F32)]
    flat_gain = jnp.concatenate(
        [side[i : i + 1, :] for side in wide_gain for i in range(lines)], axis=1
    )
    hid[...] = normed(whole, flat_gain)

    own_rows = pl.ds(pl.multiple_of(s * rows, rows), rows)

    def rows_of(owner):
        return pl.ds(pl.multiple_of(owner * rows, rows), rows)

    if n_sp == 4:
        peers_to = (s + 1 - 2 * parity, (s + 2) % 4, 3 - s)
        peers_from = peers_to
    else:
        peers_to = tuple((s + j) % n_sp for j in range(1, n_sp))
        peers_from = tuple((s + n_sp - j) % n_sp for j in range(1, n_sp))

    def rope_copy(owner, device):
        return remote(ropes.at[owner], ropes.at[owner], BLOCK, ROPE, device)

    def latent(owner, sent, slot, device):
        here = kv_lat.at[rows_of(owner)]
        return remote(here, here, sent, slot, device)

    base = STAGE + kv_turns + 1
    taken = LATENT
    c_own = latent(s, GATHER, taken, mate)
    order_to = list(enumerate(peers_to))
    if n_sp == 4:
        high = s // 2
        edge = 1 - (s + high) % 2
        order_to = [(1 + edge, 3 - 3 * high), (2 - edge, 2 - high), order_to[0]]
    gather_out = [latent(s, GATHER, base + j, {"sp": peer}) for j, peer in order_to]
    gather_in = [latent(owner, GATHER, base + j, mate) for j, owner in enumerate(peers_from)]
    passed = [latent(owner, PASS, taken, mate) for owner in peers_from]

    all_loaded(wkr, wpi)
    pool_in = mm(hid[...], wpi[...]).astype(BF16)
    halo_out[0] = pool_in[rows - 2 * RIM :, :].astype(F32)[RIM:, :]
    halo_out[1] = pool_in[: 2 * RIM, :].astype(F32)[:RIM, :]
    c_up = remote(halo_out.at[0], halo_in.at[0], SIDE_A, UP, above)
    c_dn = remote(halo_out.at[1], halo_in.at[1], SIDE_B, DOWN, below)
    c_gain.wait_send()
    c_tok.wait_send()
    pl.when(has_next)(c_up.start)
    pl.when(has_prev)(c_dn.start)

    @pl.when(q_core)
    def _():
        l_q.wait()
        for copies in q_out:
            start(copies)


    key_pre = mm_t(hid[...], wkr[...])
    key_rope = rotated(jnp.concatenate([key_pre, key_pre], axis=1))
    lower_half = lax.broadcasted_iota(jnp.int32, (half, 128), 1) < ROPE_DIM
    ropes[s] = jnp.where(lower_half, key_rope[:half], key_rope[half:]).astype(BF16)
    if line:
        hear_word()
    for peer in peers_to:
        copy = rope_copy(s, {"sp": peer})
        copy.start()

    @pl.when(kv_core)
    def _():
        for turn in range(kv_turns):
            all_taken(wkv_all, len(senders) * kv_rows, STAGE + turn)
            start(kv_on[turn])

    def no_rim(side):
        def clear():
            halo_in[side] = jnp.zeros(halo_in.shape[1:], F32)

        return clear

    pl.when(has_prev)(c_up.wait_recv)
    pl.when(has_next)(c_dn.wait_recv)
    pl.when(s == 0)(no_rim(0))
    pl.when(s == n_sp - 1)(no_rim(1))
    halo = jnp.concatenate([halo_in[0], halo_in[1]], axis=0).astype(BF16)
    padded = jnp.concatenate([pool_in, halo], axis=0)
    span = rows + 2 * RIM
    k_index = lax.broadcasted_iota(jnp.int32, (rows, span), 1)
    q_index = lax.broadcasted_iota(jnp.int32, (rows, span), 0)
    k_place = jnp.where(
        k_index < rows,
        k_index,
        jnp.where(k_index < rows + RIM, k_index - rows - RIM, k_index - RIM),
    )
    offset = k_place - q_index
    l_kvg.wait()
    l_qg.wait()
    all_loaded(mix, wop)
    inside = (k_place + s * rows >= 0) & (k_place + s * rows < length)
    pooled = []
    for g in range(groups):
        group = t * groups + g
        window = jnp.int32(0)
        for index, size in enumerate(WINDOWS):
            window = jnp.where(group == index, size, window)
        before = window // 2
        band = jnp.where(
            inside & (offset >= -before) & (offset < window - before), 1.0, 0.0
        )
        count = jnp.sum(band, axis=1, keepdims=True)
        cols = slice(g * POOL_GROUP, (g + 1) * POOL_GROUP)
        mean = (mm(band.astype(BF16), padded[:, cols]) / count).astype(BF16)
        spread = (mean.astype(F32) - pool_in[:, cols].astype(F32)).astype(BF16)
        pooled.append(mm(spread, mix[g]).astype(BF16))
    pl.when(has_next)(c_up.wait_send)
    pl.when(has_prev)(c_dn.wait_send)
    acc[...] = mm(jnp.concatenate(pooled, axis=1), wop[...])


    @pl.when(kv_core)
    def _():
        kv_sum = from_near(wkv_all)
        if hops:
            all_taken(wkv_all, depth, kv_last)
            kv_sum = kv_sum + from_shard(wkv_all, across)
        kv_lat[own_rows] = normed(kv_sum.astype(BF16).astype(F32), kvg[...])
        start(gather_out + [c_own])

    @pl.when(q_core)
    def _():
        for turn in turns:
            all_taken(wq_all, len(senders) * sizes[turn], STAGE + turn)
            start(q_on[turn])

    def finish_rope(owner):
        here = rows_of(owner)
        packed = ropes[owner].astype(F32)
        swapped = pltpu.roll(packed, ROPE_DIM, 1)
        low = jnp.where(lower_half, packed, swapped)
        high = jnp.where(lower_half, swapped, packed)
        kcat[here, kv_rank:] = jnp.concatenate([low, high], axis=0).astype(BF16)

    all_taken(ropes, n_sp - 1, ROPE)
    all_sent(ropes, n_sp - 1, BLOCK)
    for owner in (s,) + peers_from:
        finish_rope(owner)

    c_first = remote(q_part, q_first, GATHER, LATENT, mate)
    c_lat = remote(q_lat, q_lat, SIDE_A, lat_slot, mate)
    lat_parts = [q_lat.at[pl.ds(part * half, half)] for part in range(2)]

    def pass_on(j):
        gather_in[j].wait_recv()
        passed[j].start()

    @pl.when(kv_core)
    def _():
        for j in range(n_sp - 3):
            pass_on(j)
        c_first.wait_recv()
        q_sum = q_first[...]
        if hops:
            all_taken(wq_all, depth, q_last)
            q_sum = q_sum + from_shard(wq_all, across)
        for part, piece in enumerate(lat_parts):
            some = q_sum[part * half : (part + 1) * half].astype(BF16).astype(F32)
            piece[...] = normed(some, qg[...])
            remote(piece, piece, SIDE_A, lat_slot, mate).start()
        for j in range(n_sp - 3, n_sp - 1):
            pass_on(j)

    @pl.when(q_core)
    def _():
        q_part[...] = from_near(wq_all)
        c_first.start()
        c_lat.wait_recv()

    q_latent = q_lat[...]
    all_loaded(wqn, wqr, wku, wvu)
    l_oa.wait()
    q_nope = mm(q_latent, wqn[...]).astype(BF16)
    q_pre = mm(q_latent, wqr[...])
    low_lanes = lane < ROPE_DIM
    for h in range(heads):
        cols = slice(h * NOPE_DIM, (h + 1) * NOPE_DIM)
        absorbed = mm_t(q_nope[:, cols], wku[:, cols]).astype(BF16)
        if h % 2 == 0:
            turned = rotated(q_pre[:, h * ROPE_DIM : (h + 2) * ROPE_DIM])
        rope = jnp.where(low_lanes if h % 2 == 0 else ~low_lanes, turned, 0.0).astype(BF16)
        for part in range(2):
            piece = slice(part * half, (part + 1) * half)
            qcat[part, h * half : (h + 1) * half, :kv_rank] = absorbed[piece]
            qcat[part, h * half : (h + 1) * half, kv_rank:] = rope[piece]

    factor = (NOPE_DIM + ROPE_DIM) ** (-0.5) * math.log2(math.e)
    span_keys = rows * max(
        c for c in range(1, n_sp + 1) if n_sp % c == 0 and (c == 1 or rows * c <= SPAN_LIMIT)
    )
    spans = length // span_keys
    block = 4 * half

    @pl.when(q_core)
    def _():
        all_taken(kv_lat, n_sp * rows, LATENT)

    kcat[:, :kv_rank] = kv_lat[...]

    def scored(part, first, keys):
        return mm_t(qcat[part, pl.ds(first, block), :], keys)

    def weighed(scores, keys, state):
        top = jnp.max(scores, axis=1, keepdims=True)
        if state is not None:
            top = jnp.maximum(top, state[0])
        weights = jnp.exp2((scores - top) * factor)
        total = jnp.sum(weights, axis=1, keepdims=True)
        summed = mm(weights.astype(BF16), keys[:, :kv_rank])
        if state is not None:
            shrink = jnp.exp2((state[0] - top) * factor)
            total = total + state[1] * shrink
            summed = summed + state[2] * shrink
        return top, total, summed

    part_rows = heads * half
    blocks = part_rows // block

    def keep(order, index, state):
        ctx[pl.ds(order * part_rows + index * block, block), :] = (state[2] / state[1]).astype(BF16)

    def attended(order):
        pieces = []
        for h in range(heads):
            mixed_latent = ctx[pl.ds(order * part_rows + h * half, half), :]
            cols = slice(h * VALUE_DIM, (h + 1) * VALUE_DIM)
            pieces.append(mm(mixed_latent, wvu[:, cols]).astype(BF16))
        return jnp.concatenate(pieces, axis=1)

    def projected(features, part):
        own = acc[pl.ds(pl.multiple_of(part * half, half), half), :]
        return own + mm(features, woa[...])

    parts = (1 - t, t)
    c_share = remote(share, arrived, BLOCK, SHARE, mate)

    def give():
        share[...] = projected(attended(0), parts[0]).astype(BF16)
        c_share.start()

    if spans == 1:
        jobs = [(order, index) for order in range(2) for index in range(blocks)]
        ahead = scored(parts[0], 0, kcat[...])
        for i, (order, index) in enumerate(jobs):
            scores = ahead
            if i + 1 < len(jobs):
                later, place_of = jobs[i + 1]
                ahead = scored(parts[later], place_of * block, kcat[...])
            keep(order, index, weighed(scores, kcat[...], None))
            if i == blocks:
                give()
    else:
        for order in range(2):

            def one_block(index, carry):
                first = pl.multiple_of(index * block, block)

                def step(i, state):
                    start_key = pl.multiple_of(i * span_keys, span_keys)
                    keys = kcat[pl.ds(start_key, span_keys), :]
                    return weighed(scored(parts[order], first, keys), keys, state)

                keys = kcat[:span_keys, :]
                state = weighed(scored(parts[order], first, keys), keys, None)
                state = lax.fori_loop(1, spans, step, state)
                row = pl.multiple_of(order * part_rows + first, block)
                ctx[pl.ds(row, block), :] = (state[2] / state[1]).astype(BF16)
                return carry

            lax.fori_loop(0, blocks, one_block, 0, unroll=True)
            if order == 0:
                give()
    mine = projected(attended(1), parts[1])
    c_share.wait()
    out[0] = (mine + arrived[...].astype(F32)).astype(BF16)

    @pl.when(kv_core)
    def _():
        all_sent(wkv_all, (n_fs - 1) * depth, MAIN)
        all_sent(kv_lat, n_sp * rows, GATHER)
        all_sent(kv_lat, (n_sp - 1) * rows, PASS)
        c_lat.wait_send()

    @pl.when(q_core)
    def _():
        all_sent(wq_all, (n_fs - 1) * depth, MAIN)
        c_first.wait_send()


def solution(mesh):
    n_sp, n_fs = mesh.shape["sp"], mesh.shape["fs"]

    def on_device(*args):
        args = list(args)
        args[1] = args[1].reshape(-1, 128)
        for i in (3, 7):
            args[i] = args[i].reshape(1, -1)
        args[10] = args[10].T
        (tokens, gain, wqd, qg, wqn, wqr, wkvd, kvg, wku, wvu, wkr, wpi, mix, woa, wop) = args
        rows, cols = tokens.shape[1:]
        half = rows // 2
        heads = wqn.shape[1] // NOPE_DIM
        kv_rank = wkvd.shape[1]
        q_rank = wqd.shape[1]
        d_model = woa.shape[1]
        groups = wpi.shape[1] // POOL_GROUP

        def vmem(*shape, kind=BF16):
            return pltpu.VMEM(shape, kind)

        def same(array):
            return pltpu.VMEM(array.shape, array.dtype)

        dma = pltpu.SemaphoreType.DMA
        return pl.pallas_call(
            functools.partial(layer, n_sp, n_fs),
            out_shape=pltpu.VMEM((1, half, d_model), BF16),
            in_specs=[pl.BlockSpec(memory_space=pltpu.HBM)] * len(args),
            out_specs=pl.BlockSpec(memory_space=pltpu.VMEM),
            scratch_shapes=[
                vmem(2, rows, cols),
                vmem(2, cols // 128, 128),
                vmem(rows, 2 * cols),
                vmem(n_fs * wqd.shape[0], q_rank),
                vmem(n_fs * wkvd.shape[0], kv_rank),
                same(qg),
                same(kvg),
                same(wqn),
                same(wqr),
                same(wku),
                same(wvu),
                same(wkr),
                same(wpi),
                vmem(groups, POOL_GROUP, POOL_GROUP),
                same(woa),
                same(wop),
                vmem(2, RIM, wpi.shape[1], kind=F32),
                vmem(2, RIM, wpi.shape[1], kind=F32),
                vmem(rows, q_rank, kind=F32),
                vmem(rows, q_rank, kind=F32),
                vmem(rows, q_rank),
                vmem(n_sp * rows, kv_rank),
                vmem(n_sp, half, 2 * ROPE_DIM),
                vmem(n_sp * rows, kv_rank + 2 * ROPE_DIM),
                vmem(2, heads * half, kv_rank + 2 * ROPE_DIM),
                vmem(2 * heads * half, kv_rank),
                vmem(rows, d_model, kind=F32),
                vmem(half, d_model),
                vmem(half, d_model),
                dma((9,)),
                dma((6,)),
                dma((STAGE + max(6, n_sp + 2) + 1,)),
                pltpu.SemaphoreType.REGULAR((2,)),
            ],
            compiler_params=pltpu.CompilerParams(collective_id=0, has_side_effects=True, vmem_limit_bytes=40 * 1024 * 1024),
        )(*[pltpu.with_memory_space_constraint(a, pltpu.HBM) for a in args])

    placed = (
        P("fs", "sp", "tp"),
        P("tp"),
        P("fs", None),
        P(),
        P(None, "tp"),
        P(None, "tp"),
        P("fs", None),
        P(),
        P(None, "tp"),
        P(None, "tp"),
        P(),
        P(None, "tp"),
        P(),
        P("tp", None),
        P("tp", None),
    )
    return jax.shard_map(
        on_device,
        mesh=mesh,
        in_specs=placed,
        out_specs=P("fs", ("sp", "tp"), None),
        check_vma=False,
    )
```

```python
import functools
import math

import jax
import jax.numpy as jnp
from jax import lax
from jax.experimental import pallas as pl
from jax.experimental.pallas import tpu as pltpu
from jax.sharding import PartitionSpec as P

NOPE_DIM = 128
ROPE_DIM = 64
VALUE_DIM = 128
GRID_W = 64
POOL_GROUP = 256
EPS = 1e-06
THETA = 10000.0
WINDOWS = (2, 4, 8, 16)
RIM = 8
SPAN_LIMIT = 1024
F32 = jnp.float32
BF16 = jnp.bfloat16
MESH = pl.DeviceIdType.MESH
TOK, GAIN, UP, DOWN, LATENT, SHARE, ROPE, STAGE = range(8)
MAIN, GATHER, PASS, BLOCK, SIDE_A, SIDE_B = range(6)


def mm(a, b):
    return jnp.dot(a, b, preferred_element_type=F32)


def mm_t(a, b):
    return lax.dot_general(a, b, (((1,), (1,)), ((), ())), preferred_element_type=F32)


def normed(wide, gain):
    scale = lax.rsqrt(jnp.mean(wide * wide, axis=-1, keepdims=True) + EPS)
    return (wide * scale * gain).astype(BF16)


def layer(
    n_sp,
    n_fs,
    tokens,
    norm_gain,
    w_q_down,
    q_gain,
    w_q_nope,
    w_q_rope,
    w_kv_down,
    kv_gain,
    w_k_up,
    w_v_up,
    w_k_rope,
    w_pool_in,
    w_pool_mix,
    w_out_attn,
    w_out_pool,
    out,
    tok,
    gain,
    hid,
    wq_all,
    wkv_all,
    qg,
    kvg,
    wqn,
    wqr,
    wku,
    wvu,
    wkr,
    wpi,
    mix,
    woa,
    wop,
    halo_out,
    halo_in,
    q_part,
    q_first,
    q_lat,
    kv_lat,
    ropes,
    kcat,
    qcat,
    ctx,
    acc,
    share,
    arrived,
    local_sem,
    send_sem,
    recv_sem,
    word,
):
    s = lax.axis_index("sp")
    f = lax.axis_index("fs")
    t = lax.axis_index("tp")
    rows = tok.shape[1]
    half = rows // 2
    depth = w_q_down.shape[0]
    kv_rank = wkv_all.shape[1]
    kv_core, q_core = t == 1, t == 0
    heads = wqn.shape[1] // NOPE_DIM
    groups = wpi.shape[1] // POOL_GROUP
    length = rows * n_sp

    def down(ref, owner, first=0, size=depth):
        start = pl.multiple_of(owner * depth + first, 16)
        return ref.at[pl.ds(start, size), :]

    pairs = (
        (w_kv_down, down(wkv_all, f)),
        (tokens.at[0], tok.at[t]),
        (norm_gain, gain.at[t]),
        (w_q_down, down(wq_all, f)),
        (w_k_rope, wkr),
        (w_pool_in, wpi),
        (kv_gain, kvg),
        (q_gain, qg),
        (w_pool_mix.at[pl.ds(t * groups, groups)], mix),
        (w_out_pool, wop),
        (w_q_nope, wqn),
        (w_q_rope, wqr),
        (w_k_up, wku),
        (w_v_up, wvu),
        (w_out_attn, woa),
    )
    slots = (0, 1, 2, 0, 3, 3, 4, 5, 6, 6, 7, 7, 7, 7, 8)
    loads = [
        pltpu.make_async_copy(src, dst, local_sem.at[slot])
        for slot, (src, dst) in zip(slots, pairs)
    ]
    (
        l_kv,
        l_tok,
        l_gain,
        l_q,
        l_kr,
        l_pi,
        l_kvg,
        l_qg,
        l_mix,
        l_op,
        l_qn,
        l_qr,
        l_ku,
        l_vu,
        l_oa,
    ) = loads
    for load in loads:
        if load is l_kv:
            pl.when(kv_core)(load.start)
        elif load is l_q:
            pl.when(q_core)(load.start)
        else:
            load.start()

    barrier = pltpu.get_barrier_semaphore()

    def greet(device):
        pl.semaphore_signal(barrier, inc=1, device_id=device, device_id_type=MESH)

    hops = n_fs == 4
    line = hops and n_sp == 4
    has_prev, has_next = s > 0, s < n_sp - 1
    mate = {"tp": 1 - t}
    above, below = {"sp": (s + 1) % n_sp}, {"sp": (s + n_sp - 1) % n_sp}
    parity = s % 2
    if hops:
        near = f + 1 - 2 * (f % 2)
        far = (f + 2) % 4
        across = 3 - f
    greet(mate)
    if line:
        greet({"fs": near})
        greet({"fs": far})
        pl.when(has_next)(lambda: greet(above))
        pl.when(has_prev)(lambda: greet(below))
        guests = 5 - (s == 0).astype(jnp.int32) - (s == n_sp - 1).astype(jnp.int32)
    else:
        for j in range(1, n_fs):
            greet({"fs": (f + j) % n_fs})
        for j in range(1, n_sp):
            greet({"sp": (s + j) % n_sp})
        guests = n_sp + n_fs - 1
    pl.semaphore_wait(barrier, guests)

    def tell(side, device):
        pl.semaphore_signal(word.at[side], inc=1, device_id=device, device_id_type=MESH)

    def hear(side, count):
        return lambda: pl.semaphore_wait(word.at[side], count)

    if line:

        def both_ways():
            tell(0, above)
            tell(1, below)

        pl.when(has_prev & has_next)(both_ways)

    def spread_word():
        def up():
            hear(0, 1)()
            tell(0, above)

        def down_():
            hear(1, 1)()
            tell(1, below)

        pl.when(s == n_sp - 2)(up)
        pl.when(s == 1)(down_)

    def hear_word():
        pl.when(s == n_sp - 1)(hear(0, 2))
        pl.when(s == 0)(hear(1, 2))

    def remote(src, dst, sent, slot, device):
        return pltpu.make_async_remote_copy(
            src_ref=src,
            dst_ref=dst,
            send_sem=send_sem.at[sent],
            recv_sem=recv_sem.at[slot],
            device_id=device,
            device_id_type=MESH,
        )

    def part_of(ref, count):
        return ref.at[pl.ds(0, count)]

    def all_sent(ref, count, sent):
        part = part_of(ref, count)
        remote(part, part, sent, TOK, mate).wait_send()

    def all_taken(ref, count, slot):
        part = part_of(ref, count)
        remote(part, part, MAIN, slot, mate).wait_recv()

    def all_loaded(*refs):
        slot = {id(ref): i for ref, i in zip((dst for _, dst in pairs), slots)}[id(refs[0])]
        line_bytes = 2 * woa.shape[1]
        total = sum(math.prod(ref.shape) * ref.dtype.itemsize for ref in refs)
        part = part_of(woa, total // line_bytes)
        pltpu.make_async_copy(part, part, local_sem.at[slot]).wait()

    sizes = (depth // 4,) * 3 + (depth // 8, depth // 16, depth // 16)
    places = tuple(sum(sizes[:turn]) for turn in range(len(sizes)))
    kv_turns = 2
    kv_rows = depth // kv_turns
    if hops:
        partners = senders = (near, far)
    else:
        partners = tuple((f + j) % n_fs for j in range(1, n_fs))
        senders = tuple((f + n_fs - j) % n_fs for j in range(1, n_fs))
    turns = range(len(sizes))

    def outgoing(ref, slot, first, size):
        part = down(ref, f, first, size)
        return [remote(part, part, MAIN, slot, {"fs": peer}) for peer in partners]

    def onward(ref, slot, first, size, core):
        piece = size // 2
        low, high = down(ref, near, first, piece), down(ref, far, first + piece, piece)
        return [
            remote(low, low, MAIN, slot, {"fs": far, "tp": core}),
            remote(high, high, MAIN, slot, {"fs": near, "tp": core}),
        ]

    def start(copies):
        for copy in copies:
            copy.start()

    kv_out = [
        outgoing(wkv_all, STAGE + turn, turn * kv_rows, kv_rows) for turn in range(kv_turns)
    ]
    q_out = [outgoing(wq_all, STAGE + turn, places[turn], sizes[turn]) for turn in turns]
    kv_last, lat_slot = STAGE + kv_turns, STAGE + len(sizes)
    q_last = STAGE + max(len(sizes) + 1, kv_turns + n_sp)
    if hops:
        kv_on = [
            onward(wkv_all, kv_last, turn * kv_rows, kv_rows, t) for turn in range(kv_turns)
        ]
        q_on = [
            onward(wq_all, q_last + turn // 3, places[turn], sizes[turn], 1 - t)
            for turn in turns
        ]
    else:
        kv_on = [[] for turn in range(kv_turns)]
        q_on = [[] for turn in turns]

    def from_shard(ref, owner, at=0, size=depth):
        first = pl.multiple_of(owner * depth + at, 128)
        return mm(hid[:, pl.ds(first, size)], ref[pl.ds(first, size), :])

    def from_near(ref):
        return functools.reduce(jnp.add, [from_shard(ref, owner) for owner in (f,) + senders])

    @pl.when(kv_core)
    def _():
        l_kv.wait()
        for copies in kv_out:
            start(copies)

    l_tok.wait()
    l_gain.wait()
    c_tok = remote(tok.at[t], tok.at[t], SIDE_A, TOK, mate)
    c_tok.start()
    c_gain = remote(gain.at[t], gain.at[t], SIDE_B, GAIN, mate)
    c_gain.start()
    lane = lax.broadcasted_iota(jnp.int32, (rows, 128), 1)
    place = s * rows + lax.broadcasted_iota(jnp.int32, (rows, 128), 0)
    quarter = ROPE_DIM // 4
    power = (lane % quarter).astype(F32) * (2.0 / (ROPE_DIM // 2))
    inverse = jnp.exp(power * (-math.log(THETA)))
    grid_row = place // GRID_W
    grid_col = place - grid_row * GRID_W
    in_a = (lane % ROPE_DIM) < (ROPE_DIM // 2)
    angle = jnp.where(in_a, grid_row, grid_col).astype(F32) * inverse
    is_u = (lane % (2 * quarter)) < quarter
    cosine = jnp.cos(angle)
    sine = jnp.where(is_u, -jnp.sin(angle), jnp.sin(angle))

    def rotated(pre):
        wide = pre.astype(BF16).astype(F32)
        swapped = jnp.where(is_u, pltpu.roll(wide, 128 - quarter, 1), pltpu.roll(wide, quarter, 1))
        return wide * cosine + swapped * sine

    if line:
        spread_word()
    c_gain.wait_recv()
    c_tok.wait_recv()
    whole = jnp.concatenate([tok[0], tok[1]], axis=1).astype(F32)
    lines = gain.shape[1]
    wide_gain = [gain[0].astype(F32), gain[1].astype(F32)]
    flat_gain = jnp.concatenate(
        [side[i : i + 1, :] for side in wide_gain for i in range(lines)], axis=1
    )
    hid[...] = normed(whole, flat_gain)

    own_rows = pl.ds(pl.multiple_of(s * rows, rows), rows)

    def rows_of(owner):
        return pl.ds(pl.multiple_of(owner * rows, rows), rows)

    if n_sp == 4:
        peers_to = (s + 1 - 2 * parity, (s + 2) % 4, 3 - s)
        peers_from = peers_to
    else:
        peers_to = tuple((s + j) % n_sp for j in range(1, n_sp))
        peers_from = tuple((s + n_sp - j) % n_sp for j in range(1, n_sp))

    def rope_copy(owner, device):
        return remote(ropes.at[owner], ropes.at[owner], BLOCK, ROPE, device)

    def latent(owner, sent, slot, device):
        here = kv_lat.at[rows_of(owner)]
        return remote(here, here, sent, slot, device)

    base = STAGE + kv_turns + 1
    taken = LATENT
    c_own = latent(s, GATHER, taken, mate)
    order_to = list(enumerate(peers_to))
    if n_sp == 4:
        high = s // 2
        edge = 1 - (s + high) % 2
        order_to = [(1 + edge, 3 - 3 * high), (2 - edge, 2 - high), order_to[0]]
    gather_out = [latent(s, GATHER, base + j, {"sp": peer}) for j, peer in order_to]
    gather_in = [latent(owner, GATHER, base + j, mate) for j, owner in enumerate(peers_from)]
    passed = [latent(owner, PASS, taken, mate) for owner in peers_from]

    all_loaded(wkr, wpi)
    pool_in = mm(hid[...], wpi[...]).astype(BF16)
    halo_out[0] = pool_in[rows - 2 * RIM :, :].astype(F32)[RIM:, :]
    halo_out[1] = pool_in[: 2 * RIM, :].astype(F32)[:RIM, :]
    c_up = remote(halo_out.at[0], halo_in.at[0], SIDE_A, UP, above)
    c_dn = remote(halo_out.at[1], halo_in.at[1], SIDE_B, DOWN, below)
    c_gain.wait_send()
    c_tok.wait_send()
    pl.when(has_next)(c_up.start)
    pl.when(has_prev)(c_dn.start)

    @pl.when(q_core)
    def _():
        l_q.wait()
        for copies in q_out:
            start(copies)


    key_pre = mm_t(hid[...], wkr[...])
    key_rope = rotated(jnp.concatenate([key_pre, key_pre], axis=1))
    lower_half = lax.broadcasted_iota(jnp.int32, (half, 128), 1) < ROPE_DIM
    ropes[s] = jnp.where(lower_half, key_rope[:half], key_rope[half:]).astype(BF16)
    if line:
        hear_word()
    for peer in peers_to:
        copy = rope_copy(s, {"sp": peer})
        copy.start()

    @pl.when(kv_core)
    def _():
        for turn in range(kv_turns):
            all_taken(wkv_all, len(senders) * kv_rows, STAGE + turn)
            start(kv_on[turn])

    def no_rim(side):
        def clear():
            halo_in[side] = jnp.zeros(halo_in.shape[1:], F32)

        return clear

    pl.when(has_prev)(c_up.wait_recv)
    pl.when(has_next)(c_dn.wait_recv)
    pl.when(s == 0)(no_rim(0))
    pl.when(s == n_sp - 1)(no_rim(1))
    halo = jnp.concatenate([halo_in[0], halo_in[1]], axis=0).astype(BF16)
    padded = jnp.concatenate([pool_in, halo], axis=0)
    span = rows + 2 * RIM
    k_index = lax.broadcasted_iota(jnp.int32, (rows, span), 1)
    q_index = lax.broadcasted_iota(jnp.int32, (rows, span), 0)
    k_place = jnp.where(
        k_index < rows,
        k_index,
        jnp.where(k_index < rows + RIM, k_index - rows - RIM, k_index - RIM),
    )
    offset = k_place - q_index
    l_kvg.wait()
    l_qg.wait()
    all_loaded(mix, wop)
    inside = (k_place + s * rows >= 0) & (k_place + s * rows < length)
    pooled = []
    for g in range(groups):
        group = t * groups + g
        window = jnp.int32(0)
        for index, size in enumerate(WINDOWS):
            window = jnp.where(group == index, size, window)
        before = window // 2
        band = jnp.where(
            inside & (offset >= -before) & (offset < window - before), 1.0, 0.0
        )
        count = jnp.sum(band, axis=1, keepdims=True)
        cols = slice(g * POOL_GROUP, (g + 1) * POOL_GROUP)
        mean = (mm(band.astype(BF16), padded[:, cols]) / count).astype(BF16)
        spread = (mean.astype(F32) - pool_in[:, cols].astype(F32)).astype(BF16)
        pooled.append(mm(spread, mix[g]).astype(BF16))
    pl.when(has_next)(c_up.wait_send)
    pl.when(has_prev)(c_dn.wait_send)
    acc[...] = mm(jnp.concatenate(pooled, axis=1), wop[...])


    @pl.when(kv_core)
    def _():
        kv_sum = from_near(wkv_all)
        if hops:
            all_taken(wkv_all, depth, kv_last)
            kv_sum = kv_sum + from_shard(wkv_all, across)
        kv_lat[own_rows] = normed(kv_sum.astype(BF16).astype(F32), kvg[...])
        start(gather_out + [c_own])

    @pl.when(q_core)
    def _():
        for turn in turns:
            all_taken(wq_all, len(senders) * sizes[turn], STAGE + turn)
            start(q_on[turn])

    def finish_rope(owner):
        here = rows_of(owner)
        packed = ropes[owner].astype(F32)
        swapped = pltpu.roll(packed, ROPE_DIM, 1)
        low = jnp.where(lower_half, packed, swapped)
        high = jnp.where(lower_half, swapped, packed)
        kcat[here, kv_rank:] = jnp.concatenate([low, high], axis=0).astype(BF16)

    all_taken(ropes, n_sp - 1, ROPE)
    all_sent(ropes, n_sp - 1, BLOCK)
    for owner in (s,) + peers_from:
        finish_rope(owner)

    c_first = remote(q_part, q_first, GATHER, LATENT, mate)
    c_lat = remote(q_lat, q_lat, SIDE_A, lat_slot, mate)
    lat_parts = [q_lat.at[pl.ds(part * half, half)] for part in range(2)]

    def pass_on(j):
        gather_in[j].wait_recv()
        passed[j].start()

    @pl.when(kv_core)
    def _():
        for j in range(n_sp - 3):
            pass_on(j)
        c_first.wait_recv()
        q_sum = q_first[...]
        if hops:
            early = sum(sizes[:3])
            all_taken(wq_all, early, q_last)
            q_sum = q_sum + from_shard(wq_all, across, 0, early)
            all_taken(wq_all, depth - early, q_last + 1)
            q_sum = q_sum + from_shard(wq_all, across, early, depth - early)
        for part, piece in enumerate(lat_parts):
            some = q_sum[part * half : (part + 1) * half].astype(BF16).astype(F32)
            piece[...] = normed(some, qg[...])
            remote(piece, piece, SIDE_A, lat_slot, mate).start()
        for j in range(n_sp - 3, n_sp - 1):
            pass_on(j)

    @pl.when(q_core)
    def _():
        q_part[...] = from_near(wq_all)
        c_first.start()
        c_lat.wait_recv()

    q_latent = q_lat[...]
    all_loaded(wqn, wqr, wku, wvu)
    l_oa.wait()
    q_nope = mm(q_latent, wqn[...]).astype(BF16)
    q_pre = mm(q_latent, wqr[...])
    low_lanes = lane < ROPE_DIM
    for h in range(heads):
        cols = slice(h * NOPE_DIM, (h + 1) * NOPE_DIM)
        absorbed = mm_t(q_nope[:, cols], wku[:, cols]).astype(BF16)
        if h % 2 == 0:
            turned = rotated(q_pre[:, h * ROPE_DIM : (h + 2) * ROPE_DIM])
        rope = jnp.where(low_lanes if h % 2 == 0 else ~low_lanes, turned, 0.0).astype(BF16)
        for part in range(2):
            piece = slice(part * half, (part + 1) * half)
            qcat[part, h * half : (h + 1) * half, :kv_rank] = absorbed[piece]
            qcat[part, h * half : (h + 1) * half, kv_rank:] = rope[piece]

    factor = (NOPE_DIM + ROPE_DIM) ** (-0.5) * math.log2(math.e)
    span_keys = rows * max(
        c for c in range(1, n_sp + 1) if n_sp % c == 0 and (c == 1 or rows * c <= SPAN_LIMIT)
    )
    spans = length // span_keys
    block = 4 * half

    @pl.when(q_core)
    def _():
        all_taken(kv_lat, n_sp * rows, LATENT)

    kcat[:, :kv_rank] = kv_lat[...]

    def scored(part, first, keys):
        return mm_t(qcat[part, pl.ds(first, block), :], keys)

    def weighed(scores, keys, state):
        top = jnp.max(scores, axis=1, keepdims=True)
        if state is not None:
            top = jnp.maximum(top, state[0])
        weights = jnp.exp2((scores - top) * factor)
        total = jnp.sum(weights, axis=1, keepdims=True)
        summed = mm(weights.astype(BF16), keys[:, :kv_rank])
        if state is not None:
            shrink = jnp.exp2((state[0] - top) * factor)
            total = total + state[1] * shrink
            summed = summed + state[2] * shrink
        return top, total, summed

    part_rows = heads * half
    blocks = part_rows // block

    def keep(order, index, state):
        ctx[pl.ds(order * part_rows + index * block, block), :] = (state[2] / state[1]).astype(BF16)

    def attended(order):
        pieces = []
        for h in range(heads):
            mixed_latent = ctx[pl.ds(order * part_rows + h * half, half), :]
            cols = slice(h * VALUE_DIM, (h + 1) * VALUE_DIM)
            pieces.append(mm(mixed_latent, wvu[:, cols]).astype(BF16))
        return jnp.concatenate(pieces, axis=1)

    def projected(features, part):
        own = acc[pl.ds(pl.multiple_of(part * half, half), half), :]
        return own + mm(features, woa[...])

    parts = (1 - t, t)
    c_share = remote(share, arrived, BLOCK, SHARE, mate)

    def give():
        share[...] = projected(attended(0), parts[0]).astype(BF16)
        c_share.start()

    if spans == 1:
        jobs = [(order, index) for order in range(2) for index in range(blocks)]
        ahead = scored(parts[0], 0, kcat[...])
        for i, (order, index) in enumerate(jobs):
            scores = ahead
            if i + 1 < len(jobs):
                later, place_of = jobs[i + 1]
                ahead = scored(parts[later], place_of * block, kcat[...])
            keep(order, index, weighed(scores, kcat[...], None))
            if i == blocks:
                give()
    else:
        for order in range(2):

            def one_block(index, carry):
                first = pl.multiple_of(index * block, block)

                def step(i, state):
                    start_key = pl.multiple_of(i * span_keys, span_keys)
                    keys = kcat[pl.ds(start_key, span_keys), :]
                    return weighed(scored(parts[order], first, keys), keys, state)

                keys = kcat[:span_keys, :]
                state = weighed(scored(parts[order], first, keys), keys, None)
                state = lax.fori_loop(1, spans, step, state)
                row = pl.multiple_of(order * part_rows + first, block)
                ctx[pl.ds(row, block), :] = (state[2] / state[1]).astype(BF16)
                return carry

            lax.fori_loop(0, blocks, one_block, 0, unroll=True)
            if order == 0:
                give()
    mine = projected(attended(1), parts[1])
    c_share.wait()
    out[0] = (mine + arrived[...].astype(F32)).astype(BF16)

    @pl.when(kv_core)
    def _():
        all_sent(wkv_all, (n_fs - 1) * depth, MAIN)
        all_sent(kv_lat, n_sp * rows, GATHER)
        all_sent(kv_lat, (n_sp - 1) * rows, PASS)
        c_lat.wait_send()

    @pl.when(q_core)
    def _():
        all_sent(wq_all, (n_fs - 1) * depth, MAIN)
        c_first.wait_send()


def solution(mesh):
    n_sp, n_fs = mesh.shape["sp"], mesh.shape["fs"]

    def on_device(*args):
        args = list(args)
        args[1] = args[1].reshape(-1, 128)
        for i in (3, 7):
            args[i] = args[i].reshape(1, -1)
        args[10] = args[10].T
        (tokens, gain, wqd, qg, wqn, wqr, wkvd, kvg, wku, wvu, wkr, wpi, mix, woa, wop) = args
        rows, cols = tokens.shape[1:]
        half = rows // 2
        heads = wqn.shape[1] // NOPE_DIM
        kv_rank = wkvd.shape[1]
        q_rank = wqd.shape[1]
        d_model = woa.shape[1]
        groups = wpi.shape[1] // POOL_GROUP

        def vmem(*shape, kind=BF16):
            return pltpu.VMEM(shape, kind)

        def same(array):
            return pltpu.VMEM(array.shape, array.dtype)

        dma = pltpu.SemaphoreType.DMA
        return pl.pallas_call(
            functools.partial(layer, n_sp, n_fs),
            out_shape=pltpu.VMEM((1, half, d_model), BF16),
            in_specs=[pl.BlockSpec(memory_space=pltpu.HBM)] * len(args),
            out_specs=pl.BlockSpec(memory_space=pltpu.VMEM),
            scratch_shapes=[
                vmem(2, rows, cols),
                vmem(2, cols // 128, 128),
                vmem(rows, 2 * cols),
                vmem(n_fs * wqd.shape[0], q_rank),
                vmem(n_fs * wkvd.shape[0], kv_rank),
                same(qg),
                same(kvg),
                same(wqn),
                same(wqr),
                same(wku),
                same(wvu),
                same(wkr),
                same(wpi),
                vmem(groups, POOL_GROUP, POOL_GROUP),
                same(woa),
                same(wop),
                vmem(2, RIM, wpi.shape[1], kind=F32),
                vmem(2, RIM, wpi.shape[1], kind=F32),
                vmem(rows, q_rank, kind=F32),
                vmem(rows, q_rank, kind=F32),
                vmem(rows, q_rank),
                vmem(n_sp * rows, kv_rank),
                vmem(n_sp, half, 2 * ROPE_DIM),
                vmem(n_sp * rows, kv_rank + 2 * ROPE_DIM),
                vmem(2, heads * half, kv_rank + 2 * ROPE_DIM),
                vmem(2 * heads * half, kv_rank),
                vmem(rows, d_model, kind=F32),
                vmem(half, d_model),
                vmem(half, d_model),
                dma((9,)),
                dma((6,)),
                dma((STAGE + max(7, n_sp + 2) + 2,)),
                pltpu.SemaphoreType.REGULAR((2,)),
            ],
            compiler_params=pltpu.CompilerParams(collective_id=0, has_side_effects=True, vmem_limit_bytes=40 * 1024 * 1024),
        )(*[pltpu.with_memory_space_constraint(a, pltpu.HBM) for a in args])

    placed = (
        P("fs", "sp", "tp"),
        P("tp"),
        P("fs", None),
        P(),
        P(None, "tp"),
        P(None, "tp"),
        P("fs", None),
        P(),
        P(None, "tp"),
        P(None, "tp"),
        P(),
        P(None, "tp"),
        P(),
        P("tp", None),
        P("tp", None),
    )
    return jax.shard_map(
        on_device,
        mesh=mesh,
        in_specs=placed,
        out_specs=P("fs", ("sp", "tp"), None),
        check_vma=False,
    )
```

```python
import functools
import math

import jax
import jax.numpy as jnp
from jax import lax
from jax.experimental import pallas as pl
from jax.experimental.pallas import tpu as pltpu
from jax.sharding import PartitionSpec as P

NOPE_DIM = 128
ROPE_DIM = 64
VALUE_DIM = 128
GRID_W = 64
POOL_GROUP = 256
EPS = 1e-06
THETA = 10000.0
WINDOWS = (2, 4, 8, 16)
RIM = 8
SPAN_LIMIT = 1024
F32 = jnp.float32
BF16 = jnp.bfloat16
MESH = pl.DeviceIdType.MESH
TOK, GAIN, UP, DOWN, LATENT, SHARE, ROPE, STAGE = range(8)
MAIN, GATHER, PASS, BLOCK, SIDE_A, SIDE_B = range(6)


def mm(a, b):
    return jnp.dot(a, b, preferred_element_type=F32)


def mm_t(a, b):
    return lax.dot_general(a, b, (((1,), (1,)), ((), ())), preferred_element_type=F32)


def normed(wide, gain):
    scale = lax.rsqrt(jnp.mean(wide * wide, axis=-1, keepdims=True) + EPS)
    return (wide * scale * gain).astype(BF16)


def layer(
    n_sp,
    n_fs,
    tokens,
    norm_gain,
    w_q_down,
    q_gain,
    w_q_nope,
    w_q_rope,
    w_kv_down,
    kv_gain,
    w_k_up,
    w_v_up,
    w_k_rope,
    w_pool_in,
    w_pool_mix,
    w_out_attn,
    w_out_pool,
    out,
    tok,
    gain,
    hid,
    wq_all,
    wkv_all,
    qg,
    kvg,
    wqn,
    wqr,
    wku,
    wvu,
    wkr,
    wpi,
    mix,
    woa,
    wop,
    halo_out,
    halo_in,
    q_part,
    q_first,
    q_lat,
    kv_lat,
    ropes,
    kcat,
    qcat,
    ctx,
    acc,
    share,
    arrived,
    local_sem,
    send_sem,
    recv_sem,
    word,
):
    s = lax.axis_index("sp")
    f = lax.axis_index("fs")
    t = lax.axis_index("tp")
    rows = tok.shape[1]
    half = rows // 2
    depth = w_q_down.shape[0]
    kv_rank = wkv_all.shape[1]
    kv_core, q_core = t == 1, t == 0
    heads = wqn.shape[1] // NOPE_DIM
    groups = wpi.shape[1] // POOL_GROUP
    length = rows * n_sp

    def down(ref, owner, first=0, size=depth):
        start = pl.multiple_of(owner * depth + first, 16)
        return ref.at[pl.ds(start, size), :]

    pairs = (
        (w_kv_down, down(wkv_all, f)),
        (tokens.at[0], tok.at[t]),
        (norm_gain, gain.at[t]),
        (w_q_down, down(wq_all, f)),
        (w_k_rope, wkr),
        (w_pool_in, wpi),
        (kv_gain, kvg),
        (q_gain, qg),
        (w_pool_mix.at[pl.ds(t * groups, groups)], mix),
        (w_out_pool, wop),
        (w_q_nope, wqn),
        (w_q_rope, wqr),
        (w_k_up, wku),
        (w_v_up, wvu),
        (w_out_attn, woa),
    )
    slots = (0, 1, 2, 0, 3, 3, 4, 5, 6, 6, 7, 7, 7, 7, 8)
    loads = [
        pltpu.make_async_copy(src, dst, local_sem.at[slot])
        for slot, (src, dst) in zip(slots, pairs)
    ]
    (
        l_kv,
        l_tok,
        l_gain,
        l_q,
        l_kr,
        l_pi,
        l_kvg,
        l_qg,
        l_mix,
        l_op,
        l_qn,
        l_qr,
        l_ku,
        l_vu,
        l_oa,
    ) = loads
    first_loads, later_loads = loads[:8], loads[8:]
    for load in first_loads:
        if load is l_kv:
            pl.when(kv_core)(load.start)
        elif load is l_q:
            pl.when(q_core)(load.start)
        else:
            load.start()

    barrier = pltpu.get_barrier_semaphore()

    def greet(device):
        pl.semaphore_signal(barrier, inc=1, device_id=device, device_id_type=MESH)

    hops = n_fs == 4
    line = hops and n_sp == 4
    has_prev, has_next = s > 0, s < n_sp - 1
    mate = {"tp": 1 - t}
    above, below = {"sp": (s + 1) % n_sp}, {"sp": (s + n_sp - 1) % n_sp}
    parity = s % 2
    if hops:
        near = f + 1 - 2 * (f % 2)
        far = (f + 2) % 4
        across = 3 - f
    greet(mate)
    if line:
        greet({"fs": near})
        greet({"fs": far})
        pl.when(has_next)(lambda: greet(above))
        pl.when(has_prev)(lambda: greet(below))
        guests = 5 - (s == 0).astype(jnp.int32) - (s == n_sp - 1).astype(jnp.int32)
    else:
        for j in range(1, n_fs):
            greet({"fs": (f + j) % n_fs})
        for j in range(1, n_sp):
            greet({"sp": (s + j) % n_sp})
        guests = n_sp + n_fs - 1
    pl.semaphore_wait(barrier, guests)

    def tell(side, device):
        pl.semaphore_signal(word.at[side], inc=1, device_id=device, device_id_type=MESH)

    def hear(side, count):
        return lambda: pl.semaphore_wait(word.at[side], count)

    if line:

        def both_ways():
            tell(0, above)
            tell(1, below)

        pl.when(has_prev & has_next)(both_ways)

    def spread_word():
        def up():
            hear(0, 1)()
            tell(0, above)

        def down_():
            hear(1, 1)()
            tell(1, below)

        pl.when(s == n_sp - 2)(up)
        pl.when(s == 1)(down_)

    def hear_word():
        pl.when(s == n_sp - 1)(hear(0, 2))
        pl.when(s == 0)(hear(1, 2))

    def remote(src, dst, sent, slot, device):
        return pltpu.make_async_remote_copy(
            src_ref=src,
            dst_ref=dst,
            send_sem=send_sem.at[sent],
            recv_sem=recv_sem.at[slot],
            device_id=device,
            device_id_type=MESH,
        )

    def part_of(ref, count):
        return ref.at[pl.ds(0, count)]

    def all_sent(ref, count, sent):
        part = part_of(ref, count)
        remote(part, part, sent, TOK, mate).wait_send()

    def all_taken(ref, count, slot):
        part = part_of(ref, count)
        remote(part, part, MAIN, slot, mate).wait_recv()

    def all_loaded(*refs):
        slot = {id(ref): i for ref, i in zip((dst for _, dst in pairs), slots)}[id(refs[0])]
        line_bytes = 2 * woa.shape[1]
        total = sum(math.prod(ref.shape) * ref.dtype.itemsize for ref in refs)
        part = part_of(woa, total // line_bytes)
        pltpu.make_async_copy(part, part, local_sem.at[slot]).wait()

    sizes = (depth // 4,) * 3 + (depth // 8, depth // 16, depth // 16)
    places = tuple(sum(sizes[:turn]) for turn in range(len(sizes)))
    kv_turns = 2
    kv_rows = depth // kv_turns
    if hops:
        partners = senders = (near, far)
    else:
        partners = tuple((f + j) % n_fs for j in range(1, n_fs))
        senders = tuple((f + n_fs - j) % n_fs for j in range(1, n_fs))
    turns = range(len(sizes))

    def outgoing(ref, slot, first, size):
        part = down(ref, f, first, size)
        return [remote(part, part, MAIN, slot, {"fs": peer}) for peer in partners]

    def onward(ref, slot, first, size, core):
        piece = size // 2
        low, high = down(ref, near, first, piece), down(ref, far, first + piece, piece)
        return [
            remote(low, low, MAIN, slot, {"fs": far, "tp": core}),
            remote(high, high, MAIN, slot, {"fs": near, "tp": core}),
        ]

    def start(copies):
        for copy in copies:
            copy.start()

    kv_out = [
        outgoing(wkv_all, STAGE + turn, turn * kv_rows, kv_rows) for turn in range(kv_turns)
    ]
    q_out = [outgoing(wq_all, STAGE + turn, places[turn], sizes[turn]) for turn in turns]
    kv_last, lat_slot = STAGE + kv_turns, STAGE + len(sizes)
    q_last = STAGE + max(len(sizes) + 1, kv_turns + n_sp)
    if hops:
        kv_on = [
            onward(wkv_all, kv_last, turn * kv_rows, kv_rows, t) for turn in range(kv_turns)
        ]
        q_on = [
            onward(wq_all, q_last + turn // 3, places[turn], sizes[turn], 1 - t)
            for turn in turns
        ]
    else:
        kv_on = [[] for turn in range(kv_turns)]
        q_on = [[] for turn in turns]

    def from_shard(ref, owner, at=0, size=depth):
        first = pl.multiple_of(owner * depth + at, 128)
        return mm(hid[:, pl.ds(first, size)], ref[pl.ds(first, size), :])

    def from_near(ref):
        return functools.reduce(jnp.add, [from_shard(ref, owner) for owner in (f,) + senders])

    @pl.when(kv_core)
    def _():
        l_kv.wait()
        for copies in kv_out:
            start(copies)

    l_tok.wait()
    l_gain.wait()
    c_tok = remote(tok.at[t], tok.at[t], SIDE_A, TOK, mate)
    c_tok.start()
    c_gain = remote(gain.at[t], gain.at[t], SIDE_B, GAIN, mate)
    c_gain.start()
    for load in later_loads:
        load.start()
    lane = lax.broadcasted_iota(jnp.int32, (rows, 128), 1)
    place = s * rows + lax.broadcasted_iota(jnp.int32, (rows, 128), 0)
    quarter = ROPE_DIM // 4
    power = (lane % quarter).astype(F32) * (2.0 / (ROPE_DIM // 2))
    inverse = jnp.exp(power * (-math.log(THETA)))
    grid_row = place // GRID_W
    grid_col = place - grid_row * GRID_W
    in_a = (lane % ROPE_DIM) < (ROPE_DIM // 2)
    angle = jnp.where(in_a, grid_row, grid_col).astype(F32) * inverse
    is_u = (lane % (2 * quarter)) < quarter
    cosine = jnp.cos(angle)
    sine = jnp.where(is_u, -jnp.sin(angle), jnp.sin(angle))

    def rotated(pre):
        wide = pre.astype(BF16).astype(F32)
        swapped = jnp.where(is_u, pltpu.roll(wide, 128 - quarter, 1), pltpu.roll(wide, quarter, 1))
        return wide * cosine + swapped * sine

    if line:
        spread_word()
    c_gain.wait_recv()
    c_tok.wait_recv()
    whole = jnp.concatenate([tok[0], tok[1]], axis=1).astype(F32)
    lines = gain.shape[1]
    wide_gain = [gain[0].astype(F32), gain[1].astype(F32)]
    flat_gain = jnp.concatenate(
        [side[i : i + 1, :] for side in wide_gain for i in range(lines)], axis=1
    )
    hid[...] = normed(whole, flat_gain)

    own_rows = pl.ds(pl.multiple_of(s * rows, rows), rows)

    def rows_of(owner):
        return pl.ds(pl.multiple_of(owner * rows, rows), rows)

    if n_sp == 4:
        peers_to = (s + 1 - 2 * parity, (s + 2) % 4, 3 - s)
        peers_from = peers_to
    else:
        peers_to = tuple((s + j) % n_sp for j in range(1, n_sp))
        peers_from = tuple((s + n_sp - j) % n_sp for j in range(1, n_sp))

    def rope_copy(owner, device):
        return remote(ropes.at[owner], ropes.at[owner], BLOCK, ROPE, device)

    def latent(owner, sent, slot, device):
        here = kv_lat.at[rows_of(owner)]
        return remote(here, here, sent, slot, device)

    base = STAGE + kv_turns + 1
    taken = LATENT
    c_own = latent(s, GATHER, taken, mate)
    order_to = list(enumerate(peers_to))
    if n_sp == 4:
        high = s // 2
        edge = 1 - (s + high) % 2
        order_to = [(1 + edge, 3 - 3 * high), (2 - edge, 2 - high), order_to[0]]
    gather_out = [latent(s, GATHER, base + j, {"sp": peer}) for j, peer in order_to]
    gather_in = [latent(owner, GATHER, base + j, mate) for j, owner in enumerate(peers_from)]
    passed = [latent(owner, PASS, taken, mate) for owner in peers_from]

    all_loaded(wkr, wpi)
    pool_in = mm(hid[...], wpi[...]).astype(BF16)
    halo_out[0] = pool_in[rows - 2 * RIM :, :].astype(F32)[RIM:, :]
    halo_out[1] = pool_in[: 2 * RIM, :].astype(F32)[:RIM, :]
    c_up = remote(halo_out.at[0], halo_in.at[0], SIDE_A, UP, above)
    c_dn = remote(halo_out.at[1], halo_in.at[1], SIDE_B, DOWN, below)
    c_gain.wait_send()
    c_tok.wait_send()
    pl.when(has_next)(c_up.start)
    pl.when(has_prev)(c_dn.start)

    @pl.when(q_core)
    def _():
        l_q.wait()
        for copies in q_out:
            start(copies)


    key_pre = mm_t(hid[...], wkr[...])
    key_rope = rotated(jnp.concatenate([key_pre, key_pre], axis=1))
    lower_half = lax.broadcasted_iota(jnp.int32, (half, 128), 1) < ROPE_DIM
    ropes[s] = jnp.where(lower_half, key_rope[:half], key_rope[half:]).astype(BF16)
    if line:
        hear_word()
    for peer in peers_to:
        copy = rope_copy(s, {"sp": peer})
        copy.start()

    @pl.when(kv_core)
    def _():
        for turn in range(kv_turns):
            all_taken(wkv_all, len(senders) * kv_rows, STAGE + turn)
            start(kv_on[turn])

    def no_rim(side):
        def clear():
            halo_in[side] = jnp.zeros(halo_in.shape[1:], F32)

        return clear

    pl.when(has_prev)(c_up.wait_recv)
    pl.when(has_next)(c_dn.wait_recv)
    pl.when(s == 0)(no_rim(0))
    pl.when(s == n_sp - 1)(no_rim(1))
    halo = jnp.concatenate([halo_in[0], halo_in[1]], axis=0).astype(BF16)
    padded = jnp.concatenate([pool_in, halo], axis=0)
    span = rows + 2 * RIM
    k_index = lax.broadcasted_iota(jnp.int32, (rows, span), 1)
    q_index = lax.broadcasted_iota(jnp.int32, (rows, span), 0)
    k_place = jnp.where(
        k_index < rows,
        k_index,
        jnp.where(k_index < rows + RIM, k_index - rows - RIM, k_index - RIM),
    )
    offset = k_place - q_index
    l_kvg.wait()
    l_qg.wait()
    all_loaded(mix, wop)
    inside = (k_place + s * rows >= 0) & (k_place + s * rows < length)
    pooled = []
    for g in range(groups):
        group = t * groups + g
        window = jnp.int32(0)
        for index, size in enumerate(WINDOWS):
            window = jnp.where(group == index, size, window)
        before = window // 2
        band = jnp.where(
            inside & (offset >= -before) & (offset < window - before), 1.0, 0.0
        )
        count = jnp.sum(band, axis=1, keepdims=True)
        cols = slice(g * POOL_GROUP, (g + 1) * POOL_GROUP)
        mean = (mm(band.astype(BF16), padded[:, cols]) / count).astype(BF16)
        spread = (mean.astype(F32) - pool_in[:, cols].astype(F32)).astype(BF16)
        pooled.append(mm(spread, mix[g]).astype(BF16))
    pl.when(has_next)(c_up.wait_send)
    pl.when(has_prev)(c_dn.wait_send)
    acc[...] = mm(jnp.concatenate(pooled, axis=1), wop[...])


    @pl.when(kv_core)
    def _():
        kv_sum = from_near(wkv_all)
        if hops:
            all_taken(wkv_all, depth, kv_last)
            kv_sum = kv_sum + from_shard(wkv_all, across)
        kv_lat[own_rows] = normed(kv_sum.astype(BF16).astype(F32), kvg[...])
        start(gather_out + [c_own])

    @pl.when(q_core)
    def _():
        for turn in turns:
            all_taken(wq_all, len(senders) * sizes[turn], STAGE + turn)
            start(q_on[turn])

    def finish_rope(owner):
        here = rows_of(owner)
        packed = ropes[owner].astype(F32)
        swapped = pltpu.roll(packed, ROPE_DIM, 1)
        low = jnp.where(lower_half, packed, swapped)
        high = jnp.where(lower_half, swapped, packed)
        kcat[here, kv_rank:] = jnp.concatenate([low, high], axis=0).astype(BF16)

    all_taken(ropes, n_sp - 1, ROPE)
    all_sent(ropes, n_sp - 1, BLOCK)
    for owner in (s,) + peers_from:
        finish_rope(owner)

    c_first = remote(q_part, q_first, GATHER, LATENT, mate)
    c_lat = remote(q_lat, q_lat, SIDE_A, lat_slot, mate)
    lat_parts = [q_lat.at[pl.ds(part * half, half)] for part in range(2)]

    def pass_on(j):
        gather_in[j].wait_recv()
        passed[j].start()

    @pl.when(kv_core)
    def _():
        for j in range(n_sp - 3):
            pass_on(j)
        c_first.wait_recv()
        q_sum = q_first[...]
        if hops:
            early = sum(sizes[:3])
            all_taken(wq_all, early, q_last)
            q_sum = q_sum + from_shard(wq_all, across, 0, early)
            all_taken(wq_all, depth - early, q_last + 1)
            q_sum = q_sum + from_shard(wq_all, across, early, depth - early)
        for part, piece in enumerate(lat_parts):
            some = q_sum[part * half : (part + 1) * half].astype(BF16).astype(F32)
            piece[...] = normed(some, qg[...])
            remote(piece, piece, SIDE_A, lat_slot, mate).start()
        for j in range(n_sp - 3, n_sp - 1):
            pass_on(j)

    @pl.when(q_core)
    def _():
        q_part[...] = from_near(wq_all)
        c_first.start()
        c_lat.wait_recv()

    q_latent = q_lat[...]
    all_loaded(wqn, wqr, wku, wvu)
    l_oa.wait()
    q_nope = mm(q_latent, wqn[...]).astype(BF16)
    q_pre = mm(q_latent, wqr[...])
    low_lanes = lane < ROPE_DIM
    for h in range(heads):
        cols = slice(h * NOPE_DIM, (h + 1) * NOPE_DIM)
        absorbed = mm_t(q_nope[:, cols], wku[:, cols]).astype(BF16)
        if h % 2 == 0:
            turned = rotated(q_pre[:, h * ROPE_DIM : (h + 2) * ROPE_DIM])
        rope = jnp.where(low_lanes if h % 2 == 0 else ~low_lanes, turned, 0.0).astype(BF16)
        for part in range(2):
            piece = slice(part * half, (part + 1) * half)
            qcat[part, h * half : (h + 1) * half, :kv_rank] = absorbed[piece]
            qcat[part, h * half : (h + 1) * half, kv_rank:] = rope[piece]

    factor = (NOPE_DIM + ROPE_DIM) ** (-0.5) * math.log2(math.e)
    span_keys = rows * max(
        c for c in range(1, n_sp + 1) if n_sp % c == 0 and (c == 1 or rows * c <= SPAN_LIMIT)
    )
    spans = length // span_keys
    block = 4 * half

    @pl.when(q_core)
    def _():
        all_taken(kv_lat, n_sp * rows, LATENT)

    kcat[:, :kv_rank] = kv_lat[...]

    def scored(part, first, keys):
        return mm_t(qcat[part, pl.ds(first, block), :], keys)

    def weighed(scores, keys, state):
        top = jnp.max(scores, axis=1, keepdims=True)
        if state is not None:
            top = jnp.maximum(top, state[0])
        weights = jnp.exp2((scores - top) * factor)
        total = jnp.sum(weights, axis=1, keepdims=True)
        summed = mm(weights.astype(BF16), keys[:, :kv_rank])
        if state is not None:
            shrink = jnp.exp2((state[0] - top) * factor)
            total = total + state[1] * shrink
            summed = summed + state[2] * shrink
        return top, total, summed

    part_rows = heads * half
    blocks = part_rows // block

    def keep(order, index, state):
        ctx[pl.ds(order * part_rows + index * block, block), :] = (state[2] / state[1]).astype(BF16)

    def attended(order):
        pieces = []
        for h in range(heads):
            mixed_latent = ctx[pl.ds(order * part_rows + h * half, half), :]
            cols = slice(h * VALUE_DIM, (h + 1) * VALUE_DIM)
            pieces.append(mm(mixed_latent, wvu[:, cols]).astype(BF16))
        return jnp.concatenate(pieces, axis=1)

    def projected(features, part):
        own = acc[pl.ds(pl.multiple_of(part * half, half), half), :]
        return own + mm(features, woa[...])

    parts = (1 - t, t)
    c_share = remote(share, arrived, BLOCK, SHARE, mate)

    def give():
        share[...] = projected(attended(0), parts[0]).astype(BF16)
        c_share.start()

    if spans == 1:
        jobs = [(order, index) for order in range(2) for index in range(blocks)]
        ahead = scored(parts[0], 0, kcat[...])
        for i, (order, index) in enumerate(jobs):
            scores = ahead
            if i + 1 < len(jobs):
                later, place_of = jobs[i + 1]
                ahead = scored(parts[later], place_of * block, kcat[...])
            keep(order, index, weighed(scores, kcat[...], None))
            if i == blocks:
                give()
    else:
        for order in range(2):

            def one_block(index, carry):
                first = pl.multiple_of(index * block, block)

                def step(i, state):
                    start_key = pl.multiple_of(i * span_keys, span_keys)
                    keys = kcat[pl.ds(start_key, span_keys), :]
                    return weighed(scored(parts[order], first, keys), keys, state)

                keys = kcat[:span_keys, :]
                state = weighed(scored(parts[order], first, keys), keys, None)
                state = lax.fori_loop(1, spans, step, state)
                row = pl.multiple_of(order * part_rows + first, block)
                ctx[pl.ds(row, block), :] = (state[2] / state[1]).astype(BF16)
                return carry

            lax.fori_loop(0, blocks, one_block, 0, unroll=True)
            if order == 0:
                give()
    mine = projected(attended(1), parts[1])
    c_share.wait()
    out[0] = (mine + arrived[...].astype(F32)).astype(BF16)

    @pl.when(kv_core)
    def _():
        all_sent(wkv_all, (n_fs - 1) * depth, MAIN)
        all_sent(kv_lat, n_sp * rows, GATHER)
        all_sent(kv_lat, (n_sp - 1) * rows, PASS)
        c_lat.wait_send()

    @pl.when(q_core)
    def _():
        all_sent(wq_all, (n_fs - 1) * depth, MAIN)
        c_first.wait_send()


def solution(mesh):
    n_sp, n_fs = mesh.shape["sp"], mesh.shape["fs"]

    def on_device(*args):
        args = list(args)
        args[1] = args[1].reshape(-1, 128)
        for i in (3, 7):
            args[i] = args[i].reshape(1, -1)
        args[10] = args[10].T
        (tokens, gain, wqd, qg, wqn, wqr, wkvd, kvg, wku, wvu, wkr, wpi, mix, woa, wop) = args
        rows, cols = tokens.shape[1:]
        half = rows // 2
        heads = wqn.shape[1] // NOPE_DIM
        kv_rank = wkvd.shape[1]
        q_rank = wqd.shape[1]
        d_model = woa.shape[1]
        groups = wpi.shape[1] // POOL_GROUP

        def vmem(*shape, kind=BF16):
            return pltpu.VMEM(shape, kind)

        def same(array):
            return pltpu.VMEM(array.shape, array.dtype)

        dma = pltpu.SemaphoreType.DMA
        return pl.pallas_call(
            functools.partial(layer, n_sp, n_fs),
            out_shape=pltpu.VMEM((1, half, d_model), BF16),
            in_specs=[pl.BlockSpec(memory_space=pltpu.HBM)] * len(args),
            out_specs=pl.BlockSpec(memory_space=pltpu.VMEM),
            scratch_shapes=[
                vmem(2, rows, cols),
                vmem(2, cols // 128, 128),
                vmem(rows, 2 * cols),
                vmem(n_fs * wqd.shape[0], q_rank),
                vmem(n_fs * wkvd.shape[0], kv_rank),
                same(qg),
                same(kvg),
                same(wqn),
                same(wqr),
                same(wku),
                same(wvu),
                same(wkr),
                same(wpi),
                vmem(groups, POOL_GROUP, POOL_GROUP),
                same(woa),
                same(wop),
                vmem(2, RIM, wpi.shape[1], kind=F32),
                vmem(2, RIM, wpi.shape[1], kind=F32),
                vmem(rows, q_rank, kind=F32),
                vmem(rows, q_rank, kind=F32),
                vmem(rows, q_rank),
                vmem(n_sp * rows, kv_rank),
                vmem(n_sp, half, 2 * ROPE_DIM),
                vmem(n_sp * rows, kv_rank + 2 * ROPE_DIM),
                vmem(2, heads * half, kv_rank + 2 * ROPE_DIM),
                vmem(2 * heads * half, kv_rank),
                vmem(rows, d_model, kind=F32),
                vmem(half, d_model),
                vmem(half, d_model),
                dma((9,)),
                dma((6,)),
                dma((STAGE + max(7, n_sp + 2) + 2,)),
                pltpu.SemaphoreType.REGULAR((2,)),
            ],
            compiler_params=pltpu.CompilerParams(collective_id=0, has_side_effects=True, vmem_limit_bytes=40 * 1024 * 1024),
        )(*[pltpu.with_memory_space_constraint(a, pltpu.HBM) for a in args])

    placed = (
        P("fs", "sp", "tp"),
        P("tp"),
        P("fs", None),
        P(),
        P(None, "tp"),
        P(None, "tp"),
        P("fs", None),
        P(),
        P(None, "tp"),
        P(None, "tp"),
        P(),
        P(None, "tp"),
        P(),
        P("tp", None),
        P("tp", None),
    )
    return jax.shard_map(
        on_device,
        mesh=mesh,
        in_specs=placed,
        out_specs=P("fs", ("sp", "tp"), None),
        check_vma=False,
    )
```
